256 devices in a mesh: sp: 16 (over y, x), tp: 16 (over z, core).
Axes of the slice: x: 4, y: 4, z: 8, core: 2. Of those that a mesh axis runs over, the one named last changes fastest.
Arguments:
- upstream: bfloat16 [4096, 4096], P('sp', 'tp'), may hold values from -6 to 6
- stream: bfloat16 [4096, 4096], P('sp', 'tp'), may hold values from -400 to 400
- norm_gain: float32 [4096], P('tp'), may hold values from 0.1 to 1.9
- routes: int32 [4096, 2], P('sp'), may hold values from 0 to 15, all different within a row; in each aligned block of 256 rows (0 to 255, 256 to 511, ...) at most 48 rows name the same one
- route_weights: float32 [4096, 2], P('sp'), may hold values from 0.1 to 1
- w_gate: bfloat16 [16, 4096, 2048], P('sp', None, 'tp'), may hold values from -0.09375 to 0.09375
- w_up: bfloat16 [16, 4096, 2048], P('sp', None, 'tp'), may hold values from -0.09375 to 0.09375
- w_down: bfloat16 [16, 2048, 4096], P('sp', 'tp'), may hold values from -0.125 to 0.125
- value_in: bfloat16 [4096, 2048], P('sp', 'tp'), may hold values from -6 to 6
- gate_in: bfloat16 [4096, 2048], P('sp', 'tp'), may hold values from -6 to 6
- conv_pre: bfloat16 [4096, 2048], P('sp', 'tp'), may hold values from -200 to 200
- ln_gain: float32 [2048], P('tp'), may hold values from 0.1 to 1.9
- conv_taps: float32 [31, 2048], P(None, 'tp'), may hold values from -1 to 1
- w_out: bfloat16 [2048, 4096], P('tp'), may hold values from -0.125 to 0.125
Outputs:
- grad_gate: float32 [16, 4096, 2048], P('sp', None, 'tp')
- grad_up: float32 [16, 4096, 2048], P('sp', None, 'tp')
- grad_down: float32 [16, 2048, 4096], P('sp', 'tp')
- grad_out: float32 [2048, 4096], P('tp', 'sp')
- value_grad: bfloat16 [4096, 2048], P('sp', 'tp')
- gate_grad: bfloat16 [4096, 2048], P('sp', 'tp')
The draws below stay inside these ranges and needn't reach their ends.
Inputs may be any that keep to these rules, and one draw needn't show every extreme that they name: `routes`: each token names two different experts. Among the tokens of one index of sp no expert is named more than 48 times, and in every draw some expert exactly 48 times.
All inputs are finite; a program needn't handle non-finite values.
Results may differ from the reference program's by a relative error of at most 0.0071.
Values may be sent and summed in bfloat16 or wider, within the bound.
No kernel may reach another device: no remote copies, remote signals or barrier semaphores. Data moves between devices by JAX's collectives and lax.ppermute only.
A program may use at most 128 MiB of HBM per device.

```python
import math
import jax
import jax.numpy as jnp
import numpy as np
from jax import lax

D = 4096
C = 2048
FF = 2048
TAPS = 31
TOK_DEV = 256
TOKENS = 4096
EXPERTS = 16
CAP = 48
N_SP = 16


def draw_stream(key, part):
    subkeys = jax.random.split(jax.random.fold_in(key, 11), 3)
    random_part = jnp.clip(jax.random.normal(subkeys[0], (TOKENS, D), jnp.float32), -6.0, 6.0)
    row_scale = jnp.exp(jax.random.uniform(subkeys[1], (TOKENS, 1), jnp.float32, 0.0, math.log(10.0)))
    rising = jnp.exp(math.log(10.0) * (jnp.arange(D, dtype=jnp.float32) + 0.5) / D)
    jitter = jnp.exp(jax.random.uniform(subkeys[2], (D,), jnp.float32, -0.3, 0.3))
    column_scale = rising * jitter
    return (random_part * row_scale * column_scale[None, :] / 3.0).astype(jnp.bfloat16)


def draw_conv_pre(key, part):
    subkeys = jax.random.split(jax.random.fold_in(key, 23), 4)
    random_part = jnp.clip(jax.random.normal(subkeys[0], (TOKENS, C), jnp.float32), -6.0, 6.0)
    row_scale = jnp.exp(jax.random.uniform(subkeys[1], (TOKENS, 1), jnp.float32, 0.0, math.log(4.0)))
    rising = jnp.exp(math.log(10.0) * (jnp.arange(C, dtype=jnp.float32) + 0.5) / C)
    jitter = jnp.exp(jax.random.uniform(subkeys[2], (C,), jnp.float32, -0.3, 0.3))
    column_scale = rising * jitter
    row_offset = 1.5 * jnp.clip(jax.random.normal(subkeys[3], (TOKENS, 1), jnp.float32), -3.0, 3.0)
    return ((random_part * column_scale[None, :] / 3.0 + row_offset) * row_scale).astype(jnp.bfloat16)


def with_spikes(entries, rng, source, target, blocks, factor):
    def block_of(position):
        return (jnp.arange(entries.shape[position]) // (entries.shape[position] // blocks)).reshape((-1,) + (1,) * (entries.ndim - 1 - position))

    first = jax.random.permutation(rng, blocks)[block_of(target)]
    other_side = (block_of(target) + blocks // 2) % blocks
    return jnp.where((block_of(source) == first) | (block_of(source) == other_side), factor * entries, entries)


def block_levels(own_key, dims, pieces, low, top_value):
    def one(position, blocks):
        draws = jax.random.uniform(jax.random.fold_in(jax.random.fold_in(own_key, 6), position), (blocks,), jnp.float32, low / len(pieces), top_value / len(pieces))
        return jnp.repeat(jnp.exp(draws), dims[position] // blocks).reshape((-1,) + (1,) * (len(dims) - position - 1))

    gain = one(*pieces[0])
    for cut in pieces[1:]:
        gain = gain * one(*cut)
    return gain


def assign_block(key, own, number, rows, count, top, reach, slope):
    sequence = jax.random.permutation(key, count)
    packed, common = shares(count, rows * top, reach, slope, True), shares(count, rows * top, reach, slope, False)
    places = jnp.arange(count)

    def named(sizes, turn):
        used = int((sizes > 0).sum())
        fixed = max(1, used // 4)
        shifted = fixed + (places - fixed + turn * (used - fixed)) % max(1, count - fixed)
        return jnp.zeros((count,), jnp.int32).at[sequence[jnp.where(places < fixed, places, shifted)]].set(jnp.asarray(sizes, jnp.int32))

    sizes = jnp.where(number % 4 == 0, named(packed, number // 4), named(common, number - number // 4 - 1))
    mixed = jax.random.permutation(jax.random.fold_in(own, 3), count)
    source_of, receiver = mixed[0:count // 2 * 2:2], mixed[1:count // 2 * 2:2]
    room = jnp.minimum(sizes[source_of] - 1, reach - sizes[receiver]) // 2
    room = jnp.where((source_of == sequence[0]) | (receiver == sequence[0]) | (sizes[receiver] == 0), 0, jnp.maximum(room, 0))
    shifted = jax.random.randint(jax.random.fold_in(own, 4), (count // 2,), 0, 1 << 20) % (room + 1)
    sizes = sizes.at[source_of].add(-shifted).at[receiver].add(shifted)
    labels = jnp.searchsorted(jnp.cumsum(sizes), jnp.arange(rows * top), side="right").astype(jnp.int32)
    listing = labels.reshape(top, rows).T
    listing = listing[jax.random.permutation(jax.random.fold_in(own, 1), rows)]
    turn = jax.random.randint(jax.random.fold_in(own, 2), (rows, 1), 0, top)
    return jnp.take_along_axis(listing, (jnp.arange(top)[None, :] + turn) % top, axis=1)


def shares(number_of, total, reach, lean, full):
    loads = [(1 << 20) // math.isqrt(grade ** lean) + 1 for grade in range(1, number_of + 1)]
    largest = reach if full else min(reach, max(-(-total // number_of), total * loads[0] // sum(loads)))
    least = 1 if total - largest >= number_of - 1 else 0
    holding, rest = [largest] + [least] * (number_of - 1), total - largest - least * (number_of - 1)
    while rest > 0:
        candidates = [i for i in range(1, number_of) if holding[i] < largest] or [i for i in range(1, number_of) if holding[i] < reach]
        whole, left = sum([loads[i] for i in candidates]), rest
        for i in candidates:
            addition = min(reach - holding[i], max(1, left * loads[i] // whole), rest)
            holding[i] = holding[i] + addition
            rest = rest - addition
    return np.array(holding)


def scatter_about(own_key, extent, width, limit, pieces=(), kind=jnp.bfloat16):
    values = jax.random.normal(own_key, extent, jnp.float32) * width
    if len(pieces) > 0:
        values = block_levels(own_key, extent, pieces, -0.22, 0.18) * values
    return jnp.clip(values, min=-limit, max=limit).astype(kind)


def bell_draw_with(own_key, extent, scale, most, cuts, heavy, held_as=jnp.bfloat16):
    drawn = scale * jax.random.normal(own_key, extent, jnp.float32)
    if cuts:
        drawn = drawn * block_levels(own_key, extent, cuts, -0.22, 0.18)
    return jnp.clip(with_spikes(drawn, jax.random.fold_in(own_key, 3), *heavy), -most, most).astype(held_as)


def setup_inputs(seed: int = 0) -> dict:
    splits = jax.random.split(jax.random.key(seed), 15)
    upstream = bell_draw_with(splits[0], (TOKENS, D), 1.0, 6.0, ((0, 16), (1, 16)), (0, 1, 16, 2.0))
    stream = draw_stream(jax.random.fold_in(splits[14], 71), 0)
    norm_gain = jnp.clip(1.0 + 0.18 * jax.random.normal(splits[2], (D,), jnp.float32), 0.1, 1.9)
    routes_keys = jax.random.split(jax.random.fold_in(splits[3], 1), TOKENS // TOK_DEV)
    routes_turns = jax.random.permutation(jax.random.fold_in(splits[3], 3), TOKENS // TOK_DEV)
    routes = jax.vmap(lambda own, number: assign_block(jax.random.fold_in(splits[3], 2), own, number, TOK_DEV, EXPERTS, 2, CAP, 1))(routes_keys, routes_turns).reshape((TOKENS, 2))
    route_weights = jnp.clip(jnp.exp(math.log(1.0) - 2.3025851 * jax.random.uniform(splits[4], (TOKENS, 2), jnp.float32) ** block_levels(splits[4], (TOKENS, 2), ((0, 16),), -0.2, 0.2)), 0.1, 1.0)
    w_gate = scatter_about(splits[5], (EXPERTS, D, FF), D ** -0.5, 0.09375, ((0, 16), (2, 16)))
    w_up = scatter_about(splits[6], (EXPERTS, D, FF), D ** -0.5, 0.09375, ((0, 16), (2, 16)))
    w_down = scatter_about(splits[7], (EXPERTS, FF, D), FF ** -0.5, 0.125, ((0, 16), (1, 16)))
    value_in = scatter_about(splits[8], (TOKENS, C), 1.0, 6.0, ((0, 16), (1, 16)))
    gate_in = scatter_about(splits[9], (TOKENS, C), 1.5, 6.0, ((0, 16), (1, 16)))
    conv_pre = draw_conv_pre(jax.random.fold_in(splits[14], 71), 0)
    ln_gain = jnp.clip(1.0 + 0.18 * jax.random.normal(splits[11], (C,), jnp.float32), 0.1, 1.9)
    conv_taps = scatter_about(splits[12], (TAPS, C), TAPS ** -0.5, 1.0, ((1, 16),), jnp.float32)
    w_out = scatter_about(splits[13], (C, D), C ** -0.5, 0.125, ((0, 16),))
    return dict(upstream=upstream, stream=stream, norm_gain=norm_gain, routes=routes, route_weights=route_weights, w_gate=w_gate, w_up=w_up, w_down=w_down, value_in=value_in, gate_in=gate_in, conv_pre=conv_pre, ln_gain=ln_gain, conv_taps=conv_taps, w_out=w_out)


EPSILON = 1e-06

def silu_slope(values):
    logistic = jax.nn.sigmoid(values)
    return logistic * (1.0 + values * (1.0 - logistic))

def reference(upstream, stream, norm_gain, routes, route_weights, w_gate, w_up, w_down, value_in, gate_in, conv_pre, ln_gain, conv_taps, w_out):
    tokens, model_width = stream.shape
    experts = w_gate.shape[0]
    channels = conv_pre.shape[1]
    tap_count = conv_taps.shape[0]
    capacity = 3 * TOK_DEV // N_SP
    expert_rows = N_SP * capacity
    residual = stream.astype(jnp.float32)
    inverse = lax.rsqrt(lax.optimization_barrier(jnp.mean(residual * residual, axis=1, keepdims=True)) + EPSILON)
    normed = (norm_gain[None, :] * residual * inverse).astype(jnp.bfloat16)
    flat_experts = routes.reshape(-1)
    one_hot = (flat_experts[:, None] == jnp.arange(experts, dtype=jnp.int32)[None, :]).astype(jnp.int32)
    blocked = one_hot.reshape(N_SP, 2 * TOK_DEV, experts)
    earlier = (jnp.cumsum(blocked, axis=1) - blocked) * blocked
    slot_rank = lax.optimization_barrier(jnp.sum(earlier, axis=2)).reshape(-1)
    source = jnp.arange(2 * tokens, dtype=jnp.int32) // (2 * TOK_DEV)
    slot_index = flat_experts * expert_rows + source * capacity + slot_rank
    token_of = jnp.full((experts * expert_rows,), tokens, jnp.int32).at[slot_index].set(jnp.arange(2 * tokens, dtype=jnp.int32) // 2)
    weight_of = jnp.zeros((experts * expert_rows,), jnp.float32).at[slot_index].set(route_weights.reshape(-1))
    normed_pad = jnp.concatenate([normed, jnp.zeros((1, model_width), jnp.bfloat16)], axis=0)
    upstream_pad = jnp.concatenate([upstream, jnp.zeros((1, model_width), jnp.bfloat16)], axis=0)

    def one_expert(operands):
        indices, weights, gate_mat, upper_mat, down_mat = operands
        inputs = normed_pad[indices]
        cotangent = (weights[:, None] * upstream_pad[indices].astype(jnp.float32)).astype(jnp.bfloat16)
        gate_pre = jnp.dot(inputs, gate_mat, preferred_element_type=jnp.float32)
        upper_pre = jnp.dot(inputs, upper_mat, preferred_element_type=jnp.float32)
        active = (jax.nn.silu(gate_pre) * upper_pre).astype(jnp.bfloat16)
        active_back = jnp.dot(cotangent, down_mat.T, preferred_element_type=jnp.float32)
        gate_back = (active_back * upper_pre * silu_slope(gate_pre)).astype(jnp.bfloat16)
        upper_back = (active_back * jax.nn.silu(gate_pre)).astype(jnp.bfloat16)
        grad_gate = jnp.dot(inputs.T, gate_back, preferred_element_type=jnp.float32)
        grad_up = jnp.dot(inputs.T, upper_back, preferred_element_type=jnp.float32)
        grad_down = jnp.dot(active.T, cotangent, preferred_element_type=jnp.float32)
        input_back = (jnp.dot(gate_back, gate_mat.T, preferred_element_type=jnp.float32) + jnp.dot(upper_back, upper_mat.T, preferred_element_type=jnp.float32)).astype(jnp.bfloat16)
        return (grad_gate, grad_up, grad_down, input_back)
    grad_gate, grad_up, grad_down, input_back = lax.map(one_expert, (token_of.reshape(experts, expert_rows), weight_of.reshape(experts, expert_rows), w_gate, w_up, w_down))
    token_back = jnp.zeros((tokens + 1, model_width), jnp.float32).at[token_of].add(input_back.reshape(-1, model_width).astype(jnp.float32))[:tokens]
    gained = norm_gain[None, :] * token_back
    inner_sum = lax.optimization_barrier(jnp.sum(gained * residual, axis=1, keepdims=True))
    norm_back = inverse * gained - residual * inverse ** 3 * inner_sum / model_width
    stream_grad = (upstream.astype(jnp.float32) + norm_back).astype(jnp.bfloat16)
    conv_vals = conv_pre.astype(jnp.float32)
    mean_val = lax.optimization_barrier(jnp.mean(conv_vals, axis=1, keepdims=True))
    variance = lax.optimization_barrier(jnp.mean(conv_vals * conv_vals, axis=1, keepdims=True)) - mean_val * mean_val
    inv_std = lax.rsqrt(variance + EPSILON)
    centred = (conv_vals - mean_val) * inv_std
    scaled = centred * ln_gain[None, :]
    mixed_out = jax.nn.silu(scaled).astype(jnp.bfloat16)
    grad_out = jnp.dot(mixed_out.T, stream_grad, preferred_element_type=jnp.float32)
    mixed_back = jnp.dot(stream_grad, w_out.T, preferred_element_type=jnp.float32)
    norm_in = mixed_back * silu_slope(scaled) * ln_gain[None, :]
    conv_back = inv_std * (norm_in - lax.optimization_barrier(jnp.mean(norm_in, axis=1, keepdims=True)) - centred * lax.optimization_barrier(jnp.mean(norm_in * centred, axis=1, keepdims=True)))
    padded = jnp.concatenate([conv_back, jnp.zeros((tap_count - 1, channels), jnp.float32)], axis=0)
    glu_back = jnp.zeros((tokens, channels), jnp.float32)
    for tap_index in range(tap_count):
        offset = tap_count - 1 - tap_index
        glu_back = glu_back + conv_taps[tap_index][None, :] * padded[offset:offset + tokens]
    gate_sigma = jax.nn.sigmoid(gate_in.astype(jnp.float32))
    value_grad = (glu_back * gate_sigma).astype(jnp.bfloat16)
    gate_grad = (glu_back * value_in.astype(jnp.float32) * gate_sigma * (1.0 - gate_sigma)).astype(jnp.bfloat16)
    return (grad_gate, grad_up, grad_down, grad_out, value_grad, gate_grad)
```

```python
import jax
import jax.numpy as jnp
from jax import lax
from jax.sharding import Mesh, PartitionSpec as P

EPSILON = 1e-06
TP = ("z", "c")
BF = jnp.bfloat16
F4 = jnp.float32


def of_everyone(value):
    count = 16
    everything = lax.all_to_all(
        jnp.broadcast_to(value[None], (count, *value.shape)), TP, 0, 0, tiled=True
    )
    return jnp.sum(everything, axis=0)


def in_one(arrays):
    total = of_everyone(jnp.concatenate([a.reshape(-1) for a in arrays]))
    out, at = [], 0
    for a in arrays:
        out.append(total[at : at + a.size].reshape(a.shape))
        at += a.size
    return out


def right(x):
    n = lax.axis_size("z")
    return lax.ppermute(x, "z", [(i, (i + 1) % n) for i in range(n)])


def left(x):
    n = lax.axis_size("z")
    return lax.ppermute(x, "z", [(i, (i - 1) % n) for i in range(n)])


def swap(x):
    return lax.ppermute(x, "c", [(0, 1), (1, 0)])


def silu_slope(values):
    logistic = jax.nn.sigmoid(values)
    return logistic * (1.0 + values * (1.0 - logistic))


def dot(a, b, ca, cb):
    return lax.dot_general(a, b, (((ca,), (cb,)), ((), ())), preferred_element_type=F4)


def per_device(
    upstream,
    stream,
    norm_gain,
    routes,
    route_weights,
    w_gate,
    w_up,
    w_down,
    value_in,
    gate_in,
    conv_pre,
    ln_gain,
    conv_taps,
    w_out,
):
    tok_rows, width_part = stream.shape
    n_sp = lax.axis_size("sp")
    n_z = lax.axis_size("z")
    n_tp = 2 * n_z
    z = lax.axis_index("z")
    core = lax.axis_index("c")
    model_width = width_part * n_tp
    channels = conv_pre.shape[1] * n_tp
    tap_count = conv_taps.shape[0]
    capacity = 3 * tok_rows // n_sp
    half_cap = capacity // 2
    experts = n_sp
    slot_count = experts * capacity
    rows = n_sp * half_cap
    wide = 2 * width_part

    gate_own, upper_own, down_own = w_gate[0], w_up[0], w_down[0]
    gu = jnp.concatenate(
        [gate_own, swap(gate_own), upper_own, swap(upper_own)], axis=1
    )
    down2 = jnp.concatenate([down_own, swap(down_own)], axis=0)
    hid = gate_own.shape[1]

    residual = stream.astype(F4)
    conv_vals = conv_pre.astype(F4)
    row_squares, conv_total, conv_squares = in_one(
        (
            jnp.sum(residual * residual, axis=1),
            jnp.sum(conv_vals, axis=1),
            jnp.sum(conv_vals * conv_vals, axis=1),
        )
    )
    inverse = lax.rsqrt(row_squares / model_width + EPSILON)[:, None]
    normed = (norm_gain[None, :] * residual * inverse).astype(BF)

    routes_t = routes.T
    weights_t = route_weights.T
    expert_iota = jnp.arange(experts, dtype=jnp.int32)[:, None]
    hot0 = (expert_iota == routes_t[0:1]).astype(BF)
    hot1 = (expert_iota == routes_t[1:2]).astype(BF)
    tok_iota = jnp.arange(tok_rows, dtype=jnp.int32)
    earlier = (tok_iota[:, None] < tok_iota[None, :]).astype(BF)
    before = dot(hot0 + hot1, earlier, 1, 0)
    rank0 = jnp.sum(before * hot0.astype(F4), axis=0).astype(jnp.int32)
    rank1 = jnp.sum(before * hot1.astype(F4), axis=0).astype(jnp.int32)
    slot0 = routes_t[0] * capacity + rank0
    slot1 = routes_t[1] * capacity + rank1
    slot_ids = jnp.arange(slot_count, dtype=jnp.int32)[:, None]
    hit0 = slot_ids == slot0[None, :]
    hit1 = slot_ids == slot1[None, :]
    picker = jnp.logical_or(hit0, hit1).astype(BF)
    slot_weight = jnp.sum(
        jnp.where(hit0, weights_t[0][None, :], 0.0) + jnp.where(hit1, weights_t[1][None, :], 0.0),
        axis=1,
    )
    sent_cot = (dot(picker, upstream, 1, 0) * slot_weight[:, None]).astype(BF)
    sent_in = dot(picker, normed, 1, 0).astype(BF)

    def dispatch(v):
        out = lax.all_to_all(
            v.reshape(2 * experts, half_cap, width_part), ("sp", "c"), 0, 0, tiled=True
        )
        out = out.reshape(n_sp, 2, half_cap, width_part)
        return jnp.concatenate([out[:, 0], out[:, 1]], axis=2).reshape(rows, wide)

    x0 = dispatch(sent_in)
    c0 = dispatch(sent_cot)

    def at(k):
        return lax.rem(z + (k + n_z), n_z)

    def piece(w, k, axis):
        return lax.dynamic_slice_in_dim(w, at(k) * wide, wide, axis=axis)

    inputs = jnp.zeros((rows, model_width), BF)
    cots = jnp.zeros((rows, model_width), BF)
    pre = jnp.zeros((rows, 4 * hid), F4)
    active_back = jnp.zeros((rows, 2 * hid), F4)
    half = n_z // 2

    def put(whole, block, k):
        return lax.dynamic_update_slice_in_dim(whole, block, at(k) * wide, axis=1)

    pre = dot(x0, piece(gu, 0, 0), 1, 0)
    active_back = dot(c0, piece(down2, 0, 1), 1, 1)
    inputs, cots = put(inputs, x0, 0), put(cots, c0, 0)
    xr = xl = x0
    cr = cl = c0
    for k in range(1, half + 1):
        xr = right(xr)
        if k < half:
            xl = left(xl)
        if k < half:
            cr = right(cr)
        cl = left(cl)
        pre = pre + dot(xr, piece(gu, -k, 0), 1, 0)
        inputs = put(inputs, xr, -k)
        active_back = active_back + dot(cl, piece(down2, k, 1), 1, 1)
        cots = put(cots, cl, k)
        if k < half:
            pre = pre + dot(xl, piece(gu, k, 0), 1, 0)
            inputs = put(inputs, xl, k)
            active_back = active_back + dot(cr, piece(down2, -k, 1), 1, 1)
            cots = put(cots, cr, -k)

    gate_pre = pre[:, : 2 * hid]
    upper_pre = pre[:, 2 * hid :]
    active = (jax.nn.silu(gate_pre) * upper_pre).astype(BF)
    gate_back = (active_back * upper_pre * silu_slope(gate_pre)).astype(BF)
    upper_back = (active_back * jax.nn.silu(gate_pre)).astype(BF)
    backs = jnp.concatenate([gate_back, upper_back], axis=1)

    hr = rows // 2

    def part(k, lo, hi):
        return dot(backs[lo:hi], piece(gu, k, 0), 1, 1)

    ra = right(part(half, 0, hr).astype(BF))
    la = left(part(half, hr, rows).astype(BF))
    rb = lb = None
    for k in range(half - 1, 0, -1):
        pr = part(k, 0, rows)
        pl_ = part(-k, 0, rows)
        ra = right((pr[:hr] + ra.astype(F4)).astype(BF))
        la = left((pl_[hr:] + la.astype(F4)).astype(BF))
        nb = pr[hr:] if rb is None else pr[hr:] + rb.astype(F4)
        mb = pl_[:hr] if lb is None else pl_[:hr] + lb.astype(F4)
        rb = right(nb.astype(BF))
        lb = left(mb.astype(BF))
    mine = part(0, 0, rows)
    input_back = jnp.concatenate(
        [
            mine[:hr] + ra.astype(F4) + lb.astype(F4),
            mine[hr:] + rb.astype(F4) + la.astype(F4),
        ],
        axis=0,
    ).astype(BF)

    def both(a, b, cols_second):
        if cols_second:
            return dot(a, b[:, :hid], 0, 0) + swap(dot(a, b[:, hid:], 0, 0))
        return dot(a[:, :hid], b, 0, 0) + swap(dot(a[:, hid:], b, 0, 0))

    grad_gate = both(inputs, gate_back, True)
    grad_up = both(inputs, upper_back, True)
    grad_down = both(active, cots, False)

    sent_back = jnp.moveaxis(input_back.reshape(n_sp, half_cap, 2, width_part), 2, 1)
    returned = lax.all_to_all(
        sent_back.reshape(2 * n_sp, half_cap, width_part), ("sp", "c"), 0, 0, tiled=True
    ).reshape(slot_count, width_part)
    token_back = dot(picker, returned, 0, 0)
    gained = norm_gain[None, :] * token_back
    inner_sum = of_everyone(jnp.sum(gained * residual, axis=1))
    norm_back = inverse * gained - residual * inverse**3 * (inner_sum / model_width)[:, None]
    stream_grad = (upstream.astype(F4) + norm_back).astype(BF)

    def put2(whole, block, k):
        return lax.dynamic_update_slice(whole, block[None], (at(k), 0, 0))

    ht = tok_rows // 2
    mine8 = jnp.zeros((n_z, tok_rows, width_part), BF)
    mine8 = put2(mine8, stream_grad, 0)
    gr = gl = stream_grad
    for k in range(1, half):
        gr = right(gr)
        gl = left(gl)
        mine8 = put2(mine8, gr, -k)
        mine8 = put2(mine8, gl, k)
    far = jnp.concatenate([right(gr[:ht]), left(gl[ht:])], axis=0)
    mine8 = put2(mine8, far, half)
    other8 = swap(mine8)

    mean_val = (conv_total / channels)[:, None]
    variance = (conv_squares / channels)[:, None] - mean_val * mean_val
    inv_std = lax.rsqrt(variance + EPSILON)
    centred = (conv_vals - mean_val) * inv_std
    scaled = centred * ln_gain[None, :]
    mixed_out = jax.nn.silu(scaled).astype(BF)

    first = core == 0
    even8 = jnp.where(first, mine8, other8)
    odd8 = jnp.where(first, other8, mine8)
    full_grad = jnp.stack([even8, odd8], axis=1).reshape(n_tp, tok_rows, width_part)
    full_grad = jnp.moveaxis(full_grad, 0, 1).reshape(tok_rows, model_width)

    out_parts = dot(full_grad, mixed_out, 0, 0).astype(BF)
    out_blocks = lax.all_to_all(
        out_parts.reshape(n_sp, model_width // n_sp, mixed_out.shape[1]), "sp", 0, 0, tiled=True
    )
    grad_out = jnp.sum(out_blocks.astype(F4), axis=0).T
    mixed_back = dot(full_grad, w_out, 1, 1)
    norm_in = mixed_back * silu_slope(scaled) * ln_gain[None, :]
    norm_total, norm_cross = in_one((jnp.sum(norm_in, axis=1), jnp.sum(norm_in * centred, axis=1)))
    conv_back = inv_std * (
        norm_in - (norm_total / channels)[:, None] - centred * (norm_cross / channels)[:, None]
    )
    next_rim = lax.ppermute(
        conv_back[: tap_count - 1], "sp", [(i + 1, i) for i in range(n_sp - 1)]
    )
    padded = jnp.concatenate([conv_back, next_rim], axis=0)
    glu_back = jnp.zeros(conv_back.shape, F4)
    for tap_index in range(tap_count):
        offset = tap_count - 1 - tap_index
        glu_back = glu_back + conv_taps[tap_index][None, :] * padded[offset : offset + tok_rows]
    gate_sigma = jax.nn.sigmoid(gate_in.astype(F4))
    value_grad = (glu_back * gate_sigma).astype(BF)
    gate_grad = (glu_back * value_in.astype(F4) * gate_sigma * (1.0 - gate_sigma)).astype(BF)
    return (grad_gate[None], grad_up[None], grad_down[None], grad_out, value_grad, gate_grad)


def solution(mesh):
    n_sp, n_tp = mesh.devices.shape
    split = Mesh(mesh.devices.reshape(n_sp, n_tp // 2, 2), ("sp", "z", "c"))
    return jax.shard_map(
        per_device,
        mesh=split,
        in_specs=(
            P("sp", TP),
            P("sp", TP),
            P(TP),
            P("sp", None),
            P("sp", None),
            P("sp", None, TP),
            P("sp", None, TP),
            P("sp", TP, None),
            P("sp", TP),
            P("sp", TP),
            P("sp", TP),
            P(TP),
            P(None, TP),
            P(TP, None),
        ),
        out_specs=(
            P("sp", None, TP),
            P("sp", None, TP),
            P("sp", TP, None),
            P(TP, "sp"),
            P("sp", TP),
            P("sp", TP),
        ),
        check_vma=False,
    )
```

```python
import jax
import jax.numpy as jnp
from jax import lax
from jax.experimental import pallas as pl
from jax.experimental.pallas import tpu as pltpu
from jax.sharding import Mesh, PartitionSpec as P

EPSILON = 1e-06
TP = ("z", "c")
BF = jnp.bfloat16
F4 = jnp.float32


def of_everyone(value):
    count = 16
    everything = lax.all_to_all(
        jnp.broadcast_to(value[None], (count, *value.shape)), TP, 0, 0, tiled=True
    )
    return jnp.sum(everything, axis=0)


def in_one(arrays):
    total = of_everyone(jnp.concatenate([a.reshape(-1) for a in arrays]))
    out, at = [], 0
    for a in arrays:
        out.append(total[at : at + a.size].reshape(a.shape))
        at += a.size
    return out


def right(x):
    n = lax.axis_size("z")
    return lax.ppermute(x, "z", [(i, (i + 1) % n) for i in range(n)])


def left(x):
    n = lax.axis_size("z")
    return lax.ppermute(x, "z", [(i, (i - 1) % n) for i in range(n)])


def hops(x, n_hops):
    n = lax.axis_size("z")
    return lax.ppermute(x, "z", [(i, (i + n_hops) % n) for i in range(n)])


def flip(x, bit):
    return lax.ppermute(x, "z", [(i, i ^ bit) for i in range(lax.axis_size("z"))])


def swap(x):
    return lax.ppermute(x, "c", [(0, 1), (1, 0)])


def silu_slope(values):
    logistic = jax.nn.sigmoid(values)
    return logistic * (1.0 + values * (1.0 - logistic))


def dot(a, b, ca, cb):
    return lax.dot_general(a, b, (((ca,), (cb,)), ((), ())), preferred_element_type=F4)


VMEM = pl.BlockSpec(memory_space=pltpu.VMEM)
SMEM = pl.BlockSpec(memory_space=pltpu.SMEM)
BIG = pltpu.CompilerParams(vmem_limit_bytes=40 * 2**20)


def scatter_body(routes, weights, upstream, picker, cot, *, experts, capacity):
    toks = upstream.shape[0]
    slots = experts * capacity
    r0, r1 = routes[0:1, :], routes[1:2, :]
    names = lax.broadcasted_iota(jnp.int32, (experts, toks), 0)
    hot0 = jnp.where(names == r0, 1.0, 0.0)
    hot1 = jnp.where(names == r1, 1.0, 0.0)
    earlier = jnp.where(
        lax.broadcasted_iota(jnp.int32, (toks, toks), 0)
        < lax.broadcasted_iota(jnp.int32, (toks, toks), 1),
        1.0,
        0.0,
    ).astype(BF)
    before = dot((hot0 + hot1).astype(BF), earlier, 1, 0)
    slot0 = r0 * capacity + jnp.sum(before * hot0, axis=0, keepdims=True).astype(jnp.int32)
    slot1 = r1 * capacity + jnp.sum(before * hot1, axis=0, keepdims=True).astype(jnp.int32)
    step = slots // 4
    for at in range(0, slots, step):
        ids = lax.broadcasted_iota(jnp.int32, (step, toks), 0) + at
        hit0, hit1 = ids == slot0, ids == slot1
        pick = (jnp.where(hit0, 1.0, 0.0) + jnp.where(hit1, 1.0, 0.0)).astype(BF)
        picker[at : at + step, :] = pick
        weight = jnp.sum(
            jnp.where(hit0, weights[0:1, :], 0.0) + jnp.where(hit1, weights[1:2, :], 0.0),
            axis=1,
            keepdims=True,
        )
        cot[at : at + step, :] = (dot(pick, upstream[...], 1, 0) * weight).astype(BF)


def grads_body(z, *refs, n, width, add):
    xs, cs = refs[:n], refs[n : 2 * n]
    backs, active_t = refs[2 * n : 2 * n + 2]
    rest = refs[2 * n + 2 :]
    old = rest[:3] if add else None
    gate, up, down = rest[-3:]
    hid = gate.shape[1]
    for k in range(n):
        at = pl.multiple_of(lax.rem(z[0] + k, n) * width, width)
        pair = dot(xs[k][...], backs[...], 0, 0)
        dn = dot(active_t[...], cs[k][...], 1, 0)
        g, u = pair[:, :hid], pair[:, hid:]
        if add:
            g = g + old[0][pl.ds(at, width), :]
            u = u + old[1][pl.ds(at, width), :]
            dn = dn + old[2][:, pl.ds(at, width)]
        gate[pl.ds(at, width), :] = g
        up[pl.ds(at, width), :] = u
        down[:, pl.ds(at, width)] = dn


def grads(z, xs, cs, backs, active_t, old):
    rows, width = xs[0].shape
    n, hid = len(xs), active_t.shape[0]
    add = old is not None
    args = [z, *xs, *cs, backs, active_t, *(old or ())]
    total = n * width
    return pl.pallas_call(
        lambda *r: grads_body(*r, n=n, width=width, add=add),
        out_shape=(
            jax.ShapeDtypeStruct((total, hid), F4),
            jax.ShapeDtypeStruct((total, hid), F4),
            jax.ShapeDtypeStruct((hid, total), F4),
        ),
        in_specs=[SMEM] + [VMEM] * (len(args) - 1),
        out_specs=(VMEM,) * 3,
        compiler_params=BIG,
        cost_estimate=pl.CostEstimate(
            flops=2 * rows * total * 3 * hid, transcendentals=0, bytes_accessed=16 * 2**20
        ),
        name="grads_own" if add else "grads_other",
    )(*args)


def mixed_body(zc, me, ml, oe, ol, w_out, slope, out, *, early, late, n):
    acc = jnp.zeros(out.shape, F4)
    width = me.shape[2]
    for ref, ks, flip_core in ((me, early, 0), (oe, early, 1), (ml, late, 0), (ol, late, 1)):
        core = zc[1] if flip_core == 0 else 1 - zc[1]
        for i, k in enumerate(ks):
            at = pl.multiple_of((2 * lax.rem(zc[0] + k, n) + core) * width, width)
            acc = acc + dot(ref[i], w_out[:, pl.ds(at, width)], 1, 1)
    out[...] = acc * slope[...]


def outer_body(zc, me, ml, oe, ol, mixed_t, out, *, early, late, n):
    for ref, ks, flip_core in ((me, early, 0), (oe, early, 1), (ml, late, 0), (ol, late, 1)):
        core = zc[1] if flip_core == 0 else 1 - zc[1]
        for i, k in enumerate(ks):
            at = 2 * lax.rem(zc[0] + k, n) + core
            out[at] = dot(mixed_t[...], ref[i], 1, 0).astype(BF)


def conv_body(back, rim, taps, value_in, gate_in, value_grad, gate_grad, padded):
    toks, n_taps = back.shape[0], taps.shape[0]
    padded[:toks, :] = back[...]
    padded[toks:, :] = rim[...]
    step = 64
    for at in range(0, toks, step):
        acc = jnp.zeros((step, back.shape[1]), F4)
        for tap in range(n_taps):
            lo = at + n_taps - 1 - tap
            acc = acc + taps[tap : tap + 1, :] * padded[lo : lo + step, :]
        sigma = jax.nn.sigmoid(gate_in[at : at + step, :].astype(F4))
        value = acc * sigma
        value_grad[at : at + step, :] = value.astype(BF)
        gate_grad[at : at + step, :] = (
            value * value_in[at : at + step, :].astype(F4) * (1.0 - sigma)
        ).astype(BF)


def per_device(
    upstream,
    stream,
    norm_gain,
    routes,
    route_weights,
    w_gate,
    w_up,
    w_down,
    value_in,
    gate_in,
    conv_pre,
    ln_gain,
    conv_taps,
    w_out,
):
    tok_rows, width_part = stream.shape
    n_sp = lax.axis_size("sp")
    n_z = lax.axis_size("z")
    n_tp = 2 * n_z
    z = lax.axis_index("z")
    core = lax.axis_index("c")
    model_width = width_part * n_tp
    channels = conv_pre.shape[1] * n_tp
    tap_count = conv_taps.shape[0]
    capacity = 3 * tok_rows // n_sp
    half_cap = capacity // 2
    experts = n_sp
    slot_count = experts * capacity
    rows = n_sp * half_cap
    wide = 2 * width_part

    gate_own, upper_own, down_own = w_gate[0], w_up[0], w_down[0]
    gu = jnp.concatenate(
        [gate_own, swap(gate_own), upper_own, swap(upper_own)], axis=1
    )
    down2 = jnp.concatenate([down_own, swap(down_own)], axis=0)
    hid = gate_own.shape[1]

    def dispatch(v):
        out = lax.all_to_all(
            v.reshape(2 * experts, half_cap, width_part), ("sp", "c"), 0, 0, tiled=True
        )
        out = out.reshape(n_sp, 2, half_cap, width_part)
        return jnp.concatenate([out[:, 0], out[:, 1]], axis=2).reshape(rows, wide)

    picker, sent_cot = pl.pallas_call(
        lambda *r: scatter_body(*r, experts=experts, capacity=capacity),
        out_shape=(
            jax.ShapeDtypeStruct((slot_count, tok_rows), BF),
            jax.ShapeDtypeStruct((slot_count, width_part), BF),
        ),
        in_specs=[VMEM] * 3,
        out_specs=(VMEM, VMEM),
        compiler_params=BIG,
        name="scatter",
    )(routes.T, route_weights.T, upstream)
    c0 = dispatch(sent_cot)

    residual = stream.astype(F4)
    conv_vals = conv_pre.astype(F4)
    sums = jnp.concatenate(
        [
            jnp.sum(residual * residual, axis=1),
            jnp.sum(conv_vals, axis=1),
            jnp.sum(conv_vals * conv_vals, axis=1),
        ]
    )
    sums, c0 = lax.optimization_barrier((sums, c0))
    row_squares, conv_total, conv_squares = jnp.split(of_everyone(sums), 3)
    inverse = lax.rsqrt(row_squares / model_width + EPSILON)[:, None]
    normed = (norm_gain[None, :] * residual * inverse).astype(BF)
    x0 = dispatch(dot(picker, normed, 1, 0).astype(BF))

    def at(k):
        return lax.rem(z + (k + n_z), n_z)

    def piece(w, k, axis):
        return lax.dynamic_slice_in_dim(w, at(k) * wide, wide, axis=axis)

    half = n_z // 2
    inputs, cots = [None] * n_z, [None] * n_z
    inputs[0], cots[0] = x0, c0
    pre = dot(x0, piece(gu, 0, 0), 1, 0)
    active_back = dot(c0, piece(down2, 0, 1), 1, 1)
    xr = xl = x0
    cr = cl = c0
    for k in range(1, half + 1):
        xr, cl = right(xr), left(cl)
        inputs[-k], cots[k] = xr, cl
        if k < half:
            xl, cr = left(xl), right(cr)
            inputs[k], cots[-k] = xl, cr
            active_back = active_back + dot(cr, piece(down2, -k, 1), 1, 1)
            pre = pre + dot(xl, piece(gu, k, 0), 1, 0)
        active_back = active_back + dot(cl, piece(down2, k, 1), 1, 1)
        pre = pre + dot(xr, piece(gu, -k, 0), 1, 0)

    gate_pre = pre[:, : 2 * hid]
    upper_pre = pre[:, 2 * hid :]
    active = (jax.nn.silu(gate_pre) * upper_pre).astype(BF)
    gate_back = (active_back * upper_pre * silu_slope(gate_pre)).astype(BF)
    upper_back = (active_back * jax.nn.silu(gate_pre)).astype(BF)
    backs = jnp.concatenate([gate_back, upper_back], axis=1)

    along = jnp.sum(gate_back.astype(F4) * gate_pre + upper_back.astype(F4) * upper_pre, axis=1)
    for bit in (1, 2, 4):
        along = along + flip(along, bit)

    hr = rows // 2

    def part(k, lo, hi):
        return dot(backs[lo:hi], piece(gu, k, 0), 1, 1)

    ra = right(part(half, 0, hr).astype(BF))
    la = left(part(half, hr, rows).astype(BF))
    rb = lb = None
    for k in range(half - 1, 0, -1):
        pr = part(k, 0, rows)
        pl_ = part(-k, 0, rows)
        ra = right((pr[:hr] + ra.astype(F4)).astype(BF))
        la = left((pl_[hr:] + la.astype(F4)).astype(BF))
        nb = pr[hr:] if rb is None else pr[hr:] + rb.astype(F4)
        mb = pl_[:hr] if lb is None else pl_[:hr] + lb.astype(F4)
        rb = right(nb.astype(BF))
        lb = left(mb.astype(BF))
    mine = part(0, 0, rows)
    input_back = jnp.concatenate(
        [
            mine[:hr] + ra.astype(F4) + lb.astype(F4),
            mine[hr:] + rb.astype(F4) + la.astype(F4),
        ],
        axis=0,
    ).astype(BF)

    def half_backs(lo):
        return jnp.concatenate([gate_back[:, lo : lo + hid], upper_back[:, lo : lo + hid]], axis=1)

    zs = z.astype(jnp.int32).reshape(1)
    others = grads(zs, inputs, cots, half_backs(hid), active[:, hid:].T, None)
    gots = [swap(v) for v in others]
    grad_gate, grad_up, grad_down = grads(
        zs, inputs, cots, half_backs(0), active[:, :hid].T, gots
    )

    hi = along.astype(BF)
    mid = (along - hi.astype(F4)).astype(BF)
    low = (along - hi.astype(F4) - mid.astype(F4)).astype(BF)
    extra = jnp.stack([hi, mid, low], axis=1)
    extra = jnp.pad(extra, ((0, 0), (0, 128 - 3)))
    sent_back = jnp.moveaxis(input_back.reshape(n_sp, half_cap, 2, width_part), 2, 1)
    extra = jnp.broadcast_to(
        extra.reshape(n_sp, 1, half_cap, 128), (n_sp, 2, half_cap, 128)
    )
    sent_back = jnp.concatenate([sent_back, extra], axis=3)
    returned = lax.all_to_all(
        sent_back.reshape(2 * n_sp, half_cap, width_part + 128), ("sp", "c"), 0, 0, tiled=True
    ).reshape(slot_count, width_part + 128)
    token_back = dot(picker, returned, 0, 0)
    inner = jnp.sum(token_back[:, width_part : width_part + 3], axis=1, keepdims=True)
    gained = norm_gain[None, :] * token_back[:, :width_part]
    norm_back = inverse * gained - residual * inverse**2 * (inner / model_width)
    stream_grad = (upstream.astype(F4) + norm_back).astype(BF)

    ht = tok_rows // 2
    p1, m1, p2, m2 = (hops(stream_grad, d) for d in (1, -1, 2, -2))
    p3, m3 = hops(p1, 2), hops(m1, -2)
    far = jnp.concatenate([hops(p2[:ht], 2), hops(m2[ht:], -2)], axis=0)
    early, late = (0, 1, 2, 6, 7), (3, 4, 5)
    mine_e = jnp.stack([stream_grad, m1, m2, p2, p1])
    mine_l = jnp.stack([m3, far, p3])
    other_e, other_l = swap(mine_e), swap(mine_l)

    mean_val = (conv_total / channels)[:, None]
    variance = (conv_squares / channels)[:, None] - mean_val * mean_val
    inv_std = lax.rsqrt(variance + EPSILON)
    centred = (conv_vals - mean_val) * inv_std
    scaled = centred * ln_gain[None, :]
    mixed_out = jax.nn.silu(scaled).astype(BF)

    zc = jnp.stack([z, core]).astype(jnp.int32)
    slope = silu_slope(scaled) * ln_gain[None, :]
    parts = (zc, mine_e, mine_l, other_e, other_l)
    norm_in = pl.pallas_call(
        lambda *r: mixed_body(*r, early=early, late=late, n=n_z),
        out_shape=jax.ShapeDtypeStruct(conv_pre.shape, F4),
        in_specs=[SMEM] + [VMEM] * 6,
        out_specs=VMEM,
        compiler_params=BIG,
        name="mixed",
    )(*parts, w_out, slope)
    out_parts = pl.pallas_call(
        lambda *r: outer_body(*r, early=early, late=late, n=n_z),
        out_shape=jax.ShapeDtypeStruct((n_sp, conv_pre.shape[1], width_part), BF),
        in_specs=[SMEM] + [VMEM] * 5,
        out_specs=VMEM,
        compiler_params=BIG,
        name="outer",
    )(*parts, mixed_out.T)
    norm_total, norm_cross = in_one((jnp.sum(norm_in, axis=1), jnp.sum(norm_in * centred, axis=1)))
    conv_back = inv_std * (
        norm_in - (norm_total / channels)[:, None] - centred * (norm_cross / channels)[:, None]
    )
    next_rim = lax.ppermute(conv_back[:32], "sp", [(i + 1, i) for i in range(n_sp - 1)])
    out_parts, next_rim = lax.optimization_barrier((out_parts, next_rim))
    grad_out = jnp.sum(
        lax.all_to_all(out_parts, "sp", 0, 0, tiled=True).astype(F4), axis=0
    )
    value_grad, gate_grad = pl.pallas_call(
        conv_body,
        out_shape=(jax.ShapeDtypeStruct(value_in.shape, BF),) * 2,
        in_specs=[VMEM] * 5,
        out_specs=(VMEM, VMEM),
        scratch_shapes=[pltpu.VMEM((tok_rows + 32, conv_pre.shape[1]), F4)],
        name="conv",
    )(conv_back, next_rim, conv_taps, value_in, gate_in)
    return (grad_gate[None], grad_up[None], grad_down[None], grad_out, value_grad, gate_grad)


def solution(mesh):
    n_sp, n_tp = mesh.devices.shape
    split = Mesh(mesh.devices.reshape(n_sp, n_tp // 2, 2), ("sp", "z", "c"))
    return jax.shard_map(
        per_device,
        mesh=split,
        in_specs=(
            P("sp", TP),
            P("sp", TP),
            P(TP),
            P("sp", None),
            P("sp", None),
            P("sp", None, TP),
            P("sp", None, TP),
            P("sp", TP, None),
            P("sp", TP),
            P("sp", TP),
            P("sp", TP),
            P(TP),
            P(None, TP),
            P(TP, None),
        ),
        out_specs=(
            P("sp", None, TP),
            P("sp", None, TP),
            P("sp", TP, None),
            P(TP, "sp"),
            P("sp", TP),
            P("sp", TP),
        ),
        check_vma=False,
    )
```

```python
import jax
import jax.numpy as jnp
from jax import lax
from jax.experimental import pallas as pl
from jax.experimental.pallas import tpu as pltpu
from jax.sharding import Mesh, PartitionSpec as P

EPSILON = 1e-06
TP = ("z", "c")
BF = jnp.bfloat16
F4 = jnp.float32


def of_everyone(value):
    count = 16
    everything = lax.all_to_all(
        jnp.broadcast_to(value[None], (count, *value.shape)), TP, 0, 0, tiled=True
    )
    return jnp.sum(everything, axis=0)


def in_one(arrays):
    total = of_everyone(jnp.concatenate([a.reshape(-1) for a in arrays]))
    out, at = [], 0
    for a in arrays:
        out.append(total[at : at + a.size].reshape(a.shape))
        at += a.size
    return out


def right(x):
    n = lax.axis_size("z")
    return lax.ppermute(x, "z", [(i, (i + 1) % n) for i in range(n)])


def left(x):
    n = lax.axis_size("z")
    return lax.ppermute(x, "z", [(i, (i - 1) % n) for i in range(n)])


def hops(x, n_hops):
    n = lax.axis_size("z")
    return lax.ppermute(x, "z", [(i, (i + n_hops) % n) for i in range(n)])


def swap(x):
    return lax.ppermute(x, "c", [(0, 1), (1, 0)])


def silu_slope(values):
    logistic = jax.nn.sigmoid(values)
    return logistic * (1.0 + values * (1.0 - logistic))


def dot(a, b, ca, cb):
    return lax.dot_general(a, b, (((ca,), (cb,)), ((), ())), preferred_element_type=F4)


VMEM = pl.BlockSpec(memory_space=pltpu.VMEM)
ANY = pl.BlockSpec(memory_space=pl.ANY)
SMEM = pl.BlockSpec(memory_space=pltpu.SMEM)
BIG = pltpu.CompilerParams(vmem_limit_bytes=40 * 2**20)


def scatter_body(routes, weights, upstream, stream, picker, sent, *, experts, capacity):
    toks = upstream.shape[0]
    slots = experts * capacity
    half = capacity // 2
    r0, r1 = routes[0:1, :], routes[1:2, :]
    names = lax.broadcasted_iota(jnp.int32, (experts, toks), 0)
    hot0 = jnp.where(names == r0, 1.0, 0.0)
    hot1 = jnp.where(names == r1, 1.0, 0.0)
    earlier = jnp.where(
        lax.broadcasted_iota(jnp.int32, (toks, toks), 0)
        < lax.broadcasted_iota(jnp.int32, (toks, toks), 1),
        1.0,
        0.0,
    ).astype(BF)
    before = dot((hot0 + hot1).astype(BF), earlier, 1, 0)
    slot0 = r0 * capacity + jnp.sum(before * hot0, axis=0, keepdims=True).astype(jnp.int32)
    slot1 = r1 * capacity + jnp.sum(before * hot1, axis=0, keepdims=True).astype(jnp.int32)
    blocks = 8
    step = blocks * capacity

    def rows_at(j, carry):
        at = j * (step // 2)
        ids = lax.broadcasted_iota(jnp.int32, (step // 2, toks), 0) + at
        one = jnp.where(ids == slot0, 1.0, 0.0) + jnp.where(ids == slot1, 1.0, 0.0)
        picker[pl.ds(pl.multiple_of(at, step // 2), step // 2), :] = one.astype(BF)
        wide = lax.broadcasted_iota(jnp.int32, (step, toks), 0)
        block = lax.shift_right_logical(wide * (65536 // capacity + 1), 16)
        place = wide - block * capacity
        ids = jnp.where(place >= half, place - half, place) + (block + j * blocks) * half
        hit0, hit1 = ids == slot0, ids == slot1
        pick = (jnp.where(hit0, 1.0, 0.0) + jnp.where(hit1, 1.0, 0.0)).astype(BF)
        weight = jnp.sum(
            jnp.where(hit0, weights[0:1, :], 0.0) + jnp.where(hit1, weights[1:2, :], 0.0),
            axis=1,
            keepdims=True,
        )
        is_cot = place[:, 0:1] >= half
        value = jnp.where(
            is_cot, dot(pick, upstream[...], 1, 0) * weight, dot(pick, stream[...], 1, 0)
        )
        sent[pl.ds(pl.multiple_of(j * step, step), step), :] = value.astype(BF)
        return carry

    lax.fori_loop(0, 2 * slots // step, rows_at, 0)


def offset_of(k, n):
    h = n // 2
    return jnp.where(k < h, jnp.where(k == 0, 0, n - k), jnp.where(k == n - 1, h, k - h + 1))


def load_all(pairs, sems):
    copies = [pltpu.make_async_copy(a, b, sems.at[i]) for i, (a, b) in enumerate(pairs)]
    for copy in copies:
        copy.start()
    for copy in copies:
        copy.wait()


def project_body(z, *refs, n):
    blocks, refs = refs[: n - 1], refs[n - 1 :]
    guo, gux, dno, dnx, gains, inv, own, oth, back, xs = refs[:10]
    buf, guo_v, gux_v, dno_v, dnx_v, sems = refs[10:]
    rows, width = own.shape[0], buf.shape[2]
    hid = dno.shape[0]
    load_all(
        [(guo, guo_v), (gux, gux_v), (dno, dno_v), (dnx, dnx_v)]
        + [(blocks[i], buf.at[i]) for i in range(n - 1)],
        sems,
    )
    own[...] = jnp.zeros(own.shape, F4)
    oth[...] = jnp.zeros(oth.shape, F4)
    back[...] = jnp.zeros(back.shape, F4)

    def step(k, carry):
        chip = lax.rem(z[0] + offset_of(k, n), n)
        at = pl.multiple_of(chip * width, width)
        x = buf[k, :rows, :].astype(F4)
        x = (gains[pl.ds(chip, 1), :] * x * inv[...]).astype(BF)
        xs[pl.ds(pl.multiple_of(k * rows, rows), rows), :] = x
        own[...] += dot(x, guo_v[pl.ds(at, width), :], 1, 0)
        oth[...] += dot(x, gux_v[pl.ds(at, width), :], 1, 0)
        c = buf[k, rows:, :]
        back[:, :hid] += dot(c, dno_v[:, pl.ds(at, width)], 1, 1)
        back[:, hid:] += dot(c, dnx_v[:, pl.ds(at, width)], 1, 1)
        return carry

    lax.fori_loop(0, n - 1, step, 0)


def in_parts(row):
    hi = row.astype(BF).astype(F4)
    mid = (row - hi).astype(BF).astype(F4)
    low = (row - hi - mid).astype(BF).astype(F4)
    return hi, mid, low


def part_rows(row):
    hi, mid, low = in_parts(row)
    shape = (16, row.shape[1])
    at = lax.broadcasted_iota(jnp.int32, shape, 0)
    rows = jnp.where(at == 0, hi, jnp.where(at == 1, mid, jnp.where(at == 2, low, 0.0)))
    return rows.astype(BF)


def whole_row(rows):
    rows = rows.astype(F4)
    return rows[0:1] + rows[1:2] + rows[2:3]


def finish_body(z, xf, cf, guo, gux, dno, dnx, gains, inv, own, oth, back, *refs, n):
    x4, b_own, b_oth, a_own, a_oth, along, send_r, send_l = refs[:8]
    guo_v, gux_v, dno_v, dnx_v, sems = refs[8:]
    rows, width = xf.shape
    hid = dno.shape[0]
    chip = lax.rem(z[0] + n // 2, n)
    at = pl.multiple_of(chip * width, width)
    load_all(
        [
            (guo.at[pl.ds(at, width), :], guo_v),
            (gux.at[pl.ds(at, width), :], gux_v),
            (dno.at[:, pl.ds(at, width)], dno_v),
            (dnx.at[:, pl.ds(at, width)], dnx_v),
        ],
        sems,
    )
    x = (gains[pl.ds(chip, 1), :] * xf[...].astype(F4) * inv[...]).astype(BF)
    x4[...] = x
    total = jnp.zeros((rows, 1), F4)
    for pre, gu_v, dn_v, lo, backs, act in (
        (own, guo_v, dno_v, 0, b_own, a_own),
        (oth, gux_v, dnx_v, hid, b_oth, a_oth),
    ):
        both = pre[...] + dot(x, gu_v[...], 1, 0)
        gate, upper = both[:, :hid], both[:, hid:]
        ab = back[:, lo : lo + hid] + dot(cf[...], dn_v[...], 1, 1)
        sig = jax.nn.sigmoid(gate)
        silu = gate * sig
        act[...] = (silu * upper).astype(BF)
        gb = (ab * upper * (sig * (1.0 + gate * (1.0 - sig)))).astype(BF)
        ub = (ab * silu).astype(BF)
        backs[:, :hid] = gb
        backs[:, hid:] = ub
        total = total + jnp.sum(
            gb.astype(F4) * gate + ub.astype(F4) * upper, axis=1, keepdims=True
        )
    row = jnp.broadcast_to(total, (rows, 128)).T[0:8, :]
    along[:, :rows] = row
    along[:, rows:] = jnp.zeros((8, width - rows), F4)
    part = dot(b_own[...], guo_v[...], 1, 1) + dot(b_oth[...], gux_v[...], 1, 1)
    hr = rows // 2
    send_r[:hr, :] = part[:hr].astype(BF)
    send_r[hr:, :] = part_rows(along[0:1, :])
    send_l[...] = part[hr:].astype(BF)


def parts_body(b_own, b_oth, guo, gux, out):
    out[...] = (dot(b_own[...], guo[...], 1, 1) + dot(b_oth[...], gux[...], 1, 1)).astype(BF)


def hop_body(z, parts, along, ra, la, out_r, out_l, *, k, n, first):
    rows = parts.shape[0]
    width = out_r.shape[1]
    hr = rows // 2

    def block(j):
        at = pl.multiple_of(lax.rem(z[0] + (j + n), n) * width, width)
        return parts[:, pl.ds(at, width)].astype(F4)

    own = along[0:1, :]
    pr, pl_ = block(k), block(-k)
    if first:
        out_r[:hr, :] = (pr[:hr] + ra[:hr, :].astype(F4)).astype(BF)
        out_r[hr:rows, :] = pr[hr:].astype(BF)
        out_r[rows:, :] = part_rows(own + whole_row(ra[hr:, :]))
        out_l[:hr, :] = pl_[:hr].astype(BF)
        out_l[hr:rows, :] = (pl_[hr:] + la[...].astype(F4)).astype(BF)
        out_l[rows:, :] = part_rows(own)
    else:
        out_r[:rows, :] = (pr + ra[:rows, :].astype(F4)).astype(BF)
        out_r[rows:, :] = part_rows(own + whole_row(ra[rows:, :]))
        out_l[:rows, :] = (pl_ + la[:rows, :].astype(F4)).astype(BF)
        out_l[rows:, :] = part_rows(own + whole_row(la[rows:, :]))


def pack_body(z, parts, along, ra, la, out, *, n_sp):
    rows = parts.shape[0]
    width = ra.shape[1]
    half = width // 2
    step = rows // n_sp
    at = pl.multiple_of(z[0] * width, width)
    row = along[0:1, :] + whole_row(ra[rows:, :]) + whole_row(la[rows:, :])
    col = jnp.broadcast_to(row[:, :rows], (128, rows)).T
    hi, mid, low = in_parts(col)
    lane = lax.broadcasted_iota(jnp.int32, (rows, 128), 1)
    extra = jnp.where(lane == 0, hi, jnp.where(lane == 1, mid, jnp.where(lane == 2, low, 0.0)))
    value = (
        parts[:, pl.ds(at, width)].astype(F4) + ra[:rows, :].astype(F4) + la[:rows, :].astype(F4)
    )
    for s in range(n_sp):
        v = value[s * step : (s + 1) * step]
        e = extra[s * step : (s + 1) * step]
        both = jnp.concatenate([v[:, :half], v[:, half:]], axis=0)
        out[2 * s * step : 2 * (s + 1) * step, :half] = both.astype(BF)
        out[2 * s * step : 2 * (s + 1) * step, half:] = jnp.concatenate([e, e], axis=0).astype(BF)


def grads_body(z, *refs, n, add):
    xs, x4 = refs[0], refs[1]
    blocks, cf = refs[2 : n + 1], refs[n + 1]
    backs, act = refs[n + 2], refs[n + 3]
    refs = refs[n + 4 :]
    if add:
        old, gate, up, down, xbuf, cbuf, sems = refs
    else:
        out, xbuf, cbuf, sems = refs
    rows, width = x4.shape
    hid = act.shape[1]
    near = (n - 1) * rows
    load_all(
        [(xs, xbuf.at[pl.ds(0, near), :]), (x4, xbuf.at[pl.ds(near, rows), :])]
        + [
            (blocks[i].at[pl.ds(rows, rows), :], cbuf.at[pl.ds(i * rows, rows), :])
            for i in range(n - 1)
        ]
        + [(cf, cbuf.at[pl.ds(near, rows), :])],
        sems,
    )

    def step(k, carry):
        at = pl.multiple_of(lax.rem(z[0] + offset_of(k, n), n) * width, width)
        mine = pl.ds(pl.multiple_of(k * rows, rows), rows)
        pair = dot(xbuf[mine, :], backs[...], 0, 0)
        dn = dot(act[...], cbuf[mine, :], 0, 0)
        if add:
            gate[pl.ds(at, width), :] = pair[:, :hid] + old[0, pl.ds(at, width), :].astype(F4)
            up[pl.ds(at, width), :] = pair[:, hid:] + old[1, pl.ds(at, width), :].astype(F4)
            for q in range(width // hid):
                lo = pl.multiple_of(at + q * hid, hid)
                down[:, pl.ds(lo, hid)] = dn[:, q * hid : (q + 1) * hid] + old[
                    2, pl.ds(lo, hid), :
                ].astype(F4)
        else:
            out[0, pl.ds(at, width), :] = pair[:, :hid].astype(BF)
            out[1, pl.ds(at, width), :] = pair[:, hid:].astype(BF)
            for q in range(width // hid):
                lo = pl.multiple_of(at + q * hid, hid)
                out[2, pl.ds(lo, hid), :] = dn[:, q * hid : (q + 1) * hid].astype(BF)
        return carry

    lax.fori_loop(0, n, step, 0)


def grads(z, xs, x4, blocks, cf, backs, act, old):
    rows, width = x4.shape
    n, hid = len(blocks) + 1, act.shape[1]
    add = old is not None
    total = n * width
    args = [z, xs, x4, *blocks, cf, backs, act] + ([old] if add else [])
    if add:
        out_shape = tuple(
            jax.ShapeDtypeStruct(t, F4) for t in ((total, hid), (total, hid), (hid, total))
        )
        out_specs = (VMEM,) * 3
    else:
        out_shape, out_specs = jax.ShapeDtypeStruct((3, total, hid), BF), VMEM
    return pl.pallas_call(
        lambda *r: grads_body(*r, n=n, add=add),
        out_shape=out_shape,
        in_specs=[SMEM] + [ANY] * (n + 2) + [VMEM] * (3 if add else 2),
        out_specs=out_specs,
        scratch_shapes=[
            pltpu.VMEM((n * rows, width), BF),
            pltpu.VMEM((n * rows, width), BF),
            pltpu.SemaphoreType.DMA((n + 2,)),
        ],
        compiler_params=BIG,
        cost_estimate=pl.CostEstimate(
            flops=8 * rows * total * 3 * hid, transcendentals=0, bytes_accessed=16 * 2**20
        ),
        name="grads_own" if add else "grads_other",
    )(*args)


def stack_body(*refs):
    refs, sems = refs[:-1], refs[-1]
    srcs, out = refs[:-1], refs[-1]
    pairs, at = [], 0
    flat = out.reshape(out.shape[0] * out.shape[1], out.shape[2])
    for src in srcs:
        pairs.append((src, flat.at[pl.ds(at, src.shape[0]), :]))
        at += src.shape[0]
    load_all(pairs, sems)


def mixed_body(zc, mine, other, w_out, slope, done, out, *, n):
    del done
    width = mine.shape[2]
    out[...] = jnp.zeros(out.shape, F4)
    for ref, core in ((mine, zc[1]), (other, 1 - zc[1])):
        acc = jnp.zeros(out.shape, F4)
        for k in range(n):
            at = pl.multiple_of((2 * lax.rem(zc[0] + k, n) + core) * width, width)
            acc = acc + dot(ref[k], w_out[:, pl.ds(at, width)], 1, 1)
        out[...] += acc
    out[...] *= slope[...]


def outer_body(zc, mine, other, mixed_t, out, *, n):
    for ref, core in ((mine, zc[1]), (other, 1 - zc[1])):
        for k in range(n):
            out[2 * lax.rem(zc[0] + k, n) + core] = dot(mixed_t[...], ref[k], 1, 0).astype(BF)


def conv_body(back, rim, taps, value_in, gate_in, value_grad, gate_grad, padded):
    toks, n_taps = back.shape[0], taps.shape[0]
    padded[:toks, :] = back[...]
    padded[toks:, :] = rim[...]
    step = 64
    for at in range(0, toks, step):
        acc = jnp.zeros((step, back.shape[1]), F4)
        for tap in range(n_taps):
            lo = at + n_taps - 1 - tap
            acc = acc + taps[tap : tap + 1, :] * padded[lo : lo + step, :]
        sigma = jax.nn.sigmoid(gate_in[at : at + step, :].astype(F4))
        value = acc * sigma
        value_grad[at : at + step, :] = value.astype(BF)
        gate_grad[at : at + step, :] = (
            value * value_in[at : at + step, :].astype(F4) * (1.0 - sigma)
        ).astype(BF)


def per_device(
    upstream,
    stream,
    norm_gain,
    routes,
    route_weights,
    w_gate,
    w_up,
    w_down,
    value_in,
    gate_in,
    conv_pre,
    ln_gain,
    conv_taps,
    w_out,
):
    tok_rows, width_part = stream.shape
    n_sp = lax.axis_size("sp")
    n_z = lax.axis_size("z")
    n_tp = 2 * n_z
    z = lax.axis_index("z")
    core = lax.axis_index("c")
    model_width = width_part * n_tp
    channels = conv_pre.shape[1] * n_tp
    tap_count = conv_taps.shape[0]
    capacity = 3 * tok_rows // n_sp
    half_cap = capacity // 2
    experts = n_sp
    slot_count = experts * capacity
    rows = n_sp * half_cap
    wide = 2 * width_part

    zs = z.astype(jnp.int32).reshape(1)
    half = n_z // 2
    hid = w_gate.shape[2]

    picker, sent = pl.pallas_call(
        lambda *r: scatter_body(*r, experts=experts, capacity=capacity),
        out_shape=(
            jax.ShapeDtypeStruct((slot_count, tok_rows), BF),
            jax.ShapeDtypeStruct((2 * slot_count, width_part), BF),
        ),
        in_specs=[VMEM] * 4,
        out_specs=(VMEM, VMEM),
        compiler_params=BIG,
        name="scatter",
    )(routes.T, route_weights.T, upstream, stream)
    arrived = lax.all_to_all(
        sent.reshape(2 * experts, capacity, width_part), ("sp", "c"), 0, 0, tiled=True
    )
    arrived = arrived.reshape(n_sp, 2, 2, half_cap, width_part)
    b0 = jnp.transpose(arrived, (2, 0, 3, 1, 4)).reshape(2 * rows, wide)

    gu_own = jnp.concatenate([w_gate[0], w_up[0]], axis=1)
    down_own = w_down[0]
    gu_oth, down_oth = swap(gu_own), swap(down_own)

    r1, l1 = right(b0), left(b0)
    r2, l2 = right(r1), left(l1)
    r3, l3 = right(r2), left(l2)
    xf, cf = right(r3[:rows]), left(l3[rows:])

    residual = stream.astype(F4)
    conv_vals = conv_pre.astype(F4)
    own_rows = b0[:rows].astype(F4)
    row_part = jnp.sum(own_rows * own_rows, axis=1)
    nothing = jnp.zeros_like(row_part)
    vector = jnp.concatenate(
        [
            jnp.sum(residual * residual, axis=1),
            jnp.sum(conv_vals, axis=1),
            jnp.sum(conv_vals * conv_vals, axis=1),
            jnp.where(core == 0, row_part, nothing),
            jnp.where(core == 0, nothing, row_part),
            norm_gain,
        ]
    )
    told = lax.all_to_all(
        jnp.broadcast_to(vector[None, None], (n_tp, 1, vector.size)), TP, 0, 0, tiled=True
    )[:, 0]
    cut = 3 * tok_rows + 2 * rows
    total = jnp.sum(told[:, :cut], axis=0)
    gains = told[:, cut:].reshape(n_z, wide)
    row_squares, conv_total, conv_squares = jnp.split(total[: 3 * tok_rows], 3)
    slot_squares = jnp.where(
        core == 0, total[3 * tok_rows : 3 * tok_rows + rows], total[3 * tok_rows + rows :]
    )
    inverse = lax.rsqrt(row_squares / model_width + EPSILON)[:, None]
    slot_inverse = lax.rsqrt(slot_squares / model_width + EPSILON)[:, None]

    blocks = [b0, r1, r2, r3, l1, l2, l3]
    weights = (gu_own, gu_oth, down_own, down_oth)
    own, oth, back, xs = pl.pallas_call(
        lambda *r: project_body(*r, n=n_z),
        out_shape=(
            jax.ShapeDtypeStruct((rows, 2 * hid), F4),
            jax.ShapeDtypeStruct((rows, 2 * hid), F4),
            jax.ShapeDtypeStruct((rows, 2 * hid), F4),
            jax.ShapeDtypeStruct(((n_z - 1) * rows, wide), BF),
        ),
        in_specs=[SMEM] + [ANY] * (n_z - 1 + 4) + [VMEM] * 2,
        out_specs=(VMEM,) * 4,
        scratch_shapes=[
            pltpu.VMEM((n_z - 1, 2 * rows, wide), BF),
            pltpu.VMEM(gu_own.shape, BF),
            pltpu.VMEM(gu_own.shape, BF),
            pltpu.VMEM(down_own.shape, BF),
            pltpu.VMEM(down_own.shape, BF),
            pltpu.SemaphoreType.DMA((n_z + 3,)),
        ],
        compiler_params=BIG,
        name="project",
    )(zs, *blocks, *weights, gains, slot_inverse)

    x4, b_own, b_oth, a_own, a_oth, along, ra, la = pl.pallas_call(
        lambda *r: finish_body(*r, n=n_z),
        out_shape=(
            jax.ShapeDtypeStruct((rows, wide), BF),
            jax.ShapeDtypeStruct((rows, 2 * hid), BF),
            jax.ShapeDtypeStruct((rows, 2 * hid), BF),
            jax.ShapeDtypeStruct((rows, hid), BF),
            jax.ShapeDtypeStruct((rows, hid), BF),
            jax.ShapeDtypeStruct((8, wide), F4),
            jax.ShapeDtypeStruct((rows // 2 + 16, wide), BF),
            jax.ShapeDtypeStruct((rows // 2, wide), BF),
        ),
        in_specs=[SMEM] + [VMEM] * 2 + [ANY] * 4 + [VMEM] * 5,
        out_specs=(VMEM,) * 8,
        scratch_shapes=[
            pltpu.VMEM((wide, 2 * hid), BF),
            pltpu.VMEM((wide, 2 * hid), BF),
            pltpu.VMEM((hid, wide), BF),
            pltpu.VMEM((hid, wide), BF),
            pltpu.SemaphoreType.DMA((4,)),
        ],
        compiler_params=BIG,
        name="finish",
    )(zs, xf, cf, *weights, gains, slot_inverse, own, oth, back)

    ra, la = right(ra), left(la)
    parts = pl.pallas_call(
        parts_body,
        grid=(n_z,),
        out_shape=jax.ShapeDtypeStruct((rows, model_width), BF),
        in_specs=[
            pl.BlockSpec((rows, 2 * hid), lambda i: (0, 0)),
            pl.BlockSpec((rows, 2 * hid), lambda i: (0, 0)),
            pl.BlockSpec((wide, 2 * hid), lambda i: (i, 0)),
            pl.BlockSpec((wide, 2 * hid), lambda i: (i, 0)),
        ],
        out_specs=pl.BlockSpec((rows, wide), lambda i: (0, i)),
        name="parts",
    )(b_own, b_oth, gu_own, gu_oth)
    message = jax.ShapeDtypeStruct((rows + 16, wide), BF)
    for k in range(half - 1, 0, -1):
        ra, la = pl.pallas_call(
            lambda *r, k=k: hop_body(*r, k=k, n=n_z, first=k == half - 1),
            out_shape=(message, message),
            in_specs=[SMEM] + [VMEM] * 4,
            out_specs=(VMEM, VMEM),
            compiler_params=BIG,
            name="hop",
        )(zs, parts, along, ra, la)
        ra, la = right(ra), left(la)
    sent_back = pl.pallas_call(
        lambda *r: pack_body(*r, n_sp=n_sp),
        out_shape=jax.ShapeDtypeStruct((slot_count, width_part + 128), BF),
        in_specs=[SMEM] + [VMEM] * 4,
        out_specs=VMEM,
        compiler_params=BIG,
        name="pack",
    )(zs, parts, along, ra, la)
    returned = lax.all_to_all(
        sent_back.reshape(2 * n_sp, half_cap, width_part + 128), ("sp", "c"), 0, 0, tiled=True
    ).reshape(slot_count, width_part + 128)

    others = grads(zs, xs, x4, blocks, cf, b_oth, a_oth, None)
    returned, others = lax.optimization_barrier((returned, others))
    grad_gate, grad_up, grad_down = grads(
        zs, xs, x4, blocks, cf, b_own, a_own, swap(others)
    )

    token_back = dot(picker, returned, 0, 0)
    inner = jnp.sum(token_back[:, width_part : width_part + 3], axis=1, keepdims=True)
    gained = norm_gain[None, :] * token_back[:, :width_part]
    norm_back = inverse * gained - residual * inverse**2 * (inner / model_width)
    stream_grad = (upstream.astype(F4) + norm_back).astype(BF)

    ht = tok_rows // 2
    p1, m1, p2, m2 = (hops(stream_grad, d) for d in (1, -1, 2, -2))
    p3, m3 = hops(p1, 2), hops(m1, -2)
    pf, mf = hops(p2[:ht], 2), hops(m2[ht:], -2)
    mine8 = pl.pallas_call(
        stack_body,
        out_shape=jax.ShapeDtypeStruct((n_z, tok_rows, width_part), BF),
        in_specs=[ANY] * 9,
        out_specs=ANY,
        scratch_shapes=[pltpu.SemaphoreType.DMA((9,))],
        name="stack",
    )(stream_grad, m1, m2, m3, pf, mf, p3, p2, p1)
    other8 = swap(mine8)

    mean_val = (conv_total / channels)[:, None]
    variance = (conv_squares / channels)[:, None] - mean_val * mean_val
    inv_std = lax.rsqrt(variance + EPSILON)
    centred = (conv_vals - mean_val) * inv_std
    scaled = centred * ln_gain[None, :]
    mixed_out = jax.nn.silu(scaled).astype(BF)

    zc = jnp.stack([z, core]).astype(jnp.int32)
    slope = silu_slope(scaled) * ln_gain[None, :]
    norm_in = pl.pallas_call(
        lambda *r: mixed_body(*r, n=n_z),
        out_shape=jax.ShapeDtypeStruct(conv_pre.shape, F4),
        in_specs=[SMEM] + [VMEM] * 4 + [ANY],
        out_specs=VMEM,
        compiler_params=BIG,
        name="mixed",
    )(zc, mine8, other8, w_out, slope, grad_gate)
    out_parts = pl.pallas_call(
        lambda *r: outer_body(*r, n=n_z),
        out_shape=jax.ShapeDtypeStruct((n_sp, conv_pre.shape[1], width_part), BF),
        in_specs=[SMEM] + [VMEM] * 3,
        out_specs=VMEM,
        compiler_params=BIG,
        name="outer",
    )(zc, mine8, other8, mixed_out.T)
    norm_total, norm_cross = in_one((jnp.sum(norm_in, axis=1), jnp.sum(norm_in * centred, axis=1)))
    conv_back = inv_std * (
        norm_in - (norm_total / channels)[:, None] - centred * (norm_cross / channels)[:, None]
    )
    next_rim = lax.ppermute(conv_back[:32], "sp", [(i + 1, i) for i in range(n_sp - 1)])
    grad_out = jnp.sum(
        lax.all_to_all(out_parts, "sp", 0, 0, tiled=True).astype(F4), axis=0
    )
    value_grad, gate_grad = pl.pallas_call(
        conv_body,
        out_shape=(jax.ShapeDtypeStruct(value_in.shape, BF),) * 2,
        in_specs=[VMEM] * 5,
        out_specs=(VMEM, VMEM),
        scratch_shapes=[pltpu.VMEM((tok_rows + 32, conv_pre.shape[1]), F4)],
        name="conv",
    )(conv_back, next_rim, conv_taps, value_in, gate_in)
    return (grad_gate[None], grad_up[None], grad_down[None], grad_out, value_grad, gate_grad)


def solution(mesh):
    n_sp, n_tp = mesh.devices.shape
    split = Mesh(mesh.devices.reshape(n_sp, n_tp // 2, 2), ("sp", "z", "c"))
    return jax.shard_map(
        per_device,
        mesh=split,
        in_specs=(
            P("sp", TP),
            P("sp", TP),
            P(TP),
            P("sp", None),
            P("sp", None),
            P("sp", None, TP),
            P("sp", None, TP),
            P("sp", TP, None),
            P("sp", TP),
            P("sp", TP),
            P("sp", TP),
            P(TP),
            P(None, TP),
            P(TP, None),
        ),
        out_specs=(
            P("sp", None, TP),
            P("sp", None, TP),
            P("sp", TP, None),
            P(TP, "sp"),
            P("sp", TP),
            P("sp", TP),
        ),
        check_vma=False,
    )
```

```python
import jax
import jax.numpy as jnp
from jax import lax
from jax.experimental import pallas as pl
from jax.experimental.pallas import tpu as pltpu
from jax.sharding import Mesh, PartitionSpec as P

EPSILON = 1e-06
TP = ("z", "c")
BF = jnp.bfloat16
F4 = jnp.float32


def of_everyone(value):
    count = 16
    everything = lax.all_to_all(
        jnp.broadcast_to(value[None], (count, *value.shape)), TP, 0, 0, tiled=True
    )
    return jnp.sum(everything, axis=0)


def in_one(arrays):
    total = of_everyone(jnp.concatenate([a.reshape(-1) for a in arrays]))
    out, at = [], 0
    for a in arrays:
        out.append(total[at : at + a.size].reshape(a.shape))
        at += a.size
    return out


def right(x):
    n = lax.axis_size("z")
    return lax.ppermute(x, "z", [(i, (i + 1) % n) for i in range(n)])


def left(x):
    n = lax.axis_size("z")
    return lax.ppermute(x, "z", [(i, (i - 1) % n) for i in range(n)])


def hops(x, n_hops):
    n = lax.axis_size("z")
    return lax.ppermute(x, "z", [(i, (i + n_hops) % n) for i in range(n)])


def swap(x):
    return lax.ppermute(x, "c", [(0, 1), (1, 0)])


def silu_slope(values):
    logistic = jax.nn.sigmoid(values)
    return logistic * (1.0 + values * (1.0 - logistic))


def dot(a, b, ca, cb):
    return lax.dot_general(a, b, (((ca,), (cb,)), ((), ())), preferred_element_type=F4)


VMEM = pl.BlockSpec(memory_space=pltpu.VMEM)
ANY = pl.BlockSpec(memory_space=pl.ANY)
SMEM = pl.BlockSpec(memory_space=pltpu.SMEM)
BIG = pltpu.CompilerParams(vmem_limit_bytes=40 * 2**20)


def scatter_body(
    routes_h, weights_h, upstream_h, stream_h, picker, sent, *scratch, experts, capacity
):
    routes, weights, upstream, stream, sems = scratch
    load_all(
        [(routes_h, routes), (weights_h, weights), (upstream_h, upstream), (stream_h, stream)],
        sems,
    )
    toks = upstream.shape[0]
    slots = experts * capacity
    half = capacity // 2
    r0, r1 = routes[0:1, :], routes[1:2, :]
    names = lax.broadcasted_iota(jnp.int32, (experts, toks), 0)
    hot0 = jnp.where(names == r0, 1.0, 0.0)
    hot1 = jnp.where(names == r1, 1.0, 0.0)
    earlier = jnp.where(
        lax.broadcasted_iota(jnp.int32, (toks, toks), 0)
        < lax.broadcasted_iota(jnp.int32, (toks, toks), 1),
        1.0,
        0.0,
    ).astype(BF)
    before = dot((hot0 + hot1).astype(BF), earlier, 1, 0)
    slot0 = r0 * capacity + jnp.sum(before * hot0, axis=0, keepdims=True).astype(jnp.int32)
    slot1 = r1 * capacity + jnp.sum(before * hot1, axis=0, keepdims=True).astype(jnp.int32)
    blocks = 8
    step = blocks * capacity

    def rows_at(j, carry):
        at = j * (step // 2)
        ids = lax.broadcasted_iota(jnp.int32, (step // 2, toks), 0) + at
        one = jnp.where(ids == slot0, 1.0, 0.0) + jnp.where(ids == slot1, 1.0, 0.0)
        picker[pl.ds(pl.multiple_of(at, step // 2), step // 2), :] = one.astype(BF)
        wide = lax.broadcasted_iota(jnp.int32, (step, toks), 0)
        block = lax.shift_right_logical(wide * (65536 // capacity + 1), 16)
        place = wide - block * capacity
        ids = jnp.where(place >= half, place - half, place) + (block + j * blocks) * half
        hit0, hit1 = ids == slot0, ids == slot1
        pick = (jnp.where(hit0, 1.0, 0.0) + jnp.where(hit1, 1.0, 0.0)).astype(BF)
        weight = jnp.sum(
            jnp.where(hit0, weights[0:1, :], 0.0) + jnp.where(hit1, weights[1:2, :], 0.0),
            axis=1,
            keepdims=True,
        )
        is_cot = place[:, 0:1] >= half
        value = jnp.where(
            is_cot, dot(pick, upstream[...], 1, 0) * weight, dot(pick, stream[...], 1, 0)
        )
        sent[pl.ds(pl.multiple_of(j * step, step), step), :] = value.astype(BF)
        return carry

    lax.fori_loop(0, 2 * slots // step, rows_at, 0)


def offset_of(k, offsets, n):
    off = jnp.int32(0)
    for i, value in enumerate(offsets):
        off = jnp.where(k == i, value % n, off)
    return off


def load_all(pairs, sems):
    copies = [pltpu.make_async_copy(a, b, sems.at[i]) for i, (a, b) in enumerate(pairs)]
    for copy in copies:
        copy.start()
    for copy in copies:
        copy.wait()


def project_body(z, *refs, offsets, n, more):
    m = len(offsets)
    blocks, refs = refs[:m], refs[m:]
    guo, gux, dno, dnx, gains, inv = refs[:6]
    refs = refs[6:]
    if more:
        starts, refs = refs[:3], refs[3:]
    sums, xs = refs[:3], refs[3]
    own, oth, back = sums
    buf, xs_v, guo_v, gux_v, dno_v, dnx_v, sems = refs[4:]
    rows, width = own.shape[0], buf.shape[2]
    hid = dno.shape[0]
    pairs = [(blocks[i], buf.at[i]) for i in range(m)]
    if more:
        for i, off in enumerate(offsets):
            at = pl.multiple_of(lax.rem(z[0] + off % n, n) * width, width)
            mine = pl.ds(i * width, width)
            pairs += [
                (guo.at[pl.ds(at, width), :], guo_v.at[mine, :]),
                (gux.at[pl.ds(at, width), :], gux_v.at[mine, :]),
                (dno.at[:, pl.ds(at, width)], dno_v.at[:, mine]),
                (dnx.at[:, pl.ds(at, width)], dnx_v.at[:, mine]),
            ]
    else:
        pairs += [(guo, guo_v), (gux, gux_v), (dno, dno_v), (dnx, dnx_v)]
    load_all(pairs, sems)
    for i, total in enumerate(sums):
        total[...] = starts[i][...] if more else jnp.zeros(total.shape, F4)

    def step(k, carry):
        chip = lax.rem(z[0] + offset_of(k, offsets, n), n)
        at = pl.multiple_of((k if more else chip) * width, width)
        x = buf[k, :rows, :].astype(F4)
        x = (gains[pl.ds(chip, 1), :] * x * inv[...]).astype(BF)
        xs_v[pl.ds(pl.multiple_of(k * rows, rows), rows), :] = x
        own[...] += dot(x, guo_v[pl.ds(at, width), :], 1, 0)
        oth[...] += dot(x, gux_v[pl.ds(at, width), :], 1, 0)
        c = buf[k, rows:, :]
        back[:, :hid] += dot(c, dno_v[:, pl.ds(at, width)], 1, 1)
        back[:, hid:] += dot(c, dnx_v[:, pl.ds(at, width)], 1, 1)
        return carry

    lax.fori_loop(0, m, step, 0)
    load_all([(xs_v, xs)], sems)


def project(z, blocks, weights, gains, inv, offsets, n, starts):
    rows2, wide = blocks[0].shape
    rows, m = rows2 // 2, len(blocks)
    hid = weights[2].shape[0]
    more = starts is not None
    cols = m * wide if more else n * wide
    total = jax.ShapeDtypeStruct((rows, 2 * hid), F4)
    return pl.pallas_call(
        lambda *r: project_body(*r, offsets=offsets, n=n, more=more),
        out_shape=(total, total, total, jax.ShapeDtypeStruct((m * rows, wide), BF)),
        in_specs=[SMEM] + [ANY] * (m + 4) + [VMEM] * (5 if more else 2),
        out_specs=(VMEM, VMEM, VMEM, ANY),
        scratch_shapes=[
            pltpu.VMEM((m, rows2, wide), BF),
            pltpu.VMEM((m * rows, wide), BF),
            pltpu.VMEM((cols, 2 * hid), BF),
            pltpu.VMEM((cols, 2 * hid), BF),
            pltpu.VMEM((hid, cols), BF),
            pltpu.VMEM((hid, cols), BF),
            pltpu.SemaphoreType.DMA((5 * m + 4,)),
        ],
        compiler_params=BIG,
        name="project",
    )(z, *blocks, *weights, gains, inv, *(starts or ()))


def in_parts(row):
    hi = row.astype(BF).astype(F4)
    mid = (row - hi).astype(BF).astype(F4)
    low = (row - hi - mid).astype(BF).astype(F4)
    return hi, mid, low


def part_rows(row):
    hi, mid, low = in_parts(row)
    shape = (16, row.shape[1])
    at = lax.broadcasted_iota(jnp.int32, shape, 0)
    rows = jnp.where(at == 0, hi, jnp.where(at == 1, mid, jnp.where(at == 2, low, 0.0)))
    return rows.astype(BF)


def whole_row(rows):
    rows = rows.astype(F4)
    return rows[0:1] + rows[1:2] + rows[2:3]


def finish_body(z, xf, cf, guo, gux, dno, dnx, gains, inv, own, oth, back, *refs, n):
    hbm, refs = refs[:5], refs[5:]
    along, send_r, send_l = refs[:3]
    held = refs[3:8]
    x4, b_own, b_oth, a_own, a_oth = held
    guo_v, gux_v, dno_v, dnx_v, sems = refs[8:]
    rows, width = xf.shape
    hid = dno.shape[0]
    chip = lax.rem(z[0] + n // 2, n)
    at = pl.multiple_of(chip * width, width)
    load_all(
        [
            (guo.at[pl.ds(at, width), :], guo_v),
            (gux.at[pl.ds(at, width), :], gux_v),
            (dno.at[:, pl.ds(at, width)], dno_v),
            (dnx.at[:, pl.ds(at, width)], dnx_v),
        ],
        sems,
    )
    x = (gains[pl.ds(chip, 1), :] * xf[...].astype(F4) * inv[...]).astype(BF)
    x4[...] = x
    total = jnp.zeros((rows, 1), F4)
    for pre, gu_v, dn_v, lo, backs, act in (
        (own, guo_v, dno_v, 0, b_own, a_own),
        (oth, gux_v, dnx_v, hid, b_oth, a_oth),
    ):
        both = pre[...] + dot(x, gu_v[...], 1, 0)
        gate, upper = both[:, :hid], both[:, hid:]
        ab = back[:, lo : lo + hid] + dot(cf[...], dn_v[...], 1, 1)
        sig = jax.nn.sigmoid(gate)
        silu = gate * sig
        act[...] = (silu * upper).astype(BF)
        gb = (ab * upper * (sig * (1.0 + gate * (1.0 - sig)))).astype(BF)
        ub = (ab * silu).astype(BF)
        backs[:, :hid] = gb
        backs[:, hid:] = ub
        total = total + jnp.sum(
            gb.astype(F4) * gate + ub.astype(F4) * upper, axis=1, keepdims=True
        )
    copies = [
        pltpu.make_async_copy(a, b, sems.at[i]) for i, (a, b) in enumerate(zip(held, hbm))
    ]
    for copy in copies:
        copy.start()
    row = jnp.broadcast_to(total, (rows, 128)).T[0:8, :]
    along[:, :rows] = row
    along[:, rows:] = jnp.zeros((8, width - rows), F4)
    part = dot(b_own[...], guo_v[...], 1, 1) + dot(b_oth[...], gux_v[...], 1, 1)
    hr = rows // 2
    send_r[:hr, :] = part[:hr].astype(BF)
    send_r[hr:, :] = part_rows(along[0:1, :])
    send_l[...] = part[hr:].astype(BF)
    for copy in copies:
        copy.wait()


def parts_body(b_own, b_oth, guo, gux, out, guo_v, gux_v, sems, *, n):
    width = guo.shape[0] // n
    pairs = []
    for k in range(n):
        at = pl.ds(k * width, width)
        pairs.append((guo.at[at, :], guo_v.at[at, :]))
        pairs.append((gux.at[at, :], gux_v.at[at, :]))
    copies = [pltpu.make_async_copy(a, b, sems.at[i]) for i, (a, b) in enumerate(pairs)]
    for copy in copies:
        copy.start()
    for k in range(n):
        copies[2 * k].wait()
        copies[2 * k + 1].wait()
        at = pl.ds(k * width, width)
        out[:, at] = (
            dot(b_own[...], guo_v[at, :], 1, 1) + dot(b_oth[...], gux_v[at, :], 1, 1)
        ).astype(BF)


def hop_body(z, parts, along, ra, la, out_r, out_l, *, k, n, first):
    rows = parts.shape[0]
    width = out_r.shape[1]
    hr = rows // 2

    def block(j):
        at = pl.multiple_of(lax.rem(z[0] + (j + n), n) * width, width)
        return parts[:, pl.ds(at, width)].astype(F4)

    own = along[0:1, :]
    pr, pl_ = block(k), block(-k)
    if first:
        out_r[:hr, :] = (pr[:hr] + ra[:hr, :].astype(F4)).astype(BF)
        out_r[hr:rows, :] = pr[hr:].astype(BF)
        out_r[rows:, :] = part_rows(own + whole_row(ra[hr:, :]))
        out_l[:hr, :] = pl_[:hr].astype(BF)
        out_l[hr:rows, :] = (pl_[hr:] + la[...].astype(F4)).astype(BF)
        out_l[rows:, :] = part_rows(own)
    else:
        out_r[:rows, :] = (pr + ra[:rows, :].astype(F4)).astype(BF)
        out_r[rows:, :] = part_rows(own + whole_row(ra[rows:, :]))
        out_l[:rows, :] = (pl_ + la[:rows, :].astype(F4)).astype(BF)
        out_l[rows:, :] = part_rows(own + whole_row(la[rows:, :]))


def pack_body(z, parts, along, ra, la, out, *, n_sp):
    rows = parts.shape[0]
    width = ra.shape[1]
    half = width // 2
    step = rows // n_sp
    at = pl.multiple_of(z[0] * width, width)
    row = along[0:1, :] + whole_row(ra[rows:, :]) + whole_row(la[rows:, :])
    col = jnp.broadcast_to(row[:, :rows], (128, rows)).T
    hi, mid, low = in_parts(col)
    lane = lax.broadcasted_iota(jnp.int32, (rows, 128), 1)
    extra = jnp.where(lane == 0, hi, jnp.where(lane == 1, mid, jnp.where(lane == 2, low, 0.0)))
    value = (
        parts[:, pl.ds(at, width)].astype(F4) + ra[:rows, :].astype(F4) + la[:rows, :].astype(F4)
    )
    for s in range(n_sp):
        v = value[s * step : (s + 1) * step]
        e = extra[s * step : (s + 1) * step]
        both = jnp.concatenate([v[:, :half], v[:, half:]], axis=0)
        out[2 * s * step : 2 * (s + 1) * step, :half] = both.astype(BF)
        out[2 * s * step : 2 * (s + 1) * step, half:] = jnp.concatenate([e, e], axis=0).astype(BF)


def grads_body(z, *refs, n, add, offsets):
    xs1, xs2, x4 = refs[:3]
    blocks, cf = refs[3 : n + 2], refs[n + 2]
    backs, act = refs[n + 3], refs[n + 4]
    refs = refs[n + 5 :]
    if add:
        old, gate, up, down, xbuf, cbuf, sems = refs
    else:
        out, xbuf, cbuf, sems = refs
    rows, width = x4.shape
    hid = act.shape[1]
    near = (n - 1) * rows
    first = xs1.shape[0]
    load_all(
        [
            (xs1, xbuf.at[pl.ds(0, first), :]),
            (xs2, xbuf.at[pl.ds(first, near - first), :]),
            (x4, xbuf.at[pl.ds(near, rows), :]),
        ]
        + [
            (blocks[i].at[pl.ds(rows, rows), :], cbuf.at[pl.ds(i * rows, rows), :])
            for i in range(n - 1)
        ]
        + [(cf, cbuf.at[pl.ds(near, rows), :])],
        sems,
    )

    def step(k, carry):
        at = pl.multiple_of(lax.rem(z[0] + offset_of(k, offsets, n), n) * width, width)
        mine = pl.ds(pl.multiple_of(k * rows, rows), rows)
        pair = dot(xbuf[mine, :], backs[...], 0, 0)
        dn = dot(act[...], cbuf[mine, :], 0, 0)
        if add:
            gate[pl.ds(at, width), :] = pair[:, :hid] + old[0, pl.ds(at, width), :].astype(F4)
            up[pl.ds(at, width), :] = pair[:, hid:] + old[1, pl.ds(at, width), :].astype(F4)
            for q in range(width // hid):
                lo = pl.multiple_of(at + q * hid, hid)
                down[:, pl.ds(lo, hid)] = dn[:, q * hid : (q + 1) * hid] + old[
                    2, pl.ds(lo, hid), :
                ].astype(F4)
        else:
            out[0, pl.ds(at, width), :] = pair[:, :hid].astype(BF)
            out[1, pl.ds(at, width), :] = pair[:, hid:].astype(BF)
            for q in range(width // hid):
                lo = pl.multiple_of(at + q * hid, hid)
                out[2, pl.ds(lo, hid), :] = dn[:, q * hid : (q + 1) * hid].astype(BF)
        return carry

    lax.fori_loop(0, n, step, 0)


def grads(z, xs, x4, blocks, cf, backs, act, old, offsets):
    rows, width = x4.shape
    n, hid = len(blocks) + 1, act.shape[1]
    add = old is not None
    total = n * width
    args = [z, *xs, x4, *blocks, cf, backs, act] + ([old] if add else [])
    if add:
        out_shape = tuple(
            jax.ShapeDtypeStruct(t, F4) for t in ((total, hid), (total, hid), (hid, total))
        )
        out_specs = (VMEM,) * 3
    else:
        out_shape, out_specs = jax.ShapeDtypeStruct((3, total, hid), BF), VMEM
    return pl.pallas_call(
        lambda *r: grads_body(*r, n=n, add=add, offsets=offsets),
        out_shape=out_shape,
        in_specs=[SMEM] + [ANY] * (n + 3) + [VMEM] * (3 if add else 2),
        out_specs=out_specs,
        scratch_shapes=[
            pltpu.VMEM((n * rows, width), BF),
            pltpu.VMEM((n * rows, width), BF),
            pltpu.SemaphoreType.DMA((n + 3,)),
        ],
        compiler_params=BIG,
        cost_estimate=pl.CostEstimate(
            flops=8 * rows * total * 3 * hid, transcendentals=0, bytes_accessed=16 * 2**20
        ),
        name="grads_own" if add else "grads_other",
    )(*args)


def stack_body(*refs):
    out, at = refs[-1], 0
    for src in refs[:-1]:
        out[pl.ds(at, src.shape[0]), :] = src[...]
        at += src.shape[0]


def mixed_body(zc, mine, other, w_out, slope, out, *, n):
    width = mine.shape[2]
    out[...] = jnp.zeros(out.shape, F4)
    for ref, core in ((mine, zc[1]), (other, 1 - zc[1])):
        acc = jnp.zeros(out.shape, F4)
        for k in range(n):
            at = pl.multiple_of((2 * lax.rem(zc[0] + k, n) + core) * width, width)
            acc = acc + dot(ref[k], w_out[:, pl.ds(at, width)], 1, 1)
        out[...] += acc
    out[...] *= slope[...]


def outer_body(zc, mine, other, mixed_t, out, *, n):
    for ref, core in ((mine, zc[1]), (other, 1 - zc[1])):
        for k in range(n):
            out[2 * lax.rem(zc[0] + k, n) + core] = dot(mixed_t[...], ref[k], 1, 0).astype(BF)


def conv_body(back, rim, taps, value_in, gate_in, value_grad, gate_grad, padded):
    toks, n_taps = back.shape[0], taps.shape[0]
    padded[:toks, :] = back[...]
    padded[toks:, :] = rim[...]
    step = 64
    for at in range(0, toks, step):
        acc = jnp.zeros((step, back.shape[1]), F4)
        for tap in range(n_taps):
            lo = at + n_taps - 1 - tap
            acc = acc + taps[tap : tap + 1, :] * padded[lo : lo + step, :]
        sigma = jax.nn.sigmoid(gate_in[at : at + step, :].astype(F4))
        value = acc * sigma
        value_grad[at : at + step, :] = value.astype(BF)
        gate_grad[at : at + step, :] = (
            value * value_in[at : at + step, :].astype(F4) * (1.0 - sigma)
        ).astype(BF)


def per_device(
    upstream,
    stream,
    norm_gain,
    routes,
    route_weights,
    w_gate,
    w_up,
    w_down,
    value_in,
    gate_in,
    conv_pre,
    ln_gain,
    conv_taps,
    w_out,
):
    tok_rows, width_part = stream.shape
    n_sp = lax.axis_size("sp")
    n_z = lax.axis_size("z")
    n_tp = 2 * n_z
    z = lax.axis_index("z")
    core = lax.axis_index("c")
    model_width = width_part * n_tp
    channels = conv_pre.shape[1] * n_tp
    tap_count = conv_taps.shape[0]
    capacity = 3 * tok_rows // n_sp
    half_cap = capacity // 2
    experts = n_sp
    slot_count = experts * capacity
    rows = n_sp * half_cap
    wide = 2 * width_part

    zs = z.astype(jnp.int32).reshape(1)
    half = n_z // 2
    hid = w_gate.shape[2]

    picker, sent = pl.pallas_call(
        lambda *r: scatter_body(*r, experts=experts, capacity=capacity),
        out_shape=(
            jax.ShapeDtypeStruct((slot_count, tok_rows), BF),
            jax.ShapeDtypeStruct((2 * slot_count, width_part), BF),
        ),
        in_specs=[ANY] * 4,
        out_specs=(VMEM, VMEM),
        scratch_shapes=[
            pltpu.VMEM((2, tok_rows), jnp.int32),
            pltpu.VMEM((2, tok_rows), F4),
            pltpu.VMEM(upstream.shape, BF),
            pltpu.VMEM(stream.shape, BF),
            pltpu.SemaphoreType.DMA((4,)),
        ],
        compiler_params=BIG,
        name="scatter",
    )(routes.T, route_weights.T, upstream, stream)
    arrived = lax.all_to_all(
        sent.reshape(2 * experts, capacity, width_part), ("sp", "c"), 0, 0, tiled=True
    )
    arrived = arrived.reshape(n_sp, 2, 2, half_cap, width_part)
    b0 = jnp.transpose(arrived, (2, 0, 3, 1, 4)).reshape(2 * rows, wide)

    gu_own = jnp.concatenate([w_gate[0], w_up[0]], axis=1)
    down_own = w_down[0]
    gu_oth, down_oth = swap(gu_own), swap(down_own)

    residual = stream.astype(F4)
    conv_vals = conv_pre.astype(F4)
    own_rows = b0[:rows].astype(F4)
    row_part = jnp.sum(own_rows * own_rows, axis=1)
    nothing = jnp.zeros_like(row_part)
    vector = jnp.concatenate(
        [
            jnp.sum(residual * residual, axis=1),
            jnp.sum(conv_vals, axis=1),
            jnp.sum(conv_vals * conv_vals, axis=1),
            jnp.where(core == 0, row_part, nothing),
            jnp.where(core == 0, nothing, row_part),
            norm_gain,
        ]
    )
    told = lax.all_to_all(
        jnp.broadcast_to(vector[None, None], (n_tp, 1, vector.size)), TP, 0, 0, tiled=True
    )[:, 0]
    cut = 3 * tok_rows + 2 * rows
    total = jnp.sum(told[:, :cut], axis=0)
    gains = told[:, cut:].reshape(n_z, wide)
    row_squares, conv_total, conv_squares = jnp.split(total[: 3 * tok_rows], 3)
    slot_squares = jnp.where(
        core == 0, total[3 * tok_rows : 3 * tok_rows + rows], total[3 * tok_rows + rows :]
    )
    inverse = lax.rsqrt(row_squares / model_width + EPSILON)[:, None]
    slot_inverse = lax.rsqrt(slot_squares / model_width + EPSILON)[:, None]

    weights = (gu_own, gu_oth, down_own, down_oth)
    r1, l1 = right(b0), left(b0)
    r2, l2 = right(r1), left(l1)
    r2, l2, gains, slot_inverse = lax.optimization_barrier((r2, l2, gains, slot_inverse))
    r3, l3 = right(r2), left(l2)
    offsets = (0, -1, -2, 1, 2, -3, 3, 4)
    *sums, xs1 = project(
        zs, [b0, r1, r2, l1, l2], weights, gains, slot_inverse, offsets[:5], n_z, None
    )
    r3, l3, sums, xs1 = lax.optimization_barrier((r3, l3, sums, xs1))
    xf, cf = right(r3[:rows]), left(l3[rows:])
    own, oth, back, xs2 = project(
        zs, [r3, l3], weights, gains, slot_inverse, offsets[5:7], n_z, sums
    )
    blocks = [b0, r1, r2, l1, l2, r3, l3]

    x4, b_own, b_oth, a_own, a_oth, along, ra, la = pl.pallas_call(
        lambda *r: finish_body(*r, n=n_z),
        out_shape=(
            jax.ShapeDtypeStruct((rows, wide), BF),
            jax.ShapeDtypeStruct((rows, 2 * hid), BF),
            jax.ShapeDtypeStruct((rows, 2 * hid), BF),
            jax.ShapeDtypeStruct((rows, hid), BF),
            jax.ShapeDtypeStruct((rows, hid), BF),
            jax.ShapeDtypeStruct((8, wide), F4),
            jax.ShapeDtypeStruct((rows // 2 + 16, wide), BF),
            jax.ShapeDtypeStruct((rows // 2, wide), BF),
        ),
        in_specs=[SMEM] + [VMEM] * 2 + [ANY] * 4 + [VMEM] * 5,
        out_specs=(ANY,) * 5 + (VMEM,) * 3,
        scratch_shapes=[
            pltpu.VMEM((rows, wide), BF),
            pltpu.VMEM((rows, 2 * hid), BF),
            pltpu.VMEM((rows, 2 * hid), BF),
            pltpu.VMEM((rows, hid), BF),
            pltpu.VMEM((rows, hid), BF),
            pltpu.VMEM((wide, 2 * hid), BF),
            pltpu.VMEM((wide, 2 * hid), BF),
            pltpu.VMEM((hid, wide), BF),
            pltpu.VMEM((hid, wide), BF),
            pltpu.SemaphoreType.DMA((5,)),
        ],
        compiler_params=BIG,
        name="finish",
    )(zs, xf, cf, *weights, gains, slot_inverse, own, oth, back)

    ra, la = right(ra), left(la)
    parts = pl.pallas_call(
        lambda *r: parts_body(*r, n=n_z),
        out_shape=jax.ShapeDtypeStruct((rows, model_width), BF),
        in_specs=[VMEM] * 2 + [ANY] * 2,
        out_specs=VMEM,
        scratch_shapes=[
            pltpu.VMEM(gu_own.shape, BF),
            pltpu.VMEM(gu_own.shape, BF),
            pltpu.SemaphoreType.DMA((2 * n_z,)),
        ],
        compiler_params=BIG,
        name="parts",
    )(b_own, b_oth, gu_own, gu_oth)
    message = jax.ShapeDtypeStruct((rows + 16, wide), BF)
    for k in range(half - 1, 0, -1):
        ra, la = pl.pallas_call(
            lambda *r, k=k: hop_body(*r, k=k, n=n_z, first=k == half - 1),
            out_shape=(message, message),
            in_specs=[SMEM] + [VMEM] * 4,
            out_specs=(VMEM, VMEM),
            compiler_params=BIG,
            name="hop",
        )(zs, parts, along, ra, la)
        ra, la = right(ra), left(la)
        if k == 2:
            others = grads(zs, (xs1, xs2), x4, blocks, cf, b_oth, a_oth, None, offsets)
            ra, la, others = lax.optimization_barrier((ra, la, others))
            others = swap(others)
    sent_back = pl.pallas_call(
        lambda *r: pack_body(*r, n_sp=n_sp),
        out_shape=jax.ShapeDtypeStruct((slot_count, width_part + 128), BF),
        in_specs=[SMEM] + [VMEM] * 4,
        out_specs=VMEM,
        compiler_params=BIG,
        name="pack",
    )(zs, parts, along, ra, la)
    returned = lax.all_to_all(
        sent_back.reshape(2 * n_sp, half_cap, width_part + 128), ("sp", "c"), 0, 0, tiled=True
    ).reshape(slot_count, width_part + 128)

    grad_gate, grad_up, grad_down = grads(
        zs, (xs1, xs2), x4, blocks, cf, b_own, a_own, others, offsets
    )
    returned, grad_gate, grad_up, grad_down = lax.optimization_barrier(
        (returned, grad_gate, grad_up, grad_down)
    )

    token_back = dot(picker, returned, 0, 0)
    inner = jnp.sum(token_back[:, width_part : width_part + 3], axis=1, keepdims=True)
    gained = norm_gain[None, :] * token_back[:, :width_part]
    norm_back = inverse * gained - residual * inverse**2 * (inner / model_width)
    stream_grad = (upstream.astype(F4) + norm_back).astype(BF)

    ht = tok_rows // 2
    p1, m1, p2, m2 = (hops(stream_grad, d) for d in (1, -1, 2, -2))
    p3, m3 = hops(p1, 2), hops(m1, -2)
    pf, mf = hops(p2[:ht], 2), hops(m2[ht:], -2)
    mine8 = pl.pallas_call(
        stack_body,
        out_shape=jax.ShapeDtypeStruct((n_z * tok_rows, width_part), BF),
        in_specs=[VMEM] * 9,
        out_specs=VMEM,
        compiler_params=BIG,
        name="stack",
    )(stream_grad, m1, m2, m3, pf, mf, p3, p2, p1).reshape(n_z, tok_rows, width_part)
    other8 = swap(mine8)

    mean_val = (conv_total / channels)[:, None]
    variance = (conv_squares / channels)[:, None] - mean_val * mean_val
    inv_std = lax.rsqrt(variance + EPSILON)
    centred = (conv_vals - mean_val) * inv_std
    scaled = centred * ln_gain[None, :]
    mixed_out = jax.nn.silu(scaled).astype(BF)

    zc = jnp.stack([z, core]).astype(jnp.int32)
    slope = silu_slope(scaled) * ln_gain[None, :]
    norm_in = pl.pallas_call(
        lambda *r: mixed_body(*r, n=n_z),
        out_shape=jax.ShapeDtypeStruct(conv_pre.shape, F4),
        in_specs=[SMEM] + [VMEM] * 4,
        out_specs=VMEM,
        compiler_params=BIG,
        name="mixed",
    )(zc, mine8, other8, w_out, slope)
    out_parts = pl.pallas_call(
        lambda *r: outer_body(*r, n=n_z),
        out_shape=jax.ShapeDtypeStruct((n_sp, conv_pre.shape[1], width_part), BF),
        in_specs=[SMEM] + [VMEM] * 3,
        out_specs=VMEM,
        compiler_params=BIG,
        name="outer",
    )(zc, mine8, other8, mixed_out.T)
    norm_total, norm_cross = in_one((jnp.sum(norm_in, axis=1), jnp.sum(norm_in * centred, axis=1)))
    conv_back = inv_std * (
        norm_in - (norm_total / channels)[:, None] - centred * (norm_cross / channels)[:, None]
    )
    next_rim = lax.ppermute(conv_back[:32], "sp", [(i + 1, i) for i in range(n_sp - 1)])
    out_blocks = lax.all_to_all(out_parts, "sp", 0, 0, tiled=True)
    value_grad, gate_grad = pl.pallas_call(
        conv_body,
        out_shape=(jax.ShapeDtypeStruct(value_in.shape, BF),) * 2,
        in_specs=[VMEM] * 5,
        out_specs=(VMEM, VMEM),
        scratch_shapes=[pltpu.VMEM((tok_rows + 32, conv_pre.shape[1]), F4)],
        name="conv",
    )(conv_back, next_rim, conv_taps, value_in, gate_in)
    out_blocks, value_grad = lax.optimization_barrier((out_blocks, value_grad))
    grad_out = jnp.sum(out_blocks.astype(F4), axis=0)
    return (grad_gate[None], grad_up[None], grad_down[None], grad_out, value_grad, gate_grad)


def solution(mesh):
    n_sp, n_tp = mesh.devices.shape
    split = Mesh(mesh.devices.reshape(n_sp, n_tp // 2, 2), ("sp", "z", "c"))
    return jax.shard_map(
        per_device,
        mesh=split,
        in_specs=(
            P("sp", TP),
            P("sp", TP),
            P(TP),
            P("sp", None),
            P("sp", None),
            P("sp", None, TP),
            P("sp", None, TP),
            P("sp", TP, None),
            P("sp", TP),
            P("sp", TP),
            P("sp", TP),
            P(TP),
            P(None, TP),
            P(TP, None),
        ),
        out_specs=(
            P("sp", None, TP),
            P("sp", None, TP),
            P("sp", TP, None),
            P(TP, "sp"),
            P("sp", TP),
            P("sp", TP),
        ),
        check_vma=False,
    )
```

```python
import jax
import jax.numpy as jnp
from jax import lax
from jax.experimental import pallas as pl
from jax.experimental.pallas import tpu as pltpu
from jax.sharding import Mesh, PartitionSpec as P

EPSILON = 1e-06
TP = ("z", "c")
BF = jnp.bfloat16
F4 = jnp.float32


def of_everyone(value):
    count = 16
    everything = lax.all_to_all(
        jnp.broadcast_to(value[None], (count, *value.shape)), TP, 0, 0, tiled=True
    )
    return jnp.sum(everything, axis=0)


def in_one(arrays):
    total = of_everyone(jnp.concatenate([a.reshape(-1) for a in arrays]))
    out, at = [], 0
    for a in arrays:
        out.append(total[at : at + a.size].reshape(a.shape))
        at += a.size
    return out


def right(x):
    n = lax.axis_size("z")
    return lax.ppermute(x, "z", [(i, (i + 1) % n) for i in range(n)])


def left(x):
    n = lax.axis_size("z")
    return lax.ppermute(x, "z", [(i, (i - 1) % n) for i in range(n)])


def hops(x, n_hops):
    n = lax.axis_size("z")
    return lax.ppermute(x, "z", [(i, (i + n_hops) % n) for i in range(n)])


def swap(x):
    return lax.ppermute(x, "c", [(0, 1), (1, 0)])


def silu_slope(values):
    logistic = jax.nn.sigmoid(values)
    return logistic * (1.0 + values * (1.0 - logistic))


def dot(a, b, ca, cb):
    return lax.dot_general(a, b, (((ca,), (cb,)), ((), ())), preferred_element_type=F4)


VMEM = pl.BlockSpec(memory_space=pltpu.VMEM)
ANY = pl.BlockSpec(memory_space=pl.ANY)
HBM = pl.BlockSpec(memory_space=pltpu.HBM)
SMEM = pl.BlockSpec(memory_space=pltpu.SMEM)
BIG = pltpu.CompilerParams(vmem_limit_bytes=40 * 2**20)


def scatter_body(
    routes_h, weights_h, upstream_h, stream_h, picker, sent, *scratch, experts, capacity
):
    routes, weights, upstream, stream, sems = scratch
    load_all(
        [(routes_h, routes), (weights_h, weights), (upstream_h, upstream), (stream_h, stream)],
        sems,
    )
    toks = upstream.shape[0]
    slots = experts * capacity
    half = capacity // 2
    r0, r1 = routes[0:1, :], routes[1:2, :]
    names = lax.broadcasted_iota(jnp.int32, (experts, toks), 0)
    hot0 = jnp.where(names == r0, 1.0, 0.0)
    hot1 = jnp.where(names == r1, 1.0, 0.0)
    earlier = jnp.where(
        lax.broadcasted_iota(jnp.int32, (toks, toks), 0)
        < lax.broadcasted_iota(jnp.int32, (toks, toks), 1),
        1.0,
        0.0,
    ).astype(BF)
    before = dot((hot0 + hot1).astype(BF), earlier, 1, 0)
    slot0 = r0 * capacity + jnp.sum(before * hot0, axis=0, keepdims=True).astype(jnp.int32)
    slot1 = r1 * capacity + jnp.sum(before * hot1, axis=0, keepdims=True).astype(jnp.int32)
    blocks = 8
    step = blocks * capacity

    def rows_at(j, carry):
        at = j * (step // 2)
        ids = lax.broadcasted_iota(jnp.int32, (step // 2, toks), 0) + at
        one = jnp.where(ids == slot0, 1.0, 0.0) + jnp.where(ids == slot1, 1.0, 0.0)
        picker[pl.ds(pl.multiple_of(at, step // 2), step // 2), :] = one.astype(BF)
        wide = lax.broadcasted_iota(jnp.int32, (step, toks), 0)
        block = lax.shift_right_logical(wide * (65536 // capacity + 1), 16)
        place = wide - block * capacity
        ids = jnp.where(place >= half, place - half, place) + (block + j * blocks) * half
        hit0, hit1 = ids == slot0, ids == slot1
        pick = (jnp.where(hit0, 1.0, 0.0) + jnp.where(hit1, 1.0, 0.0)).astype(BF)
        weight = jnp.sum(
            jnp.where(hit0, weights[0:1, :], 0.0) + jnp.where(hit1, weights[1:2, :], 0.0),
            axis=1,
            keepdims=True,
        )
        is_cot = place[:, 0:1] >= half
        value = jnp.where(
            is_cot, dot(pick, upstream[...], 1, 0) * weight, dot(pick, stream[...], 1, 0)
        )
        sent[pl.ds(pl.multiple_of(j * step, step), step), :] = value.astype(BF)
        return carry

    lax.fori_loop(0, 2 * slots // step, rows_at, 0)


def offset_of(k, offsets, n):
    off = jnp.int32(0)
    for i, value in enumerate(offsets):
        off = jnp.where(k == i, value % n, off)
    return off


def load_all(pairs, sems):
    copies = [pltpu.make_async_copy(a, b, sems.at[i]) for i, (a, b) in enumerate(pairs)]
    for copy in copies:
        copy.start()
    for copy in copies:
        copy.wait()


def phased(groups, sems, phases, step):
    copies, at = [], 0
    for group in groups:
        copies.append([])
        for a, b in group:
            copies[-1].append(pltpu.make_async_copy(a, b, sems.at[at]))
            at += 1
    for group in copies:
        for copy in group:
            copy.start()
    for lo, hi in phases:
        for group in copies[lo:hi]:
            for copy in group:
                copy.wait()
        lax.fori_loop(lo, hi, step, 0)


def unpack_body(arrived, x, c, *, n_sp):
    half = x.shape[0] // n_sp
    width = arrived.shape[1]
    for s in range(0, n_sp, 2):
        for core in range(2):
            pair = []
            for src in (s, s + 1):
                at = (2 * src + core) * 2 * half
                pair.append(arrived[at : at + 2 * half, :].astype(F4))
            lanes = pl.ds(core * width, width)
            to = pl.ds(s * half, 2 * half)
            x[to, lanes] = jnp.concatenate([p[:half] for p in pair], axis=0).astype(BF)
            c[to, lanes] = jnp.concatenate([p[half:] for p in pair], axis=0).astype(BF)


def project_body(z, *refs, offsets, n):
    m = len(offsets)
    xb, cb, refs = refs[:m], refs[m : 2 * m], refs[2 * m :]
    guo, gux, dno, dnx, gains, inv, own, oth, back, xs = refs[:10]
    xbuf, cbuf, xs_v, own_v, oth_v, dno_v, dnx_v, sems = refs[10:]
    rows, width = own.shape[0], xbuf.shape[2]
    hid = back.shape[1] // 2
    groups = []
    for i, off in enumerate(offsets):
        at = pl.multiple_of(lax.rem(z[0] + off % n, n) * width, width)
        groups.append(
            [
                (xb[i], xbuf.at[i]),
                (cb[i], cbuf.at[i]),
                (guo.at[pl.ds(at, width), :], own_v.at[i]),
                (gux.at[pl.ds(at, width), :], oth_v.at[i]),
                (dno.at[:, pl.ds(at, width)], dno_v.at[i]),
                (dnx.at[:, pl.ds(at, width)], dnx_v.at[i]),
            ]
        )
    for total in (own, oth, back):
        total[...] = jnp.zeros(total.shape, F4)

    def step(k, carry):
        chip = lax.rem(z[0] + offset_of(k, offsets, n), n)
        x = xbuf[k].astype(F4)
        x = (gains[pl.ds(chip, 1), :] * x * inv[...]).astype(BF)
        xs_v[pl.ds(pl.multiple_of(k * rows, rows), rows), :] = x
        own[...] += dot(x, own_v[k], 1, 0)
        oth[...] += dot(x, oth_v[k], 1, 0)
        c = cbuf[k]
        back[:, :hid] += dot(c, dno_v[k], 1, 1)
        back[:, hid:] += dot(c, dnx_v[k], 1, 1)
        return carry

    phased(groups, sems, ((0, 2), (2, m)), step)
    load_all([(xs_v, xs)], sems)


def project(z, xb, cb, weights, gains, inv, offsets, n):
    rows, wide = xb[0].shape
    m, hid = len(xb), weights[2].shape[0]
    total = jax.ShapeDtypeStruct((rows, 2 * hid), F4)
    return pl.pallas_call(
        lambda *r: project_body(*r, offsets=offsets, n=n),
        out_shape=(total, total, total, jax.ShapeDtypeStruct((m * rows, wide), BF)),
        in_specs=[SMEM] + [ANY] * (2 * m + 4) + [VMEM] * 2,
        out_specs=(VMEM, VMEM, VMEM, ANY),
        scratch_shapes=[
            pltpu.VMEM((m, rows, wide), BF),
            pltpu.VMEM((m, rows, wide), BF),
            pltpu.VMEM((m * rows, wide), BF),
            pltpu.VMEM((m, wide, 2 * hid), BF),
            pltpu.VMEM((m, wide, 2 * hid), BF),
            pltpu.VMEM((m, hid, wide), BF),
            pltpu.VMEM((m, hid, wide), BF),
            pltpu.SemaphoreType.DMA((6 * m,)),
        ],
        compiler_params=BIG,
        name="project",
    )(z, *xb, *cb, *weights, gains, inv)


def in_parts(row):
    hi = row.astype(BF).astype(F4)
    mid = (row - hi).astype(BF).astype(F4)
    low = (row - hi - mid).astype(BF).astype(F4)
    return hi, mid, low


def part_rows(row):
    hi, mid, low = in_parts(row)
    shape = (16, row.shape[1])
    at = lax.broadcasted_iota(jnp.int32, shape, 0)
    rows = jnp.where(at == 0, hi, jnp.where(at == 1, mid, jnp.where(at == 2, low, 0.0)))
    return rows.astype(BF)


def whole_row(rows):
    rows = rows.astype(F4)
    return rows[0:1] + rows[1:2] + rows[2:3]


def finish_body(z, xf, cf, guo, gux, dno, dnx, gains, inv, own, oth, back, *refs, n):
    hbm, refs = refs[:5], refs[5:]
    along, send_r, send_l = refs[:3]
    held = refs[3:8]
    x4, b_own, b_oth, a_own, a_oth = held
    own_v, oth_v, dno_v, dnx_v, sems = refs[8:]
    rows, width = xf.shape
    hid = dno.shape[0]
    chip = lax.rem(z[0] + n // 2, n)
    at = pl.multiple_of(chip * width, width)
    load_all(
        [
            (guo.at[pl.ds(at, width), :], own_v),
            (gux.at[pl.ds(at, width), :], oth_v),
            (dno.at[:, pl.ds(at, width)], dno_v),
            (dnx.at[:, pl.ds(at, width)], dnx_v),
        ],
        sems,
    )
    x = (gains[pl.ds(chip, 1), :] * xf[...].astype(F4) * inv[...]).astype(BF)
    x4[...] = x
    total = jnp.zeros((rows, 1), F4)
    for pre, w_v, d_v, lo, backs, act in (
        (own, own_v, dno_v, 0, b_own, a_own),
        (oth, oth_v, dnx_v, hid, b_oth, a_oth),
    ):
        both = pre[...] + dot(x, w_v[...], 1, 0)
        gate, upper = both[:, :hid], both[:, hid:]
        ab = back[:, lo : lo + hid] + dot(cf[...], d_v[...], 1, 1)
        sig = jax.nn.sigmoid(gate)
        silu = gate * sig
        act[...] = (silu * upper).astype(BF)
        gb = (ab * upper * (sig * (1.0 + gate * (1.0 - sig)))).astype(BF)
        ub = (ab * silu).astype(BF)
        backs[:, :hid] = gb
        backs[:, hid:] = ub
        total = total + jnp.sum(
            gb.astype(F4) * gate + ub.astype(F4) * upper, axis=1, keepdims=True
        )
    copies = [
        pltpu.make_async_copy(a, b, sems.at[i]) for i, (a, b) in enumerate(zip(held, hbm))
    ]
    for copy in copies:
        copy.start()
    row = jnp.broadcast_to(total, (rows, 128)).T[0:8, :]
    along[:, :rows] = row
    along[:, rows:] = jnp.zeros((8, width - rows), F4)
    part = dot(b_own[...], own_v[...], 1, 1) + dot(b_oth[...], oth_v[...], 1, 1)
    hr = rows // 2
    send_r[:hr, :] = part[:hr].astype(BF)
    send_r[hr:, :] = part_rows(along[0:1, :])
    send_l[...] = part[hr:].astype(BF)
    for copy in copies:
        copy.wait()


def parts_body(b_own, b_oth, guo, gux, out, guo_v, gux_v, sems, *, n):
    width = guo.shape[0] // n
    pairs = []
    for k in range(n):
        at = pl.ds(k * width, width)
        lanes = pl.ds(0, guo_v.shape[1])
        pairs.append((guo.at[at, lanes], guo_v.at[at, :]))
        pairs.append((gux.at[at, lanes], gux_v.at[at, :]))
    copies = [pltpu.make_async_copy(a, b, sems.at[i]) for i, (a, b) in enumerate(pairs)]
    for copy in copies:
        copy.start()
    for k in range(n):
        copies[2 * k].wait()
        copies[2 * k + 1].wait()
        at = pl.ds(k * width, width)
        out[:, at] = (
            dot(b_own[...], guo_v[at, :], 1, 1) + dot(b_oth[...], gux_v[at, :], 1, 1)
        ).astype(BF)


def hop_body(z, parts, along, ra, la, out_r, out_l, *, k, n, first):
    rows = parts.shape[0]
    width = out_r.shape[1]
    hr = rows // 2

    def block(j):
        at = pl.multiple_of(lax.rem(z[0] + (j + n), n) * width, width)
        return parts[:, pl.ds(at, width)].astype(F4)

    own = along[0:1, :]
    pr, pl_ = block(k), block(-k)
    if first:
        out_r[:hr, :] = (pr[:hr] + ra[:hr, :].astype(F4)).astype(BF)
        out_r[hr:rows, :] = pr[hr:].astype(BF)
        out_r[rows:, :] = part_rows(own + whole_row(ra[hr:, :]))
        out_l[:hr, :] = pl_[:hr].astype(BF)
        out_l[hr:rows, :] = (pl_[hr:] + la[...].astype(F4)).astype(BF)
        out_l[rows:, :] = part_rows(own)
    else:
        out_r[:rows, :] = (pr + ra[:rows, :].astype(F4)).astype(BF)
        out_r[rows:, :] = part_rows(own + whole_row(ra[rows:, :]))
        out_l[:rows, :] = (pl_ + la[:rows, :].astype(F4)).astype(BF)
        out_l[rows:, :] = part_rows(own + whole_row(la[rows:, :]))


def pack_body(z, parts, along, ra, la, out, *, n_sp):
    rows = parts.shape[0]
    width = ra.shape[1]
    half = width // 2
    step = rows // n_sp
    at = pl.multiple_of(z[0] * width, width)
    row = along[0:1, :] + whole_row(ra[rows:, :]) + whole_row(la[rows:, :])
    col = jnp.broadcast_to(row[:, :rows], (128, rows)).T
    hi, mid, low = in_parts(col)
    lane = lax.broadcasted_iota(jnp.int32, (rows, 128), 1)
    extra = jnp.where(lane == 0, hi, jnp.where(lane == 1, mid, jnp.where(lane == 2, low, 0.0)))
    value = (
        parts[:, pl.ds(at, width)].astype(F4) + ra[:rows, :].astype(F4) + la[:rows, :].astype(F4)
    )
    for s in range(n_sp):
        v = value[s * step : (s + 1) * step]
        e = extra[s * step : (s + 1) * step]
        both = jnp.concatenate([v[:, :half], v[:, half:]], axis=0)
        out[2 * s * step : 2 * (s + 1) * step, :half] = both.astype(BF)
        out[2 * s * step : 2 * (s + 1) * step, half:] = jnp.concatenate([e, e], axis=0).astype(BF)


def grads_body(z, *refs, n, add, offsets):
    xs, x4 = refs[:2]
    cb = refs[2 : n + 2]
    backs, act = refs[n + 2], refs[n + 3]
    refs = refs[n + 4 :]
    if add:
        old_h, gate, up, down, old, xbuf, cbuf, sems = refs
    else:
        out, xbuf, cbuf, sems = refs
    rows, width = x4.shape
    hid = act.shape[1]
    groups = []
    for k in range(n):
        mine = pl.ds(k * rows, rows)
        groups.append(
            [(xs.at[mine, :] if k < n - 1 else x4, xbuf.at[mine, :]), (cb[k], cbuf.at[mine, :])]
        )
    if add:
        groups[0].append((old_h, old))

    def step(k, carry):
        at = pl.multiple_of(lax.rem(z[0] + offset_of(k, offsets, n), n) * width, width)
        mine = pl.ds(pl.multiple_of(k * rows, rows), rows)
        pair = dot(xbuf[mine, :], backs[...], 0, 0)
        dn = dot(act[...], cbuf[mine, :], 0, 0)
        if add:
            gate[pl.ds(at, width), :] = pair[:, :hid] + old[0, pl.ds(at, width), :].astype(F4)
            up[pl.ds(at, width), :] = pair[:, hid:] + old[1, pl.ds(at, width), :].astype(F4)
            for q in range(width // hid):
                lo = pl.multiple_of(at + q * hid, hid)
                down[:, pl.ds(lo, hid)] = dn[:, q * hid : (q + 1) * hid] + old[
                    2, pl.ds(lo, hid), :
                ].astype(F4)
        else:
            out[0, pl.ds(at, width), :] = pair[:, :hid].astype(BF)
            out[1, pl.ds(at, width), :] = pair[:, hid:].astype(BF)
            for q in range(width // hid):
                lo = pl.multiple_of(at + q * hid, hid)
                out[2, pl.ds(lo, hid), :] = dn[:, q * hid : (q + 1) * hid].astype(BF)
        return carry

    phased(groups, sems, ((0, 2), (2, n)), step)


def grads(z, xs, x4, cb, backs, act, old, offsets):
    rows, width = x4.shape
    n, hid = len(cb), act.shape[1]
    add = old is not None
    total = n * width
    args = [z, xs, x4, *cb, backs, act] + ([old] if add else [])
    if add:
        out_shape = tuple(
            jax.ShapeDtypeStruct(t, F4) for t in ((total, hid), (total, hid), (hid, total))
        )
        out_specs = (VMEM,) * 3
    else:
        out_shape, out_specs = jax.ShapeDtypeStruct((3, total, hid), BF), VMEM
    return pl.pallas_call(
        lambda *r: grads_body(*r, n=n, add=add, offsets=offsets),
        out_shape=out_shape,
        in_specs=[SMEM] + [ANY] * (n + 2) + [VMEM] * 2 + ([ANY] if add else []),
        out_specs=out_specs,
        scratch_shapes=([pltpu.VMEM((3, total, hid), BF)] if add else [])
        + [
            pltpu.VMEM((n * rows, width), BF),
            pltpu.VMEM((n * rows, width), BF),
            pltpu.SemaphoreType.DMA((2 * n + 1,)),
        ],
        compiler_params=BIG,
        cost_estimate=pl.CostEstimate(
            flops=8 * rows * total * 3 * hid, transcendentals=0, bytes_accessed=16 * 2**20
        ),
        name="grads_own" if add else "grads_other",
    )(*args)


def stack_body(*refs):
    out, at = refs[-1], 0
    for src in refs[:-1]:
        out[pl.ds(at, src.shape[0]), :] = src[...]
        at += src.shape[0]


def mixed_body(zc, mine, other, w_out, slope, out, *, n):
    width = mine.shape[2]
    out[...] = jnp.zeros(out.shape, F4)
    for ref, core in ((mine, zc[1]), (other, 1 - zc[1])):
        acc = jnp.zeros(out.shape, F4)
        for k in range(n):
            at = pl.multiple_of((2 * lax.rem(zc[0] + k, n) + core) * width, width)
            acc = acc + dot(ref[k], w_out[:, pl.ds(at, width)], 1, 1)
        out[...] += acc
    out[...] *= slope[...]


def outer_body(zc, mine, other, mixed_t, out, *, n):
    for ref, core in ((mine, zc[1]), (other, 1 - zc[1])):
        for k in range(n):
            out[2 * lax.rem(zc[0] + k, n) + core] = dot(mixed_t[...], ref[k], 1, 0).astype(BF)


def conv_body(back, rim, taps, value_in, gate_in, value_grad, gate_grad, padded):
    toks, n_taps = back.shape[0], taps.shape[0]
    padded[:toks, :] = back[...]
    padded[toks:, :] = rim[...]
    step = 64
    for at in range(0, toks, step):
        acc = jnp.zeros((step, back.shape[1]), F4)
        for tap in range(n_taps):
            lo = at + n_taps - 1 - tap
            acc = acc + taps[tap : tap + 1, :] * padded[lo : lo + step, :]
        sigma = jax.nn.sigmoid(gate_in[at : at + step, :].astype(F4))
        value = acc * sigma
        value_grad[at : at + step, :] = value.astype(BF)
        gate_grad[at : at + step, :] = (
            value * value_in[at : at + step, :].astype(F4) * (1.0 - sigma)
        ).astype(BF)


def per_device(
    upstream,
    stream,
    norm_gain,
    routes,
    route_weights,
    w_gate,
    w_up,
    w_down,
    value_in,
    gate_in,
    conv_pre,
    ln_gain,
    conv_taps,
    w_out,
):
    tok_rows, width_part = stream.shape
    n_sp = lax.axis_size("sp")
    n_z = lax.axis_size("z")
    n_tp = 2 * n_z
    z = lax.axis_index("z")
    core = lax.axis_index("c")
    model_width = width_part * n_tp
    channels = conv_pre.shape[1] * n_tp
    tap_count = conv_taps.shape[0]
    capacity = 3 * tok_rows // n_sp
    half_cap = capacity // 2
    experts = n_sp
    slot_count = experts * capacity
    rows = n_sp * half_cap
    wide = 2 * width_part

    zs = z.astype(jnp.int32).reshape(1)
    half = n_z // 2
    hid = w_gate.shape[2]

    picker, sent = pl.pallas_call(
        lambda *r: scatter_body(*r, experts=experts, capacity=capacity),
        out_shape=(
            jax.ShapeDtypeStruct((slot_count, tok_rows), BF),
            jax.ShapeDtypeStruct((2 * slot_count, width_part), BF),
        ),
        in_specs=[HBM] * 4,
        out_specs=(VMEM, VMEM),
        scratch_shapes=[
            pltpu.VMEM((2, tok_rows), jnp.int32),
            pltpu.VMEM((2, tok_rows), F4),
            pltpu.VMEM(upstream.shape, BF),
            pltpu.VMEM(stream.shape, BF),
            pltpu.SemaphoreType.DMA((4,)),
        ],
        compiler_params=BIG,
        name="scatter",
    )(routes.T, route_weights.T, upstream, stream)
    arrived = lax.all_to_all(
        sent.reshape(2 * experts, capacity, width_part), ("sp", "c"), 0, 0, tiled=True
    )
    x0, c0 = pl.pallas_call(
        lambda *r: unpack_body(*r, n_sp=n_sp),
        out_shape=(jax.ShapeDtypeStruct((rows, wide), BF),) * 2,
        in_specs=[VMEM],
        out_specs=(VMEM, VMEM),
        compiler_params=BIG,
        name="unpack",
    )(arrived.reshape(2 * slot_count, width_part))

    gu_own = jnp.concatenate([w_gate[0], w_up[0]], axis=1)
    weights = (gu_own, swap(gu_own), w_down[0], swap(w_down[0]))

    residual = stream.astype(F4)
    conv_vals = conv_pre.astype(F4)
    own_rows = x0.astype(F4)
    row_part = jnp.sum(own_rows * own_rows, axis=1)
    nothing = jnp.zeros_like(row_part)
    vector = jnp.concatenate(
        [
            jnp.sum(residual * residual, axis=1),
            jnp.sum(conv_vals, axis=1),
            jnp.sum(conv_vals * conv_vals, axis=1),
            jnp.where(core == 0, row_part, nothing),
            jnp.where(core == 0, nothing, row_part),
            norm_gain,
        ]
    )
    told = lax.all_to_all(
        jnp.broadcast_to(vector[None, None], (n_tp, 1, vector.size)), TP, 0, 0, tiled=True
    )[:, 0]
    cut = 3 * tok_rows + 2 * rows
    total = jnp.sum(told[:, :cut], axis=0)
    gains = told[:, cut:].reshape(n_z, wide)
    row_squares, conv_total, conv_squares = jnp.split(total[: 3 * tok_rows], 3)
    slot_squares = jnp.where(
        core == 0, total[3 * tok_rows : 3 * tok_rows + rows], total[3 * tok_rows + rows :]
    )
    inverse = lax.rsqrt(row_squares / model_width + EPSILON)[:, None]
    slot_inverse = lax.rsqrt(slot_squares / model_width + EPSILON)[:, None]

    xr, cl, cr, xl = [x0], [c0], [c0], [x0]
    for _ in range(half - 1):
        xr.append(right(xr[-1]))
        cl.append(left(cl[-1]))
        cr.append(right(cr[-1]))
        xl.append(left(xl[-1]))
    xf, cf = right(xr[-1]), left(cl[-1])
    offsets = (0, -1, 1, -2, 2, -3, 3, 4)
    xb, cb = [x0], [c0]
    for k in range(1, half):
        xb += [xr[k], xl[k]]
        cb += [cr[k], cl[k]]
    own, oth, back, xs = project(
        zs, xb, cb, weights, gains, slot_inverse, offsets[:-1], n_z
    )
    cb.append(cf)

    x4, b_own, b_oth, a_own, a_oth, along, ra, la = pl.pallas_call(
        lambda *r: finish_body(*r, n=n_z),
        out_shape=(
            jax.ShapeDtypeStruct((rows, wide), BF),
            jax.ShapeDtypeStruct((rows, 2 * hid), BF),
            jax.ShapeDtypeStruct((rows, 2 * hid), BF),
            jax.ShapeDtypeStruct((rows, hid), BF),
            jax.ShapeDtypeStruct((rows, hid), BF),
            jax.ShapeDtypeStruct((8, wide), F4),
            jax.ShapeDtypeStruct((rows // 2 + 16, wide), BF),
            jax.ShapeDtypeStruct((rows // 2, wide), BF),
        ),
        in_specs=[SMEM] + [VMEM] * 2 + [ANY] * 4 + [VMEM] * 5,
        out_specs=(ANY,) * 5 + (VMEM,) * 3,
        scratch_shapes=[
            pltpu.VMEM((rows, wide), BF),
            pltpu.VMEM((rows, 2 * hid), BF),
            pltpu.VMEM((rows, 2 * hid), BF),
            pltpu.VMEM((rows, hid), BF),
            pltpu.VMEM((rows, hid), BF),
            pltpu.VMEM((wide, 2 * hid), BF),
            pltpu.VMEM((wide, 2 * hid), BF),
            pltpu.VMEM((hid, wide), BF),
            pltpu.VMEM((hid, wide), BF),
            pltpu.SemaphoreType.DMA((5,)),
        ],
        compiler_params=BIG,
        name="finish",
    )(zs, xf, cf, *weights, gains, slot_inverse, own, oth, back)

    ra, la = right(ra), left(la)
    parts = pl.pallas_call(
        lambda *r: parts_body(*r, n=n_z),
        out_shape=jax.ShapeDtypeStruct((rows, model_width), BF),
        in_specs=[VMEM] * 2 + [ANY] * 2,
        out_specs=VMEM,
        scratch_shapes=[
            pltpu.VMEM((model_width, 2 * hid), BF),
            pltpu.VMEM((model_width, 2 * hid), BF),
            pltpu.SemaphoreType.DMA((2 * n_z,)),
        ],
        compiler_params=BIG,
        name="parts",
    )(b_own, b_oth, *weights[:2])
    message = jax.ShapeDtypeStruct((rows + 16, wide), BF)
    for k in range(half - 1, 0, -1):
        ra, la = pl.pallas_call(
            lambda *r, k=k: hop_body(*r, k=k, n=n_z, first=k == half - 1),
            out_shape=(message, message),
            in_specs=[SMEM] + [VMEM] * 4,
            out_specs=(VMEM, VMEM),
            compiler_params=BIG,
            name="hop",
        )(zs, parts, along, ra, la)
        ra, la = right(ra), left(la)
        if k == 2:
            others = grads(zs, xs, x4, cb, b_oth, a_oth, None, offsets)
            ra, la, others = lax.optimization_barrier((ra, la, others))
    sent_back = pl.pallas_call(
        lambda *r: pack_body(*r, n_sp=n_sp),
        out_shape=jax.ShapeDtypeStruct((slot_count, width_part + 128), BF),
        in_specs=[SMEM] + [VMEM] * 4,
        out_specs=VMEM,
        compiler_params=BIG,
        name="pack",
    )(zs, parts, along, ra, la)
    sent_back, others = lax.optimization_barrier((sent_back, others))
    others = swap(others)
    returned = lax.all_to_all(
        sent_back.reshape(2 * n_sp, half_cap, width_part + 128), ("sp", "c"), 0, 0, tiled=True
    ).reshape(slot_count, width_part + 128)

    token_back = dot(picker, returned, 0, 0)
    inner = jnp.sum(token_back[:, width_part : width_part + 3], axis=1, keepdims=True)
    gained = norm_gain[None, :] * token_back[:, :width_part]
    norm_back = inverse * gained - residual * inverse**2 * (inner / model_width)
    stream_grad = (upstream.astype(F4) + norm_back).astype(BF)

    ht = tok_rows // 2
    p1, m1, p2, m2 = (hops(stream_grad, d) for d in (1, -1, 2, -2))
    p3, m3 = hops(p1, 2), hops(m1, -2)
    pf, mf = hops(p2[:ht], 2), hops(m2[ht:], -2)
    mine8 = pl.pallas_call(
        stack_body,
        out_shape=jax.ShapeDtypeStruct((n_z * tok_rows, width_part), BF),
        in_specs=[VMEM] * 9,
        out_specs=VMEM,
        compiler_params=BIG,
        name="stack",
    )(stream_grad, m1, m2, m3, pf, mf, p3, p2, p1).reshape(n_z, tok_rows, width_part)
    other8 = swap(mine8)

    mean_val = (conv_total / channels)[:, None]
    variance = (conv_squares / channels)[:, None] - mean_val * mean_val
    inv_std = lax.rsqrt(variance + EPSILON)
    centred = (conv_vals - mean_val) * inv_std
    scaled = centred * ln_gain[None, :]
    mixed_out = jax.nn.silu(scaled).astype(BF)

    zc = jnp.stack([z, core]).astype(jnp.int32)
    slope = silu_slope(scaled) * ln_gain[None, :]
    norm_in = pl.pallas_call(
        lambda *r: mixed_body(*r, n=n_z),
        out_shape=jax.ShapeDtypeStruct(conv_pre.shape, F4),
        in_specs=[SMEM] + [VMEM] * 4,
        out_specs=VMEM,
        compiler_params=BIG,
        name="mixed",
    )(zc, mine8, other8, w_out, slope)
    out_parts = pl.pallas_call(
        lambda *r: outer_body(*r, n=n_z),
        out_shape=jax.ShapeDtypeStruct((n_sp, conv_pre.shape[1], width_part), BF),
        in_specs=[SMEM] + [VMEM] * 3,
        out_specs=VMEM,
        compiler_params=BIG,
        name="outer",
    )(zc, mine8, other8, mixed_out.T)
    norm_total, norm_cross = in_one((jnp.sum(norm_in, axis=1), jnp.sum(norm_in * centred, axis=1)))
    conv_back = inv_std * (
        norm_in - (norm_total / channels)[:, None] - centred * (norm_cross / channels)[:, None]
    )
    next_rim = lax.ppermute(conv_back[:32], "sp", [(i + 1, i) for i in range(n_sp - 1)])
    out_blocks = lax.all_to_all(out_parts, "sp", 0, 0, tiled=True)
    grad_gate, grad_up, grad_down = grads(zs, xs, x4, cb, b_own, a_own, others, offsets)
    conv_back, grad_gate, grad_up, grad_down = lax.optimization_barrier(
        (conv_back, grad_gate, grad_up, grad_down)
    )
    value_grad, gate_grad = pl.pallas_call(
        conv_body,
        out_shape=(jax.ShapeDtypeStruct(value_in.shape, BF),) * 2,
        in_specs=[VMEM] * 5,
        out_specs=(VMEM, VMEM),
        scratch_shapes=[pltpu.VMEM((tok_rows + 32, conv_pre.shape[1]), F4)],
        name="conv",
    )(conv_back, next_rim, conv_taps, value_in, gate_in)
    out_blocks, value_grad = lax.optimization_barrier((out_blocks, value_grad))
    grad_out = jnp.sum(out_blocks.astype(F4), axis=0)
    return (grad_gate[None], grad_up[None], grad_down[None], grad_out, value_grad, gate_grad)


def solution(mesh):
    n_sp, n_tp = mesh.devices.shape
    split = Mesh(mesh.devices.reshape(n_sp, n_tp // 2, 2), ("sp", "z", "c"))
    return jax.shard_map(
        per_device,
        mesh=split,
        in_specs=(
            P("sp", TP),
            P("sp", TP),
            P(TP),
            P("sp", None),
            P("sp", None),
            P("sp", None, TP),
            P("sp", None, TP),
            P("sp", TP, None),
            P("sp", TP),
            P("sp", TP),
            P("sp", TP),
            P(TP),
            P(None, TP),
            P(TP, None),
        ),
        out_specs=(
            P("sp", None, TP),
            P("sp", None, TP),
            P("sp", TP, None),
            P(TP, "sp"),
            P("sp", TP),
            P("sp", TP),
        ),
        check_vma=False,
    )
```

```python
import jax
import jax.numpy as jnp
from jax import lax
from jax.experimental import pallas as pl
from jax.experimental.pallas import tpu as pltpu
from jax.sharding import Mesh, PartitionSpec as P

EPSILON = 1e-06
TP = ("z", "c")
BF = jnp.bfloat16
F4 = jnp.float32


def of_everyone(value):
    count = 16
    everything = lax.all_to_all(
        jnp.broadcast_to(value[None], (count, *value.shape)), TP, 0, 0, tiled=True
    )
    return jnp.sum(everything, axis=0)


def in_one(arrays):
    total = of_everyone(jnp.concatenate([a.reshape(-1) for a in arrays]))
    out, at = [], 0
    for a in arrays:
        out.append(total[at : at + a.size].reshape(a.shape))
        at += a.size
    return out


def right(x):
    n = lax.axis_size("z")
    return lax.ppermute(x, "z", [(i, (i + 1) % n) for i in range(n)])


def left(x):
    n = lax.axis_size("z")
    return lax.ppermute(x, "z", [(i, (i - 1) % n) for i in range(n)])


def hops(x, n_hops):
    n = lax.axis_size("z")
    return lax.ppermute(x, "z", [(i, (i + n_hops) % n) for i in range(n)])


def swap(x):
    return lax.ppermute(x, "c", [(0, 1), (1, 0)])


def silu_slope(values):
    logistic = jax.nn.sigmoid(values)
    return logistic * (1.0 + values * (1.0 - logistic))


def dot(a, b, ca, cb):
    return lax.dot_general(a, b, (((ca,), (cb,)), ((), ())), preferred_element_type=F4)


VMEM = pl.BlockSpec(memory_space=pltpu.VMEM)
ANY = pl.BlockSpec(memory_space=pl.ANY)
HBM = pl.BlockSpec(memory_space=pltpu.HBM)
SMEM = pl.BlockSpec(memory_space=pltpu.SMEM)
BIG = pltpu.CompilerParams(vmem_limit_bytes=40 * 2**20)


def scatter_body(
    routes_h, weights_h, upstream_h, stream_h, picker, sent, *scratch, experts, capacity
):
    routes, weights, upstream, stream, sems = scratch
    load_all(
        [(routes_h, routes), (weights_h, weights), (upstream_h, upstream), (stream_h, stream)],
        sems,
    )
    toks = upstream.shape[0]
    slots = experts * capacity
    half = capacity // 2
    r0, r1 = routes[0:1, :], routes[1:2, :]
    names = lax.broadcasted_iota(jnp.int32, (experts, toks), 0)
    hot0 = jnp.where(names == r0, 1.0, 0.0)
    hot1 = jnp.where(names == r1, 1.0, 0.0)
    earlier = jnp.where(
        lax.broadcasted_iota(jnp.int32, (toks, toks), 0)
        < lax.broadcasted_iota(jnp.int32, (toks, toks), 1),
        1.0,
        0.0,
    ).astype(BF)
    before = dot((hot0 + hot1).astype(BF), earlier, 1, 0)
    slot0 = r0 * capacity + jnp.sum(before * hot0, axis=0, keepdims=True).astype(jnp.int32)
    slot1 = r1 * capacity + jnp.sum(before * hot1, axis=0, keepdims=True).astype(jnp.int32)
    blocks = 4
    step = blocks * capacity

    def rows_at(j, carry):
        at = j * (step // 2)
        ids = lax.broadcasted_iota(jnp.int32, (step // 2, toks), 0) + at
        one = jnp.where(ids == slot0, 1.0, 0.0) + jnp.where(ids == slot1, 1.0, 0.0)
        picker[pl.ds(pl.multiple_of(at, step // 2), step // 2), :] = one.astype(BF)
        wide = lax.broadcasted_iota(jnp.int32, (step, toks), 0)
        block = lax.shift_right_logical(wide * (65536 // capacity + 1), 16)
        place = wide - block * capacity
        ids = jnp.where(place >= half, place - half, place) + (block + j * blocks) * half
        hit0, hit1 = ids == slot0, ids == slot1
        pick = (jnp.where(hit0, 1.0, 0.0) + jnp.where(hit1, 1.0, 0.0)).astype(BF)
        weight = jnp.sum(
            jnp.where(hit0, weights[0:1, :], 0.0) + jnp.where(hit1, weights[1:2, :], 0.0),
            axis=1,
            keepdims=True,
        )
        is_cot = place[:, 0:1] >= half
        value = jnp.where(
            is_cot, dot(pick, upstream[...], 1, 0) * weight, dot(pick, stream[...], 1, 0)
        )
        sent[pl.ds(pl.multiple_of(j * step, step), step), :] = value.astype(BF)
        return carry

    lax.fori_loop(0, 2 * slots // step, rows_at, 0)


def offset_of(k, offsets, n):
    off = jnp.int32(0)
    for i, value in enumerate(offsets):
        off = jnp.where(k == i, value % n, off)
    return off


def load_all(pairs, sems):
    copies = [pltpu.make_async_copy(a, b, sems.at[i]) for i, (a, b) in enumerate(pairs)]
    for copy in copies:
        copy.start()
    for copy in copies:
        copy.wait()


def loaded(groups, sems, step):
    copies, at = [], 0
    for group in groups:
        copies.append([])
        for a, b in group:
            copies[-1].append(pltpu.make_async_copy(a, b, sems.at[at]))
            at += 1
    for group in copies:
        for copy in group:
            copy.start()
    for group in copies:
        for copy in group:
            copy.wait()
    lax.fori_loop(0, len(groups), step, 0)


def unpack_body(arrived, x, c, *, n_sp):
    half = x.shape[0] // n_sp
    width = arrived.shape[1]
    for s in range(0, n_sp, 2):
        for core in range(2):
            pair = []
            for src in (s, s + 1):
                at = (2 * src + core) * 2 * half
                pair.append(arrived[at : at + 2 * half, :].astype(F4))
            lanes = pl.ds(core * width, width)
            to = pl.ds(s * half, 2 * half)
            x[to, lanes] = jnp.concatenate([p[:half] for p in pair], axis=0).astype(BF)
            c[to, lanes] = jnp.concatenate([p[half:] for p in pair], axis=0).astype(BF)


def project_body(z, *refs, offsets, n, more):
    m = len(offsets)
    xb, cb, refs = refs[:m], refs[m : 2 * m], refs[2 * m :]
    guo, gux, dno, dnx, gains, inv = refs[:6]
    starts, refs = (refs[6:9], refs[9:]) if more else (None, refs[6:])
    own, oth, back, xs = refs[:4]
    xbuf, cbuf, xs_v, own_v, oth_v, dno_v, dnx_v, sems = refs[4:]
    rows, width = own.shape[0], xbuf.shape[2]
    hid = back.shape[1] // 2
    groups = []
    for i, off in enumerate(offsets):
        at = pl.multiple_of(lax.rem(z[0] + off % n, n) * width, width)
        groups.append(
            [
                (xb[i], xbuf.at[i]),
                (cb[i], cbuf.at[i]),
                (guo.at[pl.ds(at, width), :], own_v.at[i]),
                (gux.at[pl.ds(at, width), :], oth_v.at[i]),
                (dno.at[:, pl.ds(at, width)], dno_v.at[i]),
                (dnx.at[:, pl.ds(at, width)], dnx_v.at[i]),
            ]
        )
    for i, total in enumerate((own, oth, back)):
        total[...] = starts[i][...] if more else jnp.zeros(total.shape, F4)

    def step(k, carry):
        chip = lax.rem(z[0] + offset_of(k, offsets, n), n)
        x = xbuf[k].astype(F4)
        x = (gains[pl.ds(chip, 1), :] * x * inv[...]).astype(BF)
        xs_v[pl.ds(pl.multiple_of(k * rows, rows), rows), :] = x
        own[...] += dot(x, own_v[k], 1, 0)
        oth[...] += dot(x, oth_v[k], 1, 0)
        c = cbuf[k]
        back[:, :hid] += dot(c, dno_v[k], 1, 1)
        back[:, hid:] += dot(c, dnx_v[k], 1, 1)
        return carry

    loaded(groups, sems, step)
    load_all([(xs_v, xs)], sems)


def project(z, xb, cb, weights, gains, inv, offsets, n, starts):
    rows, wide = xb[0].shape
    m, hid = len(xb), weights[2].shape[0]
    total = jax.ShapeDtypeStruct((rows, 2 * hid), F4)
    return pl.pallas_call(
        lambda *r: project_body(*r, offsets=offsets, n=n, more=starts is not None),
        out_shape=(total, total, total, jax.ShapeDtypeStruct((m * rows, wide), BF)),
        in_specs=[SMEM] + [ANY] * (2 * m + 4) + [VMEM] * (2 + len(starts or ())),
        out_specs=(VMEM, VMEM, VMEM, ANY),
        scratch_shapes=[
            pltpu.VMEM((m, rows, wide), BF),
            pltpu.VMEM((m, rows, wide), BF),
            pltpu.VMEM((m * rows, wide), BF),
            pltpu.VMEM((m, wide, 2 * hid), BF),
            pltpu.VMEM((m, wide, 2 * hid), BF),
            pltpu.VMEM((m, hid, wide), BF),
            pltpu.VMEM((m, hid, wide), BF),
            pltpu.SemaphoreType.DMA((6 * m,)),
        ],
        compiler_params=BIG,
        name="project",
    )(z, *xb, *cb, *weights, gains, inv, *(starts or ()))


def in_parts(row):
    hi = row.astype(BF).astype(F4)
    mid = (row - hi).astype(BF).astype(F4)
    low = (row - hi - mid).astype(BF).astype(F4)
    return hi, mid, low


def part_rows(row):
    hi, mid, low = in_parts(row)
    shape = (16, row.shape[1])
    at = lax.broadcasted_iota(jnp.int32, shape, 0)
    rows = jnp.where(at == 0, hi, jnp.where(at == 1, mid, jnp.where(at == 2, low, 0.0)))
    return rows.astype(BF)


def whole_row(rows):
    rows = rows.astype(F4)
    return rows[0:1] + rows[1:2] + rows[2:3]


def finish_body(z, xf, cf, guo, gux, dno, dnx, gains, inv, own, oth, back, *refs, n):
    hbm, refs = refs[:5], refs[5:]
    along, send_r, send_l = refs[:3]
    held = refs[3:8]
    x4, b_own, b_oth, a_own, a_oth = held
    own_v, oth_v, dno_v, dnx_v, sems = refs[8:]
    rows, width = xf.shape
    hid = dno.shape[0]
    chip = lax.rem(z[0] + n // 2, n)
    at = pl.multiple_of(chip * width, width)
    load_all(
        [
            (guo.at[pl.ds(at, width), :], own_v),
            (gux.at[pl.ds(at, width), :], oth_v),
            (dno.at[:, pl.ds(at, width)], dno_v),
            (dnx.at[:, pl.ds(at, width)], dnx_v),
        ],
        sems,
    )
    x = (gains[pl.ds(chip, 1), :] * xf[...].astype(F4) * inv[...]).astype(BF)
    x4[...] = x
    total = jnp.zeros((rows, 1), F4)
    for pre, w_v, d_v, lo, backs, act in (
        (own, own_v, dno_v, 0, b_own, a_own),
        (oth, oth_v, dnx_v, hid, b_oth, a_oth),
    ):
        both = pre[...] + dot(x, w_v[...], 1, 0)
        gate, upper = both[:, :hid], both[:, hid:]
        ab = back[:, lo : lo + hid] + dot(cf[...], d_v[...], 1, 1)
        sig = jax.nn.sigmoid(gate)
        silu = gate * sig
        act[...] = (silu * upper).astype(BF)
        gb = (ab * upper * (sig * (1.0 + gate * (1.0 - sig)))).astype(BF)
        ub = (ab * silu).astype(BF)
        backs[:, :hid] = gb
        backs[:, hid:] = ub
        total = total + jnp.sum(
            gb.astype(F4) * gate + ub.astype(F4) * upper, axis=1, keepdims=True
        )
    copies = [
        pltpu.make_async_copy(a, b, sems.at[i]) for i, (a, b) in enumerate(zip(held, hbm))
    ]
    for copy in copies:
        copy.start()
    row = jnp.broadcast_to(total, (rows, 128)).T[0:8, :]
    along[:, :rows] = row
    along[:, rows:] = jnp.zeros((8, width - rows), F4)
    part = dot(b_own[...], own_v[...], 1, 1) + dot(b_oth[...], oth_v[...], 1, 1)
    hr = rows // 2
    send_r[:hr, :] = part[:hr].astype(BF)
    send_r[hr:, :] = part_rows(along[0:1, :])
    send_l[...] = part[hr:].astype(BF)
    for copy in copies:
        copy.wait()


def parts_body(b_own, b_oth, guo, gux, out, guo_v, gux_v, sems, *, n):
    width = guo.shape[0] // n

    def copies(k):
        at = pl.ds(pl.multiple_of(k * width, width), width)
        return (
            pltpu.make_async_copy(guo.at[at, :], guo_v.at[at, :], sems.at[2 * k]),
            pltpu.make_async_copy(gux.at[at, :], gux_v.at[at, :], sems.at[2 * k + 1]),
        )

    def begin(k, carry):
        for copy in copies(k):
            copy.start()
        return carry

    def step(k, carry):
        for copy in copies(k):
            copy.wait()
        at = pl.ds(pl.multiple_of(k * width, width), width)
        out[:, at] = (
            dot(b_own[...], guo_v[at, :], 1, 1) + dot(b_oth[...], gux_v[at, :], 1, 1)
        ).astype(BF)
        return carry

    lax.fori_loop(0, n, begin, 0)
    lax.fori_loop(0, n, step, 0)


def hop_body(z, parts, along, ra, la, out_r, out_l, *, k, n, first):
    rows = parts.shape[0]
    width = out_r.shape[1]
    hr = rows // 2

    def block(j):
        at = pl.multiple_of(lax.rem(z[0] + (j + n), n) * width, width)
        return parts[:, pl.ds(at, width)].astype(F4)

    own = along[0:1, :]
    pr, pl_ = block(k), block(-k)
    if first:
        out_r[:hr, :] = (pr[:hr] + ra[:hr, :].astype(F4)).astype(BF)
        out_r[hr:rows, :] = pr[hr:].astype(BF)
        out_r[rows:, :] = part_rows(own + whole_row(ra[hr:, :]))
        out_l[:hr, :] = pl_[:hr].astype(BF)
        out_l[hr:rows, :] = (pl_[hr:] + la[...].astype(F4)).astype(BF)
        out_l[rows:, :] = part_rows(own)
    else:
        out_r[:rows, :] = (pr + ra[:rows, :].astype(F4)).astype(BF)
        out_r[rows:, :] = part_rows(own + whole_row(ra[rows:, :]))
        out_l[:rows, :] = (pl_ + la[:rows, :].astype(F4)).astype(BF)
        out_l[rows:, :] = part_rows(own + whole_row(la[rows:, :]))


def pack_body(z, parts, along, ra, la, out, value, extra, *, n_sp):
    rows = parts.shape[0]
    width = ra.shape[1]
    half = width // 2
    step = rows // n_sp
    at = pl.multiple_of(z[0] * width, width)
    row = along[0:1, :] + whole_row(ra[rows:, :]) + whole_row(la[rows:, :])
    col = jnp.broadcast_to(row[:, :rows], (128, rows)).T
    hi, mid, low = in_parts(col)
    lane = lax.broadcasted_iota(jnp.int32, (rows, 128), 1)
    extra[...] = jnp.where(
        lane == 0, hi, jnp.where(lane == 1, mid, jnp.where(lane == 2, low, 0.0))
    )
    value[...] = (
        parts[:, pl.ds(at, width)].astype(F4) + ra[:rows, :].astype(F4) + la[:rows, :].astype(F4)
    )

    def one(s, carry):
        at = pl.ds(pl.multiple_of(s * step, 8), step)
        to = pl.ds(pl.multiple_of(s * 2 * step, 16), 2 * step)
        v, e = value[at, :], extra[at, :]
        both = jnp.concatenate([v[:, :half], v[:, half:]], axis=0)
        out[to, :half] = both.astype(BF)
        out[to, half:] = jnp.concatenate([e, e], axis=0).astype(BF)
        return carry

    lax.fori_loop(0, n_sp, one, 0)


def grads_body(z, *refs, n, add, offsets):
    xs1, xs2, x4 = refs[:3]
    cb = refs[3 : n + 3]
    backs, act = refs[n + 3], refs[n + 4]
    refs = refs[n + 5 :]
    if add:
        old_h, gate, up, down, old, xbuf, cbuf, sems = refs
    else:
        out, xbuf, cbuf, sems = refs
    rows, width = x4.shape
    hid = act.shape[1]
    groups = []
    for k in range(n):
        groups.append([(cb[k], cbuf.at[pl.ds(k * rows, rows), :])])
    at = 0
    for x in (xs1, xs2, x4):
        groups[0].append((x, xbuf.at[pl.ds(at, x.shape[0]), :]))
        at += x.shape[0]
    if add:
        groups[0].append((old_h, old))

    def step(k, carry):
        at = pl.multiple_of(lax.rem(z[0] + offset_of(k, offsets, n), n) * width, width)
        mine = pl.ds(pl.multiple_of(k * rows, rows), rows)
        pair = dot(xbuf[mine, :], backs[...], 0, 0)
        dn = dot(act[...], cbuf[mine, :], 0, 0)
        if add:
            gate[pl.ds(at, width), :] = pair[:, :hid] + old[0, pl.ds(at, width), :].astype(F4)
            up[pl.ds(at, width), :] = pair[:, hid:] + old[1, pl.ds(at, width), :].astype(F4)
            for q in range(width // hid):
                lo = pl.multiple_of(at + q * hid, hid)
                down[:, pl.ds(lo, hid)] = dn[:, q * hid : (q + 1) * hid] + old[
                    2, pl.ds(lo, hid), :
                ].astype(F4)
        else:
            out[0, pl.ds(at, width), :] = pair[:, :hid].astype(BF)
            out[1, pl.ds(at, width), :] = pair[:, hid:].astype(BF)
            for q in range(width // hid):
                lo = pl.multiple_of(at + q * hid, hid)
                out[2, pl.ds(lo, hid), :] = dn[:, q * hid : (q + 1) * hid].astype(BF)
        return carry

    loaded(groups, sems, step)


def grads(z, xs, x4, cb, backs, act, old, offsets):
    rows, width = x4.shape
    n, hid = len(cb), act.shape[1]
    add = old is not None
    total = n * width
    args = [z, *xs, x4, *cb, backs, act] + ([old] if add else [])
    if add:
        out_shape = tuple(
            jax.ShapeDtypeStruct(t, F4) for t in ((total, hid), (total, hid), (hid, total))
        )
        out_specs = (VMEM,) * 3
    else:
        out_shape, out_specs = jax.ShapeDtypeStruct((3, total, hid), BF), VMEM
    return pl.pallas_call(
        lambda *r: grads_body(*r, n=n, add=add, offsets=offsets),
        out_shape=out_shape,
        in_specs=[SMEM] + [ANY] * (n + 3) + [VMEM] * 2 + ([ANY] if add else []),
        out_specs=out_specs,
        scratch_shapes=([pltpu.VMEM((3, total, hid), BF)] if add else [])
        + [
            pltpu.VMEM((n * rows, width), BF),
            pltpu.VMEM((n * rows, width), BF),
            pltpu.SemaphoreType.DMA((n + 4,)),
        ],
        compiler_params=BIG,
        cost_estimate=pl.CostEstimate(
            flops=8 * rows * total * 3 * hid, transcendentals=0, bytes_accessed=16 * 2**20
        ),
        name="grads_own" if add else "grads_other",
    )(*args)


def stack_body(*refs):
    out, at = refs[-1], 0
    for src in refs[:-1]:
        out[pl.ds(at, src.shape[0]), :] = src[...]
        at += src.shape[0]


def mixed_body(zc, mine, other, w_out, slope, out, *, n):
    width = mine.shape[2]
    out[...] = jnp.zeros(out.shape, F4)

    def step(k, carry):
        base = 2 * lax.rem(zc[0] + k, n)
        a = pl.multiple_of((base + zc[1]) * width, width)
        b = pl.multiple_of((base + 1 - zc[1]) * width, width)
        out[...] += dot(mine[k], w_out[:, pl.ds(a, width)], 1, 1) + dot(
            other[k], w_out[:, pl.ds(b, width)], 1, 1
        )
        return carry

    lax.fori_loop(0, n, step, 0)
    out[...] *= slope[...]


def outer_body(zc, mine, other, mixed_t, out, *, n):
    def step(k, carry):
        base = 2 * lax.rem(zc[0] + k, n)
        out[base + zc[1]] = dot(mixed_t[...], mine[k], 1, 0).astype(BF)
        out[base + 1 - zc[1]] = dot(mixed_t[...], other[k], 1, 0).astype(BF)
        return carry

    lax.fori_loop(0, n, step, 0)


def conv_body(back, rim, taps, value_in, gate_in, value_grad, gate_grad, padded):
    toks, n_taps = back.shape[0], taps.shape[0]
    padded[:toks, :] = back[...]
    padded[toks:, :] = rim[...]
    step = 128
    for at in range(0, toks, step):
        acc = jnp.zeros((step, back.shape[1]), F4)

        def one(tap, acc, at=at):
            lo = at + n_taps - 1 - tap
            return acc + taps[pl.ds(tap, 1), :] * padded[pl.ds(lo, step), :]

        acc = lax.fori_loop(0, n_taps, one, acc)
        sigma = jax.nn.sigmoid(gate_in[at : at + step, :].astype(F4))
        value = acc * sigma
        value_grad[at : at + step, :] = value.astype(BF)
        gate_grad[at : at + step, :] = (
            value * value_in[at : at + step, :].astype(F4) * (1.0 - sigma)
        ).astype(BF)


def per_device(
    upstream,
    stream,
    norm_gain,
    routes,
    route_weights,
    w_gate,
    w_up,
    w_down,
    value_in,
    gate_in,
    conv_pre,
    ln_gain,
    conv_taps,
    w_out,
):
    tok_rows, width_part = stream.shape
    n_sp = lax.axis_size("sp")
    n_z = lax.axis_size("z")
    n_tp = 2 * n_z
    z = lax.axis_index("z")
    core = lax.axis_index("c")
    model_width = width_part * n_tp
    channels = conv_pre.shape[1] * n_tp
    tap_count = conv_taps.shape[0]
    capacity = 3 * tok_rows // n_sp
    half_cap = capacity // 2
    experts = n_sp
    slot_count = experts * capacity
    rows = n_sp * half_cap
    wide = 2 * width_part

    zs = z.astype(jnp.int32).reshape(1)
    half = n_z // 2
    hid = w_gate.shape[2]

    picker, sent = pl.pallas_call(
        lambda *r: scatter_body(*r, experts=experts, capacity=capacity),
        out_shape=(
            jax.ShapeDtypeStruct((slot_count, tok_rows), BF),
            jax.ShapeDtypeStruct((2 * slot_count, width_part), BF),
        ),
        in_specs=[HBM] * 4,
        out_specs=(VMEM, VMEM),
        scratch_shapes=[
            pltpu.VMEM((2, tok_rows), jnp.int32),
            pltpu.VMEM((2, tok_rows), F4),
            pltpu.VMEM(upstream.shape, BF),
            pltpu.VMEM(stream.shape, BF),
            pltpu.SemaphoreType.DMA((4,)),
        ],
        compiler_params=BIG,
        name="scatter",
    )(routes.T, route_weights.T, upstream, stream)
    arrived = lax.all_to_all(
        sent.reshape(2 * experts, capacity, width_part), ("sp", "c"), 0, 0, tiled=True
    )
    x0, c0 = pl.pallas_call(
        lambda *r: unpack_body(*r, n_sp=n_sp),
        out_shape=(jax.ShapeDtypeStruct((rows, wide), BF),) * 2,
        in_specs=[VMEM],
        out_specs=(VMEM, VMEM),
        compiler_params=BIG,
        name="unpack",
    )(arrived.reshape(2 * slot_count, width_part))

    gu_own = jnp.concatenate([w_gate[0], w_up[0]], axis=1)
    weights = (gu_own, swap(gu_own), w_down[0], swap(w_down[0]))

    residual = stream.astype(F4)
    conv_vals = conv_pre.astype(F4)
    own_rows = x0.astype(F4)
    row_part = jnp.sum(own_rows * own_rows, axis=1)
    nothing = jnp.zeros_like(row_part)
    vector = jnp.concatenate(
        [
            jnp.sum(residual * residual, axis=1),
            jnp.sum(conv_vals, axis=1),
            jnp.sum(conv_vals * conv_vals, axis=1),
            jnp.where(core == 0, row_part, nothing),
            jnp.where(core == 0, nothing, row_part),
            norm_gain,
        ]
    )
    told = lax.all_to_all(
        jnp.broadcast_to(vector[None, None], (n_tp, 1, vector.size)), TP, 0, 0, tiled=True
    )[:, 0]
    cut = 3 * tok_rows + 2 * rows
    total = jnp.sum(told[:, :cut], axis=0)
    gains = told[:, cut:].reshape(n_z, wide)
    row_squares, conv_total, conv_squares = jnp.split(total[: 3 * tok_rows], 3)
    slot_squares = jnp.where(
        core == 0, total[3 * tok_rows : 3 * tok_rows + rows], total[3 * tok_rows + rows :]
    )
    inverse = lax.rsqrt(row_squares / model_width + EPSILON)[:, None]
    slot_inverse = lax.rsqrt(slot_squares / model_width + EPSILON)[:, None]

    xr, cl, cr, xl = [x0], [c0], [c0], [x0]
    for _ in range(half - 1):
        xr.append(right(xr[-1]))
        cl.append(left(cl[-1]))
        cr.append(right(cr[-1]))
        xl.append(left(xl[-1]))
    xf, cf = right(xr[-1]), left(cl[-1])
    offsets = (0, -1, 1, -2, 2, -3, 3, 4)
    xb, cb = [x0], [c0]
    for k in range(1, half):
        xb += [xr[k], xl[k]]
        cb += [cr[k], cl[k]]
    *sums, xs1 = project(
        zs, xb[:5], cb[:5], weights, gains, slot_inverse, offsets[:5], n_z, None
    )
    own, oth, back, xs2 = project(
        zs, xb[5:], cb[5:], weights, gains, slot_inverse, offsets[5:-1], n_z, sums
    )
    xs = (xs1, xs2)
    cb.append(cf)

    x4, b_own, b_oth, a_own, a_oth, along, ra, la = pl.pallas_call(
        lambda *r: finish_body(*r, n=n_z),
        out_shape=(
            jax.ShapeDtypeStruct((rows, wide), BF),
            jax.ShapeDtypeStruct((rows, 2 * hid), BF),
            jax.ShapeDtypeStruct((rows, 2 * hid), BF),
            jax.ShapeDtypeStruct((rows, hid), BF),
            jax.ShapeDtypeStruct((rows, hid), BF),
            jax.ShapeDtypeStruct((8, wide), F4),
            jax.ShapeDtypeStruct((rows // 2 + 16, wide), BF),
            jax.ShapeDtypeStruct((rows // 2, wide), BF),
        ),
        in_specs=[SMEM] + [VMEM] * 2 + [ANY] * 4 + [VMEM] * 5,
        out_specs=(ANY,) * 5 + (VMEM,) * 3,
        scratch_shapes=[
            pltpu.VMEM((rows, wide), BF),
            pltpu.VMEM((rows, 2 * hid), BF),
            pltpu.VMEM((rows, 2 * hid), BF),
            pltpu.VMEM((rows, hid), BF),
            pltpu.VMEM((rows, hid), BF),
            pltpu.VMEM((wide, 2 * hid), BF),
            pltpu.VMEM((wide, 2 * hid), BF),
            pltpu.VMEM((hid, wide), BF),
            pltpu.VMEM((hid, wide), BF),
            pltpu.SemaphoreType.DMA((5,)),
        ],
        compiler_params=BIG,
        name="finish",
    )(zs, xf, cf, *weights, gains, slot_inverse, own, oth, back)

    ra, la = right(ra), left(la)
    parts = pl.pallas_call(
        lambda *r: parts_body(*r, n=n_z),
        out_shape=jax.ShapeDtypeStruct((rows, model_width), BF),
        in_specs=[VMEM] * 2 + [ANY] * 2,
        out_specs=VMEM,
        scratch_shapes=[
            pltpu.VMEM((model_width, 2 * hid), BF),
            pltpu.VMEM((model_width, 2 * hid), BF),
            pltpu.SemaphoreType.DMA((2 * n_z,)),
        ],
        compiler_params=BIG,
        name="parts",
    )(b_own, b_oth, *weights[:2])
    message = jax.ShapeDtypeStruct((rows + 16, wide), BF)
    for k in range(half - 1, 0, -1):
        ra, la = pl.pallas_call(
            lambda *r, k=k: hop_body(*r, k=k, n=n_z, first=k == half - 1),
            out_shape=(message, message),
            in_specs=[SMEM] + [VMEM] * 4,
            out_specs=(VMEM, VMEM),
            compiler_params=BIG,
            name="hop",
        )(zs, parts, along, ra, la)
        ra, la = right(ra), left(la)
        if k == 2:
            others = grads(zs, xs, x4, cb, b_oth, a_oth, None, offsets)
            ra, la, others = lax.optimization_barrier((ra, la, others))
    sent_back = pl.pallas_call(
        lambda *r: pack_body(*r, n_sp=n_sp),
        out_shape=jax.ShapeDtypeStruct((slot_count, width_part + 128), BF),
        in_specs=[SMEM] + [VMEM] * 4,
        out_specs=VMEM,
        scratch_shapes=[pltpu.VMEM((rows, wide), F4), pltpu.VMEM((rows, 128), F4)],
        compiler_params=BIG,
        name="pack",
    )(zs, parts, along, ra, la)
    sent_back, others = lax.optimization_barrier((sent_back, others))
    others = swap(others)
    returned = lax.all_to_all(
        sent_back.reshape(2 * n_sp, half_cap, width_part + 128), ("sp", "c"), 0, 0, tiled=True
    ).reshape(slot_count, width_part + 128)

    token_back = dot(picker, returned, 0, 0)
    inner = jnp.sum(token_back[:, width_part : width_part + 3], axis=1, keepdims=True)
    gained = norm_gain[None, :] * token_back[:, :width_part]
    norm_back = inverse * gained - residual * inverse**2 * (inner / model_width)
    stream_grad = (upstream.astype(F4) + norm_back).astype(BF)

    p1, m1, p2, m2 = (hops(stream_grad, d) for d in (1, -1, 2, -2))
    p3, m3 = hops(p1, 2), hops(m1, -2)
    far = hops(p2, 2)
    mine8 = pl.pallas_call(
        stack_body,
        out_shape=jax.ShapeDtypeStruct((n_z * tok_rows, width_part), BF),
        in_specs=[VMEM] * 8,
        out_specs=VMEM,
        compiler_params=BIG,
        name="stack",
    )(stream_grad, m1, m2, m3, far, p3, p2, p1).reshape(n_z, tok_rows, width_part)
    other8 = swap(mine8)

    mean_val = (conv_total / channels)[:, None]
    variance = (conv_squares / channels)[:, None] - mean_val * mean_val
    inv_std = lax.rsqrt(variance + EPSILON)
    centred = (conv_vals - mean_val) * inv_std
    scaled = centred * ln_gain[None, :]
    mixed_out = jax.nn.silu(scaled).astype(BF)

    zc = jnp.stack([z, core]).astype(jnp.int32)
    slope = silu_slope(scaled) * ln_gain[None, :]
    norm_in = pl.pallas_call(
        lambda *r: mixed_body(*r, n=n_z),
        out_shape=jax.ShapeDtypeStruct(conv_pre.shape, F4),
        in_specs=[SMEM] + [VMEM] * 4,
        out_specs=VMEM,
        compiler_params=BIG,
        name="mixed",
    )(zc, mine8, other8, w_out, slope)
    out_parts = pl.pallas_call(
        lambda *r: outer_body(*r, n=n_z),
        out_shape=jax.ShapeDtypeStruct((n_sp, conv_pre.shape[1], width_part), BF),
        in_specs=[SMEM] + [VMEM] * 3,
        out_specs=VMEM,
        compiler_params=BIG,
        name="outer",
    )(zc, mine8, other8, mixed_out.T)
    norm_total, norm_cross = in_one((jnp.sum(norm_in, axis=1), jnp.sum(norm_in * centred, axis=1)))
    conv_back = inv_std * (
        norm_in - (norm_total / channels)[:, None] - centred * (norm_cross / channels)[:, None]
    )
    next_rim = lax.ppermute(conv_back[:32], "sp", [(i + 1, i) for i in range(n_sp - 1)])
    out_blocks = lax.all_to_all(out_parts, "sp", 0, 0, tiled=True)
    grad_gate, grad_up, grad_down = grads(zs, xs, x4, cb, b_own, a_own, others, offsets)
    conv_back, grad_gate, grad_up, grad_down = lax.optimization_barrier(
        (conv_back, grad_gate, grad_up, grad_down)
    )
    value_grad, gate_grad = pl.pallas_call(
        conv_body,
        out_shape=(jax.ShapeDtypeStruct(value_in.shape, BF),) * 2,
        in_specs=[VMEM] * 5,
        out_specs=(VMEM, VMEM),
        scratch_shapes=[pltpu.VMEM((tok_rows + 32, conv_pre.shape[1]), F4)],
        name="conv",
    )(conv_back, next_rim, conv_taps, value_in, gate_in)
    out_blocks, value_grad = lax.optimization_barrier((out_blocks, value_grad))
    grad_out = jnp.sum(out_blocks.astype(F4), axis=0)
    return (grad_gate[None], grad_up[None], grad_down[None], grad_out, value_grad, gate_grad)


def solution(mesh):
    n_sp, n_tp = mesh.devices.shape
    split = Mesh(mesh.devices.reshape(n_sp, n_tp // 2, 2), ("sp", "z", "c"))
    return jax.shard_map(
        per_device,
        mesh=split,
        in_specs=(
            P("sp", TP),
            P("sp", TP),
            P(TP),
            P("sp", None),
            P("sp", None),
            P("sp", None, TP),
            P("sp", None, TP),
            P("sp", TP, None),
            P("sp", TP),
            P("sp", TP),
            P("sp", TP),
            P(TP),
            P(None, TP),
            P(TP, None),
        ),
        out_specs=(
            P("sp", None, TP),
            P("sp", None, TP),
            P("sp", TP, None),
            P(TP, "sp"),
            P("sp", TP),
            P("sp", TP),
        ),
        check_vma=False,
    )
```

```python
import jax
import jax.numpy as jnp
from jax import lax
from jax.experimental import pallas as pl
from jax.experimental.pallas import tpu as pltpu
from jax.sharding import Mesh, PartitionSpec as P

EPSILON = 1e-06
TP = ("z", "c")
BF = jnp.bfloat16
F4 = jnp.float32


def of_everyone(value):
    count = 16
    everything = lax.all_to_all(
        jnp.broadcast_to(value[None], (count, *value.shape)), TP, 0, 0, tiled=True
    )
    return jnp.sum(everything, axis=0)


def in_one(arrays):
    total = of_everyone(jnp.concatenate([a.reshape(-1) for a in arrays]))
    out, at = [], 0
    for a in arrays:
        out.append(total[at : at + a.size].reshape(a.shape))
        at += a.size
    return out


def right(x):
    n = lax.axis_size("z")
    return lax.ppermute(x, "z", [(i, (i + 1) % n) for i in range(n)])


def left(x):
    n = lax.axis_size("z")
    return lax.ppermute(x, "z", [(i, (i - 1) % n) for i in range(n)])


def hops(x, n_hops):
    n = lax.axis_size("z")
    return lax.ppermute(x, "z", [(i, (i + n_hops) % n) for i in range(n)])


def swap(x):
    return lax.ppermute(x, "c", [(0, 1), (1, 0)])


def silu_slope(values):
    logistic = jax.nn.sigmoid(values)
    return logistic * (1.0 + values * (1.0 - logistic))


def dot(a, b, ca, cb):
    return lax.dot_general(a, b, (((ca,), (cb,)), ((), ())), preferred_element_type=F4)


VMEM = pl.BlockSpec(memory_space=pltpu.VMEM)
ANY = pl.BlockSpec(memory_space=pl.ANY)
HBM = pl.BlockSpec(memory_space=pltpu.HBM)
SMEM = pl.BlockSpec(memory_space=pltpu.SMEM)
BIG = pltpu.CompilerParams(vmem_limit_bytes=40 * 2**20)


def scatter_body(
    routes_h, weights_h, upstream_h, stream_h, picker, sent, *scratch, experts, capacity
):
    routes, weights, upstream, stream, sems = scratch
    load_all(
        [(routes_h, routes), (weights_h, weights), (upstream_h, upstream), (stream_h, stream)],
        sems,
    )
    toks = upstream.shape[0]
    slots = experts * capacity
    half = capacity // 2
    r0, r1 = routes[0:1, :], routes[1:2, :]
    names = lax.broadcasted_iota(jnp.int32, (experts, toks), 0)
    hot0 = jnp.where(names == r0, 1.0, 0.0)
    hot1 = jnp.where(names == r1, 1.0, 0.0)
    earlier = jnp.where(
        lax.broadcasted_iota(jnp.int32, (toks, toks), 0)
        < lax.broadcasted_iota(jnp.int32, (toks, toks), 1),
        1.0,
        0.0,
    ).astype(BF)
    before = dot((hot0 + hot1).astype(BF), earlier, 1, 0)
    slot0 = r0 * capacity + jnp.sum(before * hot0, axis=0, keepdims=True).astype(jnp.int32)
    slot1 = r1 * capacity + jnp.sum(before * hot1, axis=0, keepdims=True).astype(jnp.int32)
    blocks = 4
    step = blocks * capacity

    def rows_at(j, carry):
        at = j * (step // 2)
        ids = lax.broadcasted_iota(jnp.int32, (step // 2, toks), 0) + at
        one = jnp.where(ids == slot0, 1.0, 0.0) + jnp.where(ids == slot1, 1.0, 0.0)
        picker[pl.ds(pl.multiple_of(at, step // 2), step // 2), :] = one.astype(BF)
        wide = lax.broadcasted_iota(jnp.int32, (step, toks), 0)
        block = lax.shift_right_logical(wide * (65536 // capacity + 1), 16)
        place = wide - block * capacity
        ids = jnp.where(place >= half, place - half, place) + (block + j * blocks) * half
        hit0, hit1 = ids == slot0, ids == slot1
        pick = (jnp.where(hit0, 1.0, 0.0) + jnp.where(hit1, 1.0, 0.0)).astype(BF)
        weight = jnp.sum(
            jnp.where(hit0, weights[0:1, :], 0.0) + jnp.where(hit1, weights[1:2, :], 0.0),
            axis=1,
            keepdims=True,
        )
        is_cot = place[:, 0:1] >= half
        value = jnp.where(
            is_cot, dot(pick, upstream[...], 1, 0) * weight, dot(pick, stream[...], 1, 0)
        )
        sent[pl.ds(pl.multiple_of(j * step, step), step), :] = value.astype(BF)
        return carry

    lax.fori_loop(0, 2 * slots // step, rows_at, 0)


def offset_of(k, offsets, n):
    off = jnp.int32(0)
    for i, value in enumerate(offsets):
        off = jnp.where(k == i, value % n, off)
    return off


def load_all(pairs, sems):
    copies = [pltpu.make_async_copy(a, b, sems.at[i]) for i, (a, b) in enumerate(pairs)]
    for copy in copies:
        copy.start()
    for copy in copies:
        copy.wait()


def loaded(groups, sems, step):
    copies, at = [], 0
    for group in groups:
        copies.append([])
        for a, b in group:
            copies[-1].append(pltpu.make_async_copy(a, b, sems.at[at]))
            at += 1
    for group in copies:
        for copy in group:
            copy.start()
    for group in copies:
        for copy in group:
            copy.wait()
    lax.fori_loop(0, len(groups), step, 0)


def unpack_body(arrived, x, c, *, n_sp):
    half = x.shape[0] // n_sp
    width = arrived.shape[1]
    for s in range(0, n_sp, 2):
        for core in range(2):
            pair = []
            for src in (s, s + 1):
                at = (2 * src + core) * 2 * half
                pair.append(arrived[at : at + 2 * half, :].astype(F4))
            lanes = pl.ds(core * width, width)
            to = pl.ds(s * half, 2 * half)
            x[to, lanes] = jnp.concatenate([p[:half] for p in pair], axis=0).astype(BF)
            c[to, lanes] = jnp.concatenate([p[half:] for p in pair], axis=0).astype(BF)


def project_body(z, *refs, offsets, n, more):
    m = len(offsets)
    xb, cb, refs = refs[:m], refs[m : 2 * m], refs[2 * m :]
    guo, gux, dno, dnx, gains, inv = refs[:6]
    starts, refs = (refs[6:9], refs[9:]) if more else (None, refs[6:])
    own, oth, back, xs = refs[:4]
    xbuf, cbuf, xs_v, own_v, oth_v, dno_v, dnx_v, sems = refs[4:]
    rows, width = own.shape[0], xbuf.shape[2]
    hid = back.shape[1] // 2
    groups = []
    for i, off in enumerate(offsets):
        at = pl.multiple_of(lax.rem(z[0] + off % n, n) * width, width)
        groups.append(
            [
                (xb[i], xbuf.at[i]),
                (cb[i], cbuf.at[i]),
                (guo.at[pl.ds(at, width), :], own_v.at[i]),
                (gux.at[pl.ds(at, width), :], oth_v.at[i]),
                (dno.at[:, pl.ds(at, width)], dno_v.at[i]),
                (dnx.at[:, pl.ds(at, width)], dnx_v.at[i]),
            ]
        )
    for i, total in enumerate((own, oth, back)):
        total[...] = starts[i][...] if more else jnp.zeros(total.shape, F4)

    def step(k, carry):
        chip = lax.rem(z[0] + offset_of(k, offsets, n), n)
        x = xbuf[k].astype(F4)
        x = (gains[pl.ds(chip, 1), :] * x * inv[...]).astype(BF)
        xs_v[pl.ds(pl.multiple_of(k * rows, rows), rows), :] = x
        own[...] += dot(x, own_v[k], 1, 0)
        oth[...] += dot(x, oth_v[k], 1, 0)
        c = cbuf[k]
        back[:, :hid] += dot(c, dno_v[k], 1, 1)
        back[:, hid:] += dot(c, dnx_v[k], 1, 1)
        return carry

    loaded(groups, sems, step)
    load_all([(xs_v, xs)], sems)


def project(z, xb, cb, weights, gains, inv, offsets, n, starts):
    rows, wide = xb[0].shape
    m, hid = len(xb), weights[2].shape[0]
    total = jax.ShapeDtypeStruct((rows, 2 * hid), F4)
    return pl.pallas_call(
        lambda *r: project_body(*r, offsets=offsets, n=n, more=starts is not None),
        out_shape=(total, total, total, jax.ShapeDtypeStruct((m * rows, wide), BF)),
        in_specs=[SMEM] + [ANY] * (2 * m + 4) + [VMEM] * (2 + len(starts or ())),
        out_specs=(VMEM, VMEM, VMEM, ANY),
        scratch_shapes=[
            pltpu.VMEM((m, rows, wide), BF),
            pltpu.VMEM((m, rows, wide), BF),
            pltpu.VMEM((m * rows, wide), BF),
            pltpu.VMEM((m, wide, 2 * hid), BF),
            pltpu.VMEM((m, wide, 2 * hid), BF),
            pltpu.VMEM((m, hid, wide), BF),
            pltpu.VMEM((m, hid, wide), BF),
            pltpu.SemaphoreType.DMA((6 * m,)),
        ],
        compiler_params=BIG,
        name="project",
    )(z, *xb, *cb, *weights, gains, inv, *(starts or ()))


def in_parts(row):
    hi = row.astype(BF).astype(F4)
    mid = (row - hi).astype(BF).astype(F4)
    low = (row - hi - mid).astype(BF).astype(F4)
    return hi, mid, low


def part_rows(row):
    hi, mid, low = in_parts(row)
    shape = (16, row.shape[1])
    at = lax.broadcasted_iota(jnp.int32, shape, 0)
    rows = jnp.where(at == 0, hi, jnp.where(at == 1, mid, jnp.where(at == 2, low, 0.0)))
    return rows.astype(BF)


def whole_row(rows):
    rows = rows.astype(F4)
    return rows[0:1] + rows[1:2] + rows[2:3]


def finish_body(z, xf, cf, guo, gux, dno, dnx, gains, inv, own, oth, back, *refs, n):
    hbm, refs = refs[:5], refs[5:]
    along, send_r, send_l = refs[:3]
    held = refs[3:8]
    x4, b_own, b_oth, a_own, a_oth = held
    own_v, oth_v, dno_v, dnx_v, sems = refs[8:]
    rows, width = xf.shape
    hid = dno.shape[0]
    chip = lax.rem(z[0] + n // 2, n)
    at = pl.multiple_of(chip * width, width)
    load_all(
        [
            (guo.at[pl.ds(at, width), :], own_v),
            (gux.at[pl.ds(at, width), :], oth_v),
            (dno.at[:, pl.ds(at, width)], dno_v),
            (dnx.at[:, pl.ds(at, width)], dnx_v),
        ],
        sems,
    )
    x = (gains[pl.ds(chip, 1), :] * xf[...].astype(F4) * inv[...]).astype(BF)
    x4[...] = x
    total = jnp.zeros((rows, 1), F4)
    for pre, w_v, d_v, lo, backs, act in (
        (own, own_v, dno_v, 0, b_own, a_own),
        (oth, oth_v, dnx_v, hid, b_oth, a_oth),
    ):
        both = pre[...] + dot(x, w_v[...], 1, 0)
        gate, upper = both[:, :hid], both[:, hid:]
        ab = back[:, lo : lo + hid] + dot(cf[...], d_v[...], 1, 1)
        sig = jax.nn.sigmoid(gate)
        silu = gate * sig
        act[...] = (silu * upper).astype(BF)
        gb = (ab * upper * (sig * (1.0 + gate * (1.0 - sig)))).astype(BF)
        ub = (ab * silu).astype(BF)
        backs[:, :hid] = gb
        backs[:, hid:] = ub
        total = total + jnp.sum(
            gb.astype(F4) * gate + ub.astype(F4) * upper, axis=1, keepdims=True
        )
    copies = [
        pltpu.make_async_copy(a, b, sems.at[i]) for i, (a, b) in enumerate(zip(held, hbm))
    ]
    for copy in copies:
        copy.start()
    row = jnp.broadcast_to(total, (rows, 128)).T[0:8, :]
    along[:, :rows] = row
    along[:, rows:] = jnp.zeros((8, width - rows), F4)
    part = dot(b_own[...], own_v[...], 1, 1) + dot(b_oth[...], oth_v[...], 1, 1)
    hr = rows // 2
    send_r[:hr, :] = part[:hr].astype(BF)
    send_r[hr:, :] = part_rows(along[0:1, :])
    send_l[...] = part[hr:].astype(BF)
    for copy in copies:
        copy.wait()


def parts_body(b_own, b_oth, guo, gux, out, guo_v, gux_v, sems, *, n):
    width = guo.shape[0] // n

    def copies(k):
        at = pl.ds(pl.multiple_of(k * width, width), width)
        return (
            pltpu.make_async_copy(guo.at[at, :], guo_v.at[at, :], sems.at[2 * k]),
            pltpu.make_async_copy(gux.at[at, :], gux_v.at[at, :], sems.at[2 * k + 1]),
        )

    def begin(k, carry):
        for copy in copies(k):
            copy.start()
        return carry

    def step(k, carry):
        for copy in copies(k):
            copy.wait()
        at = pl.ds(pl.multiple_of(k * width, width), width)
        out[:, at] = (
            dot(b_own[...], guo_v[at, :], 1, 1) + dot(b_oth[...], gux_v[at, :], 1, 1)
        ).astype(BF)
        return carry

    lax.fori_loop(0, n, begin, 0)
    lax.fori_loop(0, n, step, 0)


def hop_body(z, parts, along, ra, la, out_r, out_l, *, k, n, first):
    rows = parts.shape[0]
    width = out_r.shape[1]
    hr = rows // 2

    def block(j):
        at = pl.multiple_of(lax.rem(z[0] + (j + n), n) * width, width)
        return parts[:, pl.ds(at, width)].astype(F4)

    own = along[0:1, :]
    pr, pl_ = block(k), block(-k)
    if first:
        out_r[:hr, :] = (pr[:hr] + ra[:hr, :].astype(F4)).astype(BF)
        out_r[hr:rows, :] = pr[hr:].astype(BF)
        out_r[rows:, :] = part_rows(own + whole_row(ra[hr:, :]))
        out_l[:hr, :] = pl_[:hr].astype(BF)
        out_l[hr:rows, :] = (pl_[hr:] + la[...].astype(F4)).astype(BF)
        out_l[rows:, :] = part_rows(own)
    else:
        out_r[:rows, :] = (pr + ra[:rows, :].astype(F4)).astype(BF)
        out_r[rows:, :] = part_rows(own + whole_row(ra[rows:, :]))
        out_l[:rows, :] = (pl_ + la[:rows, :].astype(F4)).astype(BF)
        out_l[rows:, :] = part_rows(own + whole_row(la[rows:, :]))


def pack_body(z, parts, along, ra, la, out, value, extra, *, n_sp):
    rows = parts.shape[0]
    width = ra.shape[1]
    half = width // 2
    step = rows // n_sp
    at = pl.multiple_of(z[0] * width, width)
    row = along[0:1, :] + whole_row(ra[rows:, :]) + whole_row(la[rows:, :])
    col = jnp.broadcast_to(row[:, :rows], (128, rows)).T
    hi, mid, low = in_parts(col)
    lane = lax.broadcasted_iota(jnp.int32, (rows, 128), 1)
    extra[...] = jnp.where(
        lane == 0, hi, jnp.where(lane == 1, mid, jnp.where(lane == 2, low, 0.0))
    )
    value[...] = (
        parts[:, pl.ds(at, width)].astype(F4) + ra[:rows, :].astype(F4) + la[:rows, :].astype(F4)
    )

    def one(s, carry):
        at = pl.ds(pl.multiple_of(s * step, 8), step)
        to = pl.ds(pl.multiple_of(s * 2 * step, 16), 2 * step)
        v, e = value[at, :], extra[at, :]
        both = jnp.concatenate([v[:, :half], v[:, half:]], axis=0)
        out[to, :half] = both.astype(BF)
        out[to, half:] = jnp.concatenate([e, e], axis=0).astype(BF)
        return carry

    lax.fori_loop(0, n_sp, one, 0)


def grads_body(z, *refs, n, add, offsets):
    xs1, xs2, x4 = refs[:3]
    cb = refs[3 : n + 3]
    backs, act = refs[n + 3], refs[n + 4]
    refs = refs[n + 5 :]
    if add:
        old_h, gate, up, down, old, xbuf, cbuf, sems = refs
    else:
        out, ready, xbuf, cbuf, sems = refs
        ready[...] = jnp.zeros(ready.shape, F4)
    rows, width = x4.shape
    hid = act.shape[1]
    groups = []
    for k in range(n):
        groups.append([(cb[k], cbuf.at[pl.ds(k * rows, rows), :])])
    at = 0
    for x in (xs1, xs2, x4):
        groups[0].append((x, xbuf.at[pl.ds(at, x.shape[0]), :]))
        at += x.shape[0]
    if add:
        groups[0].append((old_h, old))

    def step(k, carry):
        at = pl.multiple_of(lax.rem(z[0] + offset_of(k, offsets, n), n) * width, width)
        mine = pl.ds(pl.multiple_of(k * rows, rows), rows)
        pair = dot(xbuf[mine, :], backs[...], 0, 0)
        dn = dot(act[...], cbuf[mine, :], 0, 0)
        if add:
            gate[pl.ds(at, width), :] = pair[:, :hid] + old[0, pl.ds(at, width), :].astype(F4)
            up[pl.ds(at, width), :] = pair[:, hid:] + old[1, pl.ds(at, width), :].astype(F4)
            for q in range(width // hid):
                lo = pl.multiple_of(at + q * hid, hid)
                down[:, pl.ds(lo, hid)] = dn[:, q * hid : (q + 1) * hid] + old[
                    2, pl.ds(lo, hid), :
                ].astype(F4)
        else:
            out[0, pl.ds(at, width), :] = pair[:, :hid].astype(BF)
            out[1, pl.ds(at, width), :] = pair[:, hid:].astype(BF)
            for q in range(width // hid):
                lo = pl.multiple_of(at + q * hid, hid)
                out[2, pl.ds(lo, hid), :] = dn[:, q * hid : (q + 1) * hid].astype(BF)
        return carry

    loaded(groups, sems, step)


def grads(z, xs, x4, cb, backs, act, old, offsets):
    rows, width = x4.shape
    n, hid = len(cb), act.shape[1]
    add = old is not None
    total = n * width
    args = [z, *xs, x4, *cb, backs, act] + ([old] if add else [])
    if add:
        out_shape = tuple(
            jax.ShapeDtypeStruct(t, F4) for t in ((total, hid), (total, hid), (hid, total))
        )
        out_specs = (VMEM,) * 3
    else:
        out_shape = (
            jax.ShapeDtypeStruct((3, total, hid), BF),
            jax.ShapeDtypeStruct((8, 128), F4),
        )
        out_specs = (VMEM, VMEM)
    return pl.pallas_call(
        lambda *r: grads_body(*r, n=n, add=add, offsets=offsets),
        out_shape=out_shape,
        in_specs=[SMEM] + [ANY] * (n + 3) + [VMEM] * 2 + ([ANY] if add else []),
        out_specs=out_specs,
        scratch_shapes=([pltpu.VMEM((3, total, hid), BF)] if add else [])
        + [
            pltpu.VMEM((n * rows, width), BF),
            pltpu.VMEM((n * rows, width), BF),
            pltpu.SemaphoreType.DMA((n + 4,)),
        ],
        compiler_params=BIG,
        cost_estimate=pl.CostEstimate(
            flops=8 * rows * total * 3 * hid, transcendentals=0, bytes_accessed=16 * 2**20
        ),
        name="grads_own" if add else "grads_other",
    )(*args)


def stack_body(*refs):
    out, at = refs[-1], 0
    for src in refs[:-1]:
        out[pl.ds(at, src.shape[0]), :] = src[...]
        at += src.shape[0]


def mixed_body(zc, mine, other, w_out, slope, out, *, n):
    width = mine.shape[2]
    out[...] = jnp.zeros(out.shape, F4)

    def step(k, carry):
        base = 2 * lax.rem(zc[0] + k, n)
        a = pl.multiple_of((base + zc[1]) * width, width)
        b = pl.multiple_of((base + 1 - zc[1]) * width, width)
        out[...] += dot(mine[k], w_out[:, pl.ds(a, width)], 1, 1) + dot(
            other[k], w_out[:, pl.ds(b, width)], 1, 1
        )
        return carry

    lax.fori_loop(0, n, step, 0)
    out[...] *= slope[...]


def outer_body(zc, mine, other, mixed_t, out, *, n):
    def step(k, carry):
        base = 2 * lax.rem(zc[0] + k, n)
        out[base + zc[1]] = dot(mixed_t[...], mine[k], 1, 0).astype(BF)
        out[base + 1 - zc[1]] = dot(mixed_t[...], other[k], 1, 0).astype(BF)
        return carry

    lax.fori_loop(0, n, step, 0)


def conv_body(back, rim, taps, value_in, gate_in, value_grad, gate_grad, padded):
    toks, n_taps = back.shape[0], taps.shape[0]
    padded[:toks, :] = back[...]
    padded[toks:, :] = rim[...]
    step = 128
    for at in range(0, toks, step):
        acc = jnp.zeros((step, back.shape[1]), F4)

        def one(tap, acc, at=at):
            lo = at + n_taps - 1 - tap
            return acc + taps[pl.ds(tap, 1), :] * padded[pl.ds(lo, step), :]

        acc = lax.fori_loop(0, n_taps, one, acc)
        sigma = jax.nn.sigmoid(gate_in[at : at + step, :].astype(F4))
        value = acc * sigma
        value_grad[at : at + step, :] = value.astype(BF)
        gate_grad[at : at + step, :] = (
            value * value_in[at : at + step, :].astype(F4) * (1.0 - sigma)
        ).astype(BF)


def per_device(
    upstream,
    stream,
    norm_gain,
    routes,
    route_weights,
    w_gate,
    w_up,
    w_down,
    value_in,
    gate_in,
    conv_pre,
    ln_gain,
    conv_taps,
    w_out,
):
    tok_rows, width_part = stream.shape
    n_sp = lax.axis_size("sp")
    n_z = lax.axis_size("z")
    n_tp = 2 * n_z
    z = lax.axis_index("z")
    core = lax.axis_index("c")
    model_width = width_part * n_tp
    channels = conv_pre.shape[1] * n_tp
    tap_count = conv_taps.shape[0]
    capacity = 3 * tok_rows // n_sp
    half_cap = capacity // 2
    experts = n_sp
    slot_count = experts * capacity
    rows = n_sp * half_cap
    wide = 2 * width_part

    zs = z.astype(jnp.int32).reshape(1)
    half = n_z // 2
    hid = w_gate.shape[2]

    picker, sent = pl.pallas_call(
        lambda *r: scatter_body(*r, experts=experts, capacity=capacity),
        out_shape=(
            jax.ShapeDtypeStruct((slot_count, tok_rows), BF),
            jax.ShapeDtypeStruct((2 * slot_count, width_part), BF),
        ),
        in_specs=[HBM] * 4,
        out_specs=(VMEM, VMEM),
        scratch_shapes=[
            pltpu.VMEM((2, tok_rows), jnp.int32),
            pltpu.VMEM((2, tok_rows), F4),
            pltpu.VMEM(upstream.shape, BF),
            pltpu.VMEM(stream.shape, BF),
            pltpu.SemaphoreType.DMA((4,)),
        ],
        compiler_params=BIG,
        name="scatter",
    )(routes.T, route_weights.T, upstream, stream)
    arrived = lax.all_to_all(
        sent.reshape(2 * experts, capacity, width_part), ("sp", "c"), 0, 0, tiled=True
    )
    x0, c0 = pl.pallas_call(
        lambda *r: unpack_body(*r, n_sp=n_sp),
        out_shape=(jax.ShapeDtypeStruct((rows, wide), BF),) * 2,
        in_specs=[VMEM],
        out_specs=(VMEM, VMEM),
        compiler_params=BIG,
        name="unpack",
    )(arrived.reshape(2 * slot_count, width_part))

    gu_own = jnp.concatenate([w_gate[0], w_up[0]], axis=1)
    weights = (gu_own, swap(gu_own), w_down[0], swap(w_down[0]))

    residual = stream.astype(F4)
    conv_vals = conv_pre.astype(F4)
    own_rows = x0.astype(F4)
    row_part = jnp.sum(own_rows * own_rows, axis=1)
    nothing = jnp.zeros_like(row_part)
    vector = jnp.concatenate(
        [
            jnp.sum(residual * residual, axis=1),
            jnp.sum(conv_vals, axis=1),
            jnp.sum(conv_vals * conv_vals, axis=1),
            jnp.where(core == 0, row_part, nothing),
            jnp.where(core == 0, nothing, row_part),
            norm_gain,
        ]
    )
    told = lax.all_to_all(
        jnp.broadcast_to(vector[None, None], (n_tp, 1, vector.size)), TP, 0, 0, tiled=True
    )[:, 0]
    cut = 3 * tok_rows + 2 * rows
    total = jnp.sum(told[:, :cut], axis=0)
    gains = told[:, cut:].reshape(n_z, wide)
    row_squares, conv_total, conv_squares = jnp.split(total[: 3 * tok_rows], 3)
    slot_squares = jnp.where(
        core == 0, total[3 * tok_rows : 3 * tok_rows + rows], total[3 * tok_rows + rows :]
    )
    inverse = lax.rsqrt(row_squares / model_width + EPSILON)[:, None]
    slot_inverse = lax.rsqrt(slot_squares / model_width + EPSILON)[:, None]

    xr, cl, cr, xl = [x0], [c0], [c0], [x0]
    for _ in range(half - 1):
        xr.append(right(xr[-1]))
        cl.append(left(cl[-1]))
        cr.append(right(cr[-1]))
        xl.append(left(xl[-1]))
    xf, cf = right(xr[-1]), left(cl[-1])
    offsets = (0, -1, 1, -2, 2, -3, 3, 4)
    xb, cb = [x0], [c0]
    for k in range(1, half):
        xb += [xr[k], xl[k]]
        cb += [cr[k], cl[k]]
    *sums, xs1 = project(
        zs, xb[:5], cb[:5], weights, gains, slot_inverse, offsets[:5], n_z, None
    )
    own, oth, back, xs2 = project(
        zs, xb[5:], cb[5:], weights, gains, slot_inverse, offsets[5:-1], n_z, sums
    )
    xs = (xs1, xs2)
    cb.append(cf)

    x4, b_own, b_oth, a_own, a_oth, along, ra, la = pl.pallas_call(
        lambda *r: finish_body(*r, n=n_z),
        out_shape=(
            jax.ShapeDtypeStruct((rows, wide), BF),
            jax.ShapeDtypeStruct((rows, 2 * hid), BF),
            jax.ShapeDtypeStruct((rows, 2 * hid), BF),
            jax.ShapeDtypeStruct((rows, hid), BF),
            jax.ShapeDtypeStruct((rows, hid), BF),
            jax.ShapeDtypeStruct((8, wide), F4),
            jax.ShapeDtypeStruct((rows // 2 + 16, wide), BF),
            jax.ShapeDtypeStruct((rows // 2, wide), BF),
        ),
        in_specs=[SMEM] + [VMEM] * 2 + [ANY] * 4 + [VMEM] * 5,
        out_specs=(ANY,) * 5 + (VMEM,) * 3,
        scratch_shapes=[
            pltpu.VMEM((rows, wide), BF),
            pltpu.VMEM((rows, 2 * hid), BF),
            pltpu.VMEM((rows, 2 * hid), BF),
            pltpu.VMEM((rows, hid), BF),
            pltpu.VMEM((rows, hid), BF),
            pltpu.VMEM((wide, 2 * hid), BF),
            pltpu.VMEM((wide, 2 * hid), BF),
            pltpu.VMEM((hid, wide), BF),
            pltpu.VMEM((hid, wide), BF),
            pltpu.SemaphoreType.DMA((5,)),
        ],
        compiler_params=BIG,
        name="finish",
    )(zs, xf, cf, *weights, gains, slot_inverse, own, oth, back)

    ra, la = right(ra), left(la)
    parts = pl.pallas_call(
        lambda *r: parts_body(*r, n=n_z),
        out_shape=jax.ShapeDtypeStruct((rows, model_width), BF),
        in_specs=[VMEM] * 2 + [ANY] * 2,
        out_specs=VMEM,
        scratch_shapes=[
            pltpu.VMEM((model_width, 2 * hid), BF),
            pltpu.VMEM((model_width, 2 * hid), BF),
            pltpu.SemaphoreType.DMA((2 * n_z,)),
        ],
        compiler_params=BIG,
        name="parts",
    )(b_own, b_oth, *weights[:2])
    message = jax.ShapeDtypeStruct((rows + 16, wide), BF)
    for k in range(half - 1, 0, -1):
        ra, la = pl.pallas_call(
            lambda *r, k=k: hop_body(*r, k=k, n=n_z, first=k == half - 1),
            out_shape=(message, message),
            in_specs=[SMEM] + [VMEM] * 4,
            out_specs=(VMEM, VMEM),
            compiler_params=BIG,
            name="hop",
        )(zs, parts, along, ra, la)
        ra, la = right(ra), left(la)
        if k == 2:
            others, ready = grads(zs, xs, x4, cb, b_oth, a_oth, None, offsets)
            ra, la, ready = lax.optimization_barrier((ra, la, ready))
    sent_back = pl.pallas_call(
        lambda *r: pack_body(*r, n_sp=n_sp),
        out_shape=jax.ShapeDtypeStruct((slot_count, width_part + 128), BF),
        in_specs=[SMEM] + [VMEM] * 4,
        out_specs=VMEM,
        scratch_shapes=[pltpu.VMEM((rows, wide), F4), pltpu.VMEM((rows, 128), F4)],
        compiler_params=BIG,
        name="pack",
    )(zs, parts, along, ra, la)
    sent_back, others = lax.optimization_barrier((sent_back, others))
    others = swap(others)
    returned = lax.all_to_all(
        sent_back.reshape(2 * n_sp, half_cap, width_part + 128), ("sp", "c"), 0, 0, tiled=True
    ).reshape(slot_count, width_part + 128)

    token_back = dot(picker, returned, 0, 0)
    inner = jnp.sum(token_back[:, width_part : width_part + 3], axis=1, keepdims=True)
    gained = norm_gain[None, :] * token_back[:, :width_part]
    norm_back = inverse * gained - residual * inverse**2 * (inner / model_width)
    stream_grad = (upstream.astype(F4) + norm_back).astype(BF)

    p1, m1, p2, m2 = (hops(stream_grad, d) for d in (1, -1, 2, -2))
    p3, m3 = hops(p1, 2), hops(m1, -2)
    far = hops(p2, 2)
    mine8 = pl.pallas_call(
        stack_body,
        out_shape=jax.ShapeDtypeStruct((n_z * tok_rows, width_part), BF),
        in_specs=[VMEM] * 8,
        out_specs=VMEM,
        compiler_params=BIG,
        name="stack",
    )(stream_grad, m1, m2, m3, far, p3, p2, p1).reshape(n_z, tok_rows, width_part)
    other8 = swap(mine8)

    mean_val = (conv_total / channels)[:, None]
    variance = (conv_squares / channels)[:, None] - mean_val * mean_val
    inv_std = lax.rsqrt(variance + EPSILON)
    centred = (conv_vals - mean_val) * inv_std
    scaled = centred * ln_gain[None, :]
    mixed_out = jax.nn.silu(scaled).astype(BF)

    zc = jnp.stack([z, core]).astype(jnp.int32)
    slope = silu_slope(scaled) * ln_gain[None, :]
    norm_in = pl.pallas_call(
        lambda *r: mixed_body(*r, n=n_z),
        out_shape=jax.ShapeDtypeStruct(conv_pre.shape, F4),
        in_specs=[SMEM] + [VMEM] * 4,
        out_specs=VMEM,
        compiler_params=BIG,
        name="mixed",
    )(zc, mine8, other8, w_out, slope)
    out_parts = pl.pallas_call(
        lambda *r: outer_body(*r, n=n_z),
        out_shape=jax.ShapeDtypeStruct((n_sp, conv_pre.shape[1], width_part), BF),
        in_specs=[SMEM] + [VMEM] * 3,
        out_specs=VMEM,
        compiler_params=BIG,
        name="outer",
    )(zc, mine8, other8, mixed_out.T)
    norm_total, norm_cross = in_one((jnp.sum(norm_in, axis=1), jnp.sum(norm_in * centred, axis=1)))
    conv_back = inv_std * (
        norm_in - (norm_total / channels)[:, None] - centred * (norm_cross / channels)[:, None]
    )
    next_rim = lax.ppermute(conv_back[:32], "sp", [(i + 1, i) for i in range(n_sp - 1)])
    out_blocks = lax.all_to_all(out_parts, "sp", 0, 0, tiled=True)
    grad_gate, grad_up, grad_down = grads(zs, xs, x4, cb, b_own, a_own, others, offsets)
    conv_back, grad_gate, grad_up, grad_down = lax.optimization_barrier(
        (conv_back, grad_gate, grad_up, grad_down)
    )
    value_grad, gate_grad = pl.pallas_call(
        conv_body,
        out_shape=(jax.ShapeDtypeStruct(value_in.shape, BF),) * 2,
        in_specs=[VMEM] * 5,
        out_specs=(VMEM, VMEM),
        scratch_shapes=[pltpu.VMEM((tok_rows + 32, conv_pre.shape[1]), F4)],
        name="conv",
    )(conv_back, next_rim, conv_taps, value_in, gate_in)
    out_blocks, value_grad = lax.optimization_barrier((out_blocks, value_grad))
    grad_out = jnp.sum(out_blocks.astype(F4), axis=0)
    return (grad_gate[None], grad_up[None], grad_down[None], grad_out, value_grad, gate_grad)


def solution(mesh):
    n_sp, n_tp = mesh.devices.shape
    split = Mesh(mesh.devices.reshape(n_sp, n_tp // 2, 2), ("sp", "z", "c"))
    return jax.shard_map(
        per_device,
        mesh=split,
        in_specs=(
            P("sp", TP),
            P("sp", TP),
            P(TP),
            P("sp", None),
            P("sp", None),
            P("sp", None, TP),
            P("sp", None, TP),
            P("sp", TP, None),
            P("sp", TP),
            P("sp", TP),
            P("sp", TP),
            P(TP),
            P(None, TP),
            P(TP, None),
        ),
        out_specs=(
            P("sp", None, TP),
            P("sp", None, TP),
            P("sp", TP, None),
            P(TP, "sp"),
            P("sp", TP),
            P("sp", TP),
        ),
        check_vma=False,
    )
```
